32 devices in a mesh: ep: 8 (over z, x), tp: 4 (over y, core).
Axes of the slice: x: 2, y: 2, z: 4, core: 2. Of those that a mesh axis runs over, the one named last changes fastest.
Arguments:
- query_latent: bfloat16 [2048, 512], P(('ep', 'tp')), may hold values from -6 to 6
- key_latent: bfloat16 [2048, 256], P(('ep', 'tp')), may hold values from -6 to 6
- rotary_key: bfloat16 [2048, 32], P(('ep', 'tp')), may hold values from -140 to 140
- query_gain: float32 [512], replicated, may hold values from 0.1 to 1.9
- latent_gain: float32 [256], replicated, may hold values from 0.1 to 1.9
- query_content: bfloat16 [512, 512], replicated, may hold values from -0.625 to 0.625
- query_rotary: bfloat16 [512, 256], replicated, may hold values from -0.625 to 0.625
- key_content: bfloat16 [256, 512], replicated, may hold values from -0.375 to 0.375
- value_weight: bfloat16 [256, 512], replicated, may hold values from -0.375 to 0.375
- output_weight: bfloat16 [512, 2048], P('tp'), may hold values from -1 to 1
- expert_input: bfloat16 [2048, 2048], P(('ep', 'tp')), may hold values from -6 to 6
- norm_gain: float32 [2048], replicated, may hold values from 0.1 to 1.9
- routes: int32 [2048, 2], P(('ep', 'tp')), may hold values from 0 to 15, all different within a row; in each aligned block of 64 rows (0 to 63, 64 to 127, ...) at most 16 rows name the same one
- route_weight: float32 [2048, 2], P(('ep', 'tp')), may hold values from 0.25 to 2
- expert_gate: bfloat16 [16, 2048, 1024], P('ep', None, 'tp'), may hold values from -0.125 to 0.125
- expert_up: bfloat16 [16, 2048, 1024], P('ep', None, 'tp'), may hold values from -0.125 to 0.125
- expert_down: bfloat16 [16, 1024, 2048], P('ep', 'tp'), may hold values from -0.1875 to 0.1875
- shared_gate: bfloat16 [2048, 1024], P(None, 'tp'), may hold values from -0.125 to 0.125
- shared_up: bfloat16 [2048, 1024], P(None, 'tp'), may hold values from -0.125 to 0.125
- shared_down: bfloat16 [1024, 2048], P('tp'), may hold values from -0.1875 to 0.1875
Outputs:
- mixer_out: bfloat16 [2048, 2048], P(('ep', 'tp'))
- expert_out: bfloat16 [2048, 2048], P(('ep', 'tp'))
The draws below stay inside these ranges and needn't reach their ends.
Inputs may be any that keep to these rules, and one draw needn't show every extreme that they name: `routes`: each row names 2 different experts. Within the rows of one device (aligned blocks of 64 rows) no expert is named by more than 16 rows, and in every draw some expert is named by exactly 16 rows of some device.
All inputs are finite; a program needn't handle non-finite values.
Results may differ from the reference program's by a relative error of at most 0.013.
The reference program's roundings to bfloat16 on the way count: a program that leaves them out, or rounds other values in their place, can miss the bound.
Values may be sent and summed in bfloat16 or wider, within the bound.
A program may use at most 128 MiB of HBM per device.

```python
import math
from functools import partial
import jax
import jax.numpy as jnp
import numpy as np
from jax import lax

D = 2048
HEADS = 8
CONTENT = 64
ROTARY = 32
VALUE = 64
QUERY_RANK = 512
KEY_RANK = 256
EXPERT_WIDTH = 1024
SHARED_WIDTH = 1024
TOPK = 2
TOK_B = 64
EXPERTS = 16
CAPACITY = 16
TOKENS_A = 2048
TOKENS_B = 2048
N_EP = 8
N_TP = 4


def draw_rotary_key(key, part):
    normal_part = jnp.clip(jax.random.normal(jax.random.fold_in(key, 11), (TOKENS_A, ROTARY), jnp.float32), -6.0, 6.0)
    entries = normal_part
    return entries.astype(jnp.bfloat16)


def block_levels(rng, dims, shards, smallest, top_value):
    level = 1.0
    for dim, blocks in shards:
        draws = jax.random.uniform(jax.random.fold_in(jax.random.fold_in(rng, 6), dim), (blocks,), jnp.float32, smallest / len(shards), top_value / len(shards))
        level = level * jnp.repeat(jnp.exp(draws), dims[dim] // blocks).reshape((-1,) + (1,) * (len(dims) - 1 - dim))
    return level


def deal_out(rng, own, number, rows, amount, top, limit, slope):
    sequence = jax.random.permutation(rng, amount)
    crowded, ordinary = load_shares(amount, rows * top, limit, slope, True), load_shares(amount, rows * top, limit, slope, False)
    places = jnp.arange(amount)

    def named(sizes, turn):
        used = int((sizes > 0).sum())
        fixed = max(1, used // 4)
        moved = fixed + (places - fixed + turn * (used - fixed)) % max(1, amount - fixed)
        return jnp.zeros((amount,), jnp.int32).at[sequence[jnp.where(places < fixed, places, moved)]].set(jnp.asarray(sizes, jnp.int32))

    sizes = jnp.where(number % 4 == 0, named(crowded, number // 4), named(ordinary, number - number // 4 - 1))
    mixed = jax.random.permutation(jax.random.fold_in(own, 3), amount)
    source_of, taker = mixed[0:amount // 2 * 2:2], mixed[1:amount // 2 * 2:2]
    slack = jnp.minimum(sizes[source_of] - 1, limit - sizes[taker]) // 2
    slack = jnp.where((source_of == sequence[0]) | (taker == sequence[0]) | (sizes[taker] == 0), 0, jnp.maximum(slack, 0))
    moved = jax.random.randint(jax.random.fold_in(own, 4), (amount // 2,), 0, 1 << 20) % (slack + 1)
    sizes = sizes.at[source_of].add(-moved).at[taker].add(moved)
    labels = jnp.searchsorted(jnp.cumsum(sizes), jnp.arange(rows * top), side="right").astype(jnp.int32)
    grid = labels.reshape(top, rows).T
    grid = grid[jax.random.permutation(jax.random.fold_in(own, 1), rows)]
    turn = jax.random.randint(jax.random.fold_in(own, 2), (rows, 1), 0, top)
    return jnp.take_along_axis(grid, (jnp.arange(top)[None, :] + turn) % top, axis=1)


def load_shares(number_of, total, limit, skew, full):
    portions = [(1 << 20) // math.isqrt(rank ** skew) + 1 for rank in range(1, number_of + 1)]
    largest = limit if full else min(limit, max(-(-total // number_of), total * portions[0] // sum(portions)))
    least = 1 if total - largest >= number_of - 1 else 0
    holding, surplus = [largest] + [least] * (number_of - 1), total - largest - least * (number_of - 1)
    while surplus > 0:
        movable = [i for i in range(1, number_of) if holding[i] < largest] or [i for i in range(1, number_of) if holding[i] < limit]
        mass, budget = sum([portions[i] for i in movable]), surplus
        for i in movable:
            addition = min(limit - holding[i], max(1, budget * portions[i] // mass), surplus)
            holding[i] = holding[i] + addition
            surplus = surplus - addition
    return np.array(holding)


def gaussian(own_key, dims, scale, reach, pieces=(), held_as=jnp.bfloat16):
    values = jax.random.normal(own_key, dims, jnp.float32) * scale
    if len(pieces) > 0:
        values = block_levels(own_key, dims, pieces, -0.22, 0.18) * values
    return jnp.clip(values, min=-reach, max=reach).astype(held_as)


def setup_inputs(seed: int = 0) -> dict:
    streams_of = jax.random.split(jax.random.key(seed), 21)
    query_latent = gaussian(streams_of[0], (TOKENS_A, QUERY_RANK), 1.0, 6.0, ((0, 32),))
    key_latent = gaussian(streams_of[1], (TOKENS_A, KEY_RANK), 1.0, 6.0, ((0, 32),))
    rotary_key = draw_rotary_key(jax.random.fold_in(streams_of[20], 71), 0)
    query_gain = jnp.clip(1.0 + 0.18 * jax.random.normal(streams_of[3], (QUERY_RANK,), jnp.float32), 0.1, 1.9)
    latent_gain = jnp.clip(1.0 + 0.18 * jax.random.normal(streams_of[4], (KEY_RANK,), jnp.float32), 0.1, 1.9)
    query_content = gaussian(streams_of[5], (QUERY_RANK, HEADS * CONTENT), (QUERY_RANK // 6) ** -0.5, 0.625)
    query_rotary = gaussian(streams_of[6], (QUERY_RANK, HEADS * ROTARY), (QUERY_RANK // 6) ** -0.5, 0.625)
    key_content = gaussian(streams_of[7], (KEY_RANK, HEADS * CONTENT), KEY_RANK ** -0.5, 0.375)
    value_weight = gaussian(streams_of[8], (KEY_RANK, HEADS * VALUE), KEY_RANK ** -0.5, 0.375)
    output_weight = gaussian(streams_of[9], (HEADS * VALUE, D), (HEADS * VALUE // 16) ** -0.5, 1.0, ((0, 4),))
    expert_input = gaussian(streams_of[10], (TOKENS_B, D), 1.0, 6.0, ((0, 32),))
    norm_gain = jnp.clip(1.0 + 0.18 * jax.random.normal(streams_of[11], (D,), jnp.float32), 0.1, 1.9)
    routes_keys = jax.random.split(jax.random.fold_in(streams_of[12], 1), TOKENS_B // TOK_B)
    routes_turns = jax.random.permutation(jax.random.fold_in(streams_of[12], 3), TOKENS_B // TOK_B)
    routes = jax.vmap(lambda own, number: deal_out(jax.random.fold_in(streams_of[12], 2), own, number, TOK_B, EXPERTS, TOPK, CAPACITY, 1))(routes_keys, routes_turns).reshape((TOKENS_B, TOPK))
    route_weight = jnp.clip(0.25 + 1.75 * jax.random.uniform(streams_of[13], (TOKENS_B, TOPK), jnp.float32) ** block_levels(streams_of[13], (TOKENS_B, TOPK), ((0, 32),), -0.2, 0.2), 0.25, 2.0)
    expert_gate = gaussian(streams_of[14], (EXPERTS, D, EXPERT_WIDTH), D ** -0.5, 0.125, ((0, 8), (2, 4)))
    expert_up = gaussian(streams_of[15], (EXPERTS, D, EXPERT_WIDTH), D ** -0.5, 0.125, ((0, 8), (2, 4)))
    expert_down = gaussian(streams_of[16], (EXPERTS, EXPERT_WIDTH, D), EXPERT_WIDTH ** -0.5, 0.1875, ((0, 8), (1, 4)))
    shared_gate = gaussian(streams_of[17], (D, SHARED_WIDTH), D ** -0.5, 0.125, ((1, 4),))
    shared_up = gaussian(streams_of[18], (D, SHARED_WIDTH), D ** -0.5, 0.125, ((1, 4),))
    shared_down = gaussian(streams_of[19], (SHARED_WIDTH, D), SHARED_WIDTH ** -0.5, 0.1875, ((0, 4),))
    return {"query_latent": query_latent, "key_latent": key_latent, "rotary_key": rotary_key, "query_gain": query_gain, "latent_gain": latent_gain, "query_content": query_content, "query_rotary": query_rotary, "key_content": key_content, "value_weight": value_weight, "output_weight": output_weight, "expert_input": expert_input, "norm_gain": norm_gain, "routes": routes, "route_weight": route_weight, "expert_gate": expert_gate, "expert_up": expert_up, "expert_down": expert_down, "shared_gate": shared_gate, "shared_up": shared_up, "shared_down": shared_down}


norm_eps = 1e-06
rope_base = 10000.0

def rms_rows(entries, gain_row):
    widened = entries.astype(jnp.float32)
    return widened * lax.rsqrt(lax.optimization_barrier(jnp.mean(widened * widened, -1, keepdims=True)) + norm_eps) * gain_row.astype(jnp.float32)

def turn_pairs(entries, positions):
    width_full = entries.shape[-1]
    frequency = rope_base ** (-jnp.arange(width_full // 2, dtype=jnp.float32) * 2.0 / width_full)
    angles = positions.astype(jnp.float32)[:, None] * frequency[None, :]
    cosine = jnp.cos(angles)[:, None, :]
    sine_part = jnp.sin(angles)[:, None, :]
    even_part = entries[..., 0::2]
    odd_part = entries[..., 1::2]
    joined = jnp.stack([even_part * cosine - odd_part * sine_part, even_part * sine_part + odd_part * cosine], -1)
    return joined.reshape(entries.shape)

def feed_forward(row_block, gate_weight, up_weight, down_weight, groups):
    gated = jnp.dot(row_block, gate_weight, preferred_element_type=jnp.float32)
    lifted = jnp.dot(row_block, up_weight, preferred_element_type=jnp.float32)
    hidden = (jax.nn.silu(gated) * lifted).astype(jnp.bfloat16)
    group_width = hidden.shape[1] // groups
    running = jnp.zeros((row_block.shape[0], down_weight.shape[1]), jnp.float32)
    for group_index in range(groups):
        product = jnp.dot(hidden[:, group_index * group_width:(group_index + 1) * group_width], down_weight[group_index * group_width:(group_index + 1) * group_width], preferred_element_type=jnp.float32)
        running = running + lax.optimization_barrier(product.astype(jnp.bfloat16)).astype(jnp.float32)
    return running

def attend_queries(query_blocks, key_wide, turn_wide, value_wide):
    query_part, query_turn = query_blocks
    score_scale = (CONTENT + ROTARY) ** (-0.5)
    scores = jnp.einsum('qhc,khc->qhk', query_part.astype(jnp.float32), key_wide)
    scores = scores + jnp.einsum('qhr,kr->qhk', query_turn.astype(jnp.float32), turn_wide)
    scores = scores * score_scale
    weights = jnp.exp(scores - lax.optimization_barrier(jnp.max(scores, -1, keepdims=True)))
    denominator = lax.optimization_barrier(jnp.sum(weights, -1))
    rounded = lax.optimization_barrier(weights.astype(jnp.bfloat16)).astype(jnp.float32)
    numerator = jnp.einsum('qhk,khv->qhv', rounded, value_wide)
    return (numerator / denominator[..., None]).astype(jnp.bfloat16)

def block_slots(route_block):
    flat_routes = route_block.reshape(-1)
    marks = (flat_routes[:, None] == jnp.arange(EXPERTS, dtype=jnp.int32)[None, :]).astype(jnp.int32)
    return lax.optimization_barrier(jnp.sum((jnp.cumsum(marks, 0) - marks) * marks, 1)).reshape(route_block.shape)

def reference(query_latent, key_latent, rotary_key, query_gain, latent_gain, query_content, query_rotary, key_content, value_weight, output_weight, expert_input, norm_gain, routes, route_weight, expert_gate, expert_up, expert_down, shared_gate, shared_up, shared_down):
    row_count = query_latent.shape[0]
    positions = jnp.arange(row_count, dtype=jnp.int32)
    query_normed = rms_rows(query_latent, query_gain).astype(jnp.bfloat16)
    latent_normed = rms_rows(key_latent, latent_gain).astype(jnp.bfloat16)
    query_part = jnp.dot(query_normed, query_content, preferred_element_type=jnp.float32).astype(jnp.bfloat16).reshape(row_count, HEADS, CONTENT)
    query_turn = turn_pairs(jnp.dot(query_normed, query_rotary, preferred_element_type=jnp.float32).reshape(row_count, HEADS, ROTARY), positions).astype(jnp.bfloat16)
    key_turn = turn_pairs(rotary_key.astype(jnp.float32)[:, None, :], positions)[:, 0, :].astype(jnp.bfloat16)
    key_part = jnp.dot(latent_normed, key_content, preferred_element_type=jnp.float32).astype(jnp.bfloat16).reshape(row_count, HEADS, CONTENT)
    value_rows = jnp.dot(latent_normed, value_weight, preferred_element_type=jnp.float32).astype(jnp.bfloat16).reshape(row_count, HEADS, VALUE)
    query_block = math.gcd(row_count, 256)
    block_count = row_count // query_block
    query_blocks = (query_part.reshape(block_count, query_block, HEADS, CONTENT), query_turn.reshape(block_count, query_block, HEADS, ROTARY))
    attended = lax.map(partial(attend_queries, key_wide=key_part.astype(jnp.float32), turn_wide=key_turn.astype(jnp.float32), value_wide=value_rows.astype(jnp.float32)), query_blocks)
    attended = attended.reshape(row_count, HEADS * VALUE)
    group_width = HEADS * VALUE // N_TP
    mixed = jnp.zeros((row_count, output_weight.shape[1]), jnp.float32)
    for group_index in range(N_TP):
        product = jnp.dot(attended[:, group_index * group_width:(group_index + 1) * group_width], output_weight[group_index * group_width:(group_index + 1) * group_width], preferred_element_type=jnp.float32)
        mixed = mixed + lax.optimization_barrier(product.astype(jnp.bfloat16)).astype(jnp.float32)
    mixer_out = mixed.astype(jnp.bfloat16)
    token_count = expert_input.shape[0]
    device_count = N_EP * N_TP
    per_device = token_count // device_count
    expert_normed = rms_rows(expert_input, norm_gain).astype(jnp.bfloat16)
    slots = jax.vmap(block_slots)(routes.reshape(device_count, per_device, TOPK)).reshape(token_count, TOPK)
    device_of = (jnp.arange(token_count, dtype=jnp.int32) // per_device).astype(jnp.int32)
    token_index = jnp.broadcast_to(jnp.arange(token_count, dtype=jnp.int32)[:, None], (token_count, TOPK))
    table = jnp.full((EXPERTS, device_count, CAPACITY), token_count, jnp.int32)
    table = table.at[routes, jnp.broadcast_to(device_of[:, None], (token_count, TOPK)), slots].set(token_index)
    padded = jnp.concatenate([expert_normed, jnp.zeros((1, expert_normed.shape[1]), jnp.bfloat16)], 0)

    def one_expert(expert_args):
        table_row, gate_weight, up_weight, down_weight = expert_args
        row_block = padded[table_row.reshape(-1)]
        return feed_forward(row_block, gate_weight, up_weight, down_weight, N_TP).astype(jnp.bfloat16)
    results = lax.map(one_expert, (table, expert_gate, expert_up, expert_down))
    flat_index = (routes * (device_count * CAPACITY) + device_of[:, None] * CAPACITY + slots).astype(jnp.int32)
    picked = results.reshape(-1, results.shape[-1])[flat_index.reshape(-1)].reshape(token_count, TOPK, -1)
    routed = lax.optimization_barrier(jnp.sum(route_weight.astype(jnp.float32)[..., None] * picked.astype(jnp.float32), 1))
    shared_sum = feed_forward(expert_normed, shared_gate, shared_up, shared_down, N_TP)
    expert_out = (routed + shared_sum).astype(jnp.bfloat16)
    return (mixer_out, expert_out)
```

```python
import math

import jax
import jax.numpy as jnp
from jax import lax
from jax.experimental import pallas as pl
from jax.experimental.pallas import tpu as pltpu
from jax.sharding import PartitionSpec as P

HEADS = 8
CONTENT = 64
ROTARY = 32
VALUE = 64


norm_eps = 1e-06
rope_base = 10000.0


def rms_rows(entries, gain_row):
    widened = entries.astype(jnp.float32)
    return widened * lax.rsqrt(jnp.mean(widened * widened, -1, keepdims=True) + norm_eps) * gain_row


def turn_pairs(entries, positions):
    width_full = entries.shape[-1]
    frequency = rope_base ** (-jnp.arange(width_full // 2, dtype=jnp.float32) * 2.0 / width_full)
    angles = positions.astype(jnp.float32)[:, None] * frequency[None, :]
    cosine = jnp.cos(angles)[:, None, :]
    sine_part = jnp.sin(angles)[:, None, :]
    even_part = entries[..., 0::2]
    odd_part = entries[..., 1::2]
    joined = jnp.stack(
        [even_part * cosine - odd_part * sine_part, even_part * sine_part + odd_part * cosine], -1
    )
    return joined.reshape(entries.shape)


def absorb_block(carried, query_part, query_turn, key_part, key_turn, value_rows, score_scale):
    running_peak, running_total, summed = carried
    scores = jnp.einsum("qhc,khc->qhk", query_part, key_part, preferred_element_type=jnp.float32)
    scores = scores + jnp.einsum(
        "qhr,kr->qhk", query_turn, key_turn, preferred_element_type=jnp.float32
    )
    scores = scores * score_scale
    new_peak = jnp.maximum(running_peak, jnp.max(scores, -1))
    factor = jnp.exp(running_peak - new_peak)
    weights = jnp.exp(scores - new_peak[..., None])
    running_total = running_total * factor + jnp.sum(weights, -1)
    summed = summed * factor[..., None] + jnp.einsum(
        "qhk,khv->qhv", weights.astype(jnp.bfloat16), value_rows, preferred_element_type=jnp.float32
    )
    return (new_peak, running_total, summed)


def absorb_piece(carried, query_part, query_turn, key_part, key_turn, value_rows, score_scale):
    row_count = key_part.shape[0]
    key_block = math.gcd(row_count, 2048)
    if key_block == row_count:
        return absorb_block(
            carried, query_part, query_turn, key_part, key_turn, value_rows, score_scale
        )
    block_count = row_count // key_block

    def advance(state, pieces):
        return (
            absorb_block(
                state, query_part, query_turn, pieces[0], pieces[1], pieces[2], score_scale
            ),
            None,
        )

    stacked = (
        key_part.reshape((block_count, key_block) + key_part.shape[1:]),
        key_turn.reshape(block_count, key_block, key_turn.shape[1]),
        value_rows.reshape((block_count, key_block) + value_rows.shape[1:]),
    )
    carried, ignored = lax.scan(advance, carried, stacked)
    return carried


def expand_keys(latent_rows, key_columns, value_columns, head_local):
    row_count = latent_rows.shape[0]
    key_part = (
        jnp.dot(latent_rows, key_columns, preferred_element_type=jnp.float32)
        .astype(jnp.bfloat16)
        .reshape(row_count, head_local, CONTENT)
    )
    value_rows = (
        jnp.dot(latent_rows, value_columns, preferred_element_type=jnp.float32)
        .astype(jnp.bfloat16)
        .reshape(row_count, head_local, VALUE)
    )
    return (key_part, value_rows)


def expert_terms(row_block, gate_weight, up_weight, down_weight):
    gated = jnp.einsum("secd,edf->secf", row_block, gate_weight, preferred_element_type=jnp.float32)
    lifted = jnp.einsum("secd,edf->secf", row_block, up_weight, preferred_element_type=jnp.float32)
    hidden = (jax.nn.silu(gated) * lifted).astype(jnp.bfloat16)
    return jnp.einsum("secf,efd->secd", hidden, down_weight, preferred_element_type=jnp.float32)


def shared_terms(row_block, gate_weight, up_weight, down_weight):
    gated = jnp.dot(row_block, gate_weight, preferred_element_type=jnp.float32)
    lifted = jnp.dot(row_block, up_weight, preferred_element_type=jnp.float32)
    hidden = (jax.nn.silu(gated) * lifted).astype(jnp.bfloat16)
    return jnp.dot(hidden, down_weight, preferred_element_type=jnp.float32)


def shards_plain(
    query_latent,
    key_latent,
    rotary_key,
    query_gain,
    latent_gain,
    query_content,
    query_rotary,
    key_content,
    value_weight,
    output_weight,
    expert_input,
    norm_gain,
    routes,
    route_weight,
    expert_gate,
    expert_up,
    expert_down,
    shared_gate,
    shared_up,
    shared_down,
):
    group_size = lax.axis_size("tp")
    expert_groups = lax.axis_size("ep")
    own_rows = query_latent.shape[0]
    head_local = HEADS // group_size
    head_index = lax.axis_index("tp")
    group_rows_count = own_rows * group_size
    group_start = lax.axis_index("ep") * group_rows_count
    own_start = group_start + head_index * own_rows
    score_scale = (CONTENT + ROTARY) ** (-0.5)
    query_normed = rms_rows(query_latent, query_gain).astype(jnp.bfloat16)
    latent_normed = rms_rows(key_latent, latent_gain).astype(jnp.bfloat16)
    own_positions = own_start + jnp.arange(own_rows, dtype=jnp.int32)
    key_turned = turn_pairs(rotary_key.astype(jnp.float32)[:, None, :], own_positions)[
        :, 0, :
    ].astype(jnp.bfloat16)
    token_rows = expert_input.shape[0]
    picks = routes.shape[1]
    local_experts = expert_gate.shape[0]
    expert_total = local_experts * expert_groups
    capacity = 2 * token_rows * picks // expert_total
    slot_total = expert_total * capacity
    model_width = expert_input.shape[1]
    expert_normed = rms_rows(expert_input, norm_gain).astype(jnp.bfloat16)
    flat_routes = routes.reshape(-1)
    marks = (flat_routes[:, None] == jnp.arange(expert_total, dtype=jnp.int32)[None, :]).astype(
        jnp.int32
    )
    ranks = jnp.sum((jnp.cumsum(marks, 0) - marks) * marks, 1)
    targets = flat_routes * capacity + ranks
    picker = (jnp.arange(slot_total, dtype=jnp.int32)[:, None] == targets[None, :]).astype(
        jnp.int32
    )
    picker = jnp.sum(picker.reshape(slot_total, token_rows, picks), 2).astype(jnp.bfloat16)
    outgoing = jnp.dot(picker, expert_normed, preferred_element_type=jnp.float32).astype(
        jnp.bfloat16
    )
    outgoing = outgoing.reshape(expert_groups, local_experts, capacity, model_width)
    received = lax.all_to_all(outgoing, "ep", split_axis=0, concat_axis=0, tiled=True)
    group_query, group_latent, group_turn, gathered_rows, gathered_tokens = (
        lax.all_gather(query_normed, "tp", axis=0, tiled=True),
        lax.all_gather(latent_normed, "tp", axis=0, tiled=True),
        lax.all_gather(key_turned, "tp", axis=0, tiled=True),
        lax.all_gather(received, "tp", axis=0, tiled=True),
        lax.all_gather(expert_normed, "tp", axis=0, tiled=True),
    )
    positions = group_start + jnp.arange(group_rows_count, dtype=jnp.int32)
    content_columns = lax.dynamic_slice_in_dim(
        query_content, head_index * head_local * CONTENT, head_local * CONTENT, 1
    )
    rotary_columns = lax.dynamic_slice_in_dim(
        query_rotary, head_index * head_local * ROTARY, head_local * ROTARY, 1
    )
    query_part = (
        jnp.dot(group_query, content_columns, preferred_element_type=jnp.float32)
        .astype(jnp.bfloat16)
        .reshape(group_rows_count, head_local, CONTENT)
    )
    query_turn = turn_pairs(
        jnp.dot(group_query, rotary_columns, preferred_element_type=jnp.float32).reshape(
            group_rows_count, head_local, ROTARY
        ),
        positions,
    ).astype(jnp.bfloat16)
    key_columns = lax.dynamic_slice_in_dim(
        key_content, head_index * head_local * CONTENT, head_local * CONTENT, 1
    )
    value_columns = lax.dynamic_slice_in_dim(
        value_weight, head_index * head_local * VALUE, head_local * VALUE, 1
    )
    carry_start = (
        jnp.full((group_rows_count, head_local), -jnp.inf, jnp.float32),
        jnp.zeros((group_rows_count, head_local), jnp.float32),
        jnp.zeros((group_rows_count, head_local, VALUE), jnp.float32),
    )
    key_part, value_rows = expand_keys(
        lax.all_gather(group_latent, "ep", axis=0, tiled=True),
        key_columns,
        value_columns,
        head_local,
    )
    running_peak, running_total, summed = absorb_piece(
        carry_start,
        query_part,
        query_turn,
        key_part,
        lax.all_gather(group_turn, "ep", axis=0, tiled=True),
        value_rows,
        score_scale,
    )
    attended = (
        (summed / running_total[..., None])
        .astype(jnp.bfloat16)
        .reshape(group_rows_count, head_local * VALUE)
    )
    routed_term = expert_terms(gathered_rows, expert_gate, expert_up, expert_down)
    shared_term = shared_terms(gathered_tokens, shared_gate, shared_up, shared_down)
    mixer_term = jnp.dot(attended, output_weight, preferred_element_type=jnp.float32)
    mixer_sum, routed_sum, shared_sum = (
        lax.psum_scatter(
            mixer_term.astype(jnp.bfloat16), "tp", scatter_dimension=0, tiled=True
        ).astype(jnp.float32),
        lax.psum_scatter(
            routed_term.astype(jnp.bfloat16), "tp", scatter_dimension=0, tiled=True
        ).astype(jnp.float32),
        lax.psum_scatter(
            shared_term.astype(jnp.bfloat16), "tp", scatter_dimension=0, tiled=True
        ).astype(jnp.float32),
    )
    mixer_out = mixer_sum.astype(jnp.bfloat16)
    returned = lax.all_to_all(
        routed_sum.astype(jnp.bfloat16), "ep", split_axis=0, concat_axis=0, tiled=True
    )
    returned = returned.reshape(slot_total, model_width)
    picked = jnp.take(returned, targets, axis=0).reshape(token_rows, picks, model_width)
    combined = jnp.sum(route_weight[..., None] * picked.astype(jnp.float32), 1) + shared_sum
    expert_out = combined.astype(jnp.bfloat16)
    return (mixer_out, expert_out)


MESH = pl.DeviceIdType.MESH
VMEM_LIMIT = 60 * 1024 * 1024
NEAR = 4


def fits_kernel(ep_count, slot_rows):
    power = ep_count & (ep_count - 1) == 0
    return power and ep_count > NEAR and NEAR * slot_rows % 128 == 0


def flip(place, bits):
    flipped = place
    bit = 1
    while bit <= bits:
        if bits & bit:
            flipped = flipped + bit * (1 - 2 * (place // bit % 2))
        bit *= 2
    return flipped


def greet(ep_count, me, head_index):
    barrier = pltpu.get_barrier_semaphore()
    for step in range(1, ep_count):
        pl.semaphore_signal(
            barrier, inc=1, device_id=(flip(me, step), head_index), device_id_type=MESH
        )
    row, core = head_index // 2, head_index % 2
    for other in ((1 - row) * 2 + core, row * 2 + 1 - core):
        pl.semaphore_signal(barrier, inc=1, device_id=(me, other), device_id_type=MESH)
    pl.semaphore_wait(barrier, ep_count + 1)


def gated_rows(rows, gate_weight, up_weight):
    gated = jnp.dot(rows, gate_weight, preferred_element_type=jnp.float32)
    lifted = jnp.dot(rows, up_weight, preferred_element_type=jnp.float32)
    return (gated / (1.0 + jnp.exp(-gated)) * lifted).astype(jnp.bfloat16)


def wide(entries):
    return entries.astype(jnp.float32)


def narrow(entries):
    return entries.astype(jnp.bfloat16)


def choose_slots(routes, weights, expert_total, capacity, first_slot, slot_count):
    own_rows = routes.shape[0]
    expert_lane = lax.broadcasted_iota(jnp.int32, (own_rows, expert_total), 1)
    named = [
        jnp.where(routes[:, pick : pick + 1] == expert_lane, 1.0, 0.0)
        for pick in range(routes.shape[1])
    ]
    earlier = narrow(
        jnp.where(
            lax.broadcasted_iota(jnp.int32, (own_rows, own_rows), 0)
            > lax.broadcasted_iota(jnp.int32, (own_rows, own_rows), 1),
            1.0,
            0.0,
        )
    )
    ahead = jnp.dot(earlier, narrow(sum(named)), preferred_element_type=jnp.float32)
    slot_lane = lax.broadcasted_iota(jnp.int32, (own_rows, slot_count), 1) + first_slot
    picker = jnp.zeros(slot_lane.shape, jnp.float32)
    weight = jnp.zeros(slot_lane.shape, jnp.float32)
    for pick, marks in enumerate(named):
        rank = jnp.sum(ahead * marks, 1, keepdims=True).astype(jnp.int32)
        chosen = slot_lane == routes[:, pick : pick + 1] * capacity + rank
        picker = jnp.where(chosen, 1.0, picker)
        weight = jnp.where(chosen, weights[:, pick : pick + 1], weight)
    return narrow(picker.T), weight


def store_split(target, weight):
    own_rows = weight.shape[0]
    high = narrow(weight)
    rest = weight - wide(high)
    middle = narrow(rest)
    target[:own_rows] = high
    target[own_rows : 2 * own_rows] = middle
    target[2 * own_rows :] = narrow(rest - wide(middle))


def weighted_rows(split_weight, entries):
    picked = jnp.dot(split_weight, entries, preferred_element_type=jnp.float32)
    own_rows = picked.shape[0] // 3
    return picked[:own_rows] + picked[own_rows : 2 * own_rows] + picked[2 * own_rows :]


def block_kernel(
    ep_count,
    capacity,
    query_latent_ref,
    key_latent_ref,
    rotary_key_ref,
    query_gain_ref,
    latent_gain_ref,
    expert_input_ref,
    norm_gain_ref,
    routes_ref,
    route_weight_ref,
    cosine_ref,
    sine_ref,
    query_content_hbm,
    query_rotary_hbm,
    key_content_hbm,
    value_weight_hbm,
    output_weight_hbm,
    gate_hbm,
    up_hbm,
    down_hbm,
    shared_gate_hbm,
    shared_up_hbm,
    shared_down_hbm,
    both_out,
    slots_ref,
    peer_slots_ref,
    query_columns_ref,
    latent_columns_ref,
    output_weight_ref,
    weight_ref,
    peer_weight_ref,
    rows,
    latents,
    tokens,
    queries,
    gate_ref,
    up_ref,
    down_ref,
    shared_gate_ref,
    shared_up_ref,
    shared_down_ref,
    keys,
    values,
    query_wide,
    attended,
    part,
    half_rows,
    far_rows,
    returned,
    returned_peer,
    mixed,
    half_mixed,
    far_mixed,
    shared,
    half_shared,
    far_shared,
    info_ref,
    peer_info_ref,
    own_sum,
    own_stats,
    sent_sum,
    far_sum,
    ep_send,
    ep_recv,
    y_send,
    y_recv,
    core_send,
    core_recv,
    cross_send,
    cross_recv,
    peer_send,
    peer_recv,
    back_send,
    back_recv,
    far_send,
    far_recv,
    half_send,
    half_recv,
    side_send,
    side_recv,
    own_sem,
    weight_sem,
):
    me = lax.axis_index("ep")
    head_index = lax.axis_index("tp")
    row, core = head_index // 2, head_index % 2
    y_peer = (me, (1 - row) * 2 + core)
    core_peer = (me, row * 2 + 1 - core)
    local_experts = gate_ref.shape[0]
    width = rows.shape[-1]
    own_rows = tokens.shape[2]
    slot_rows = rows.shape[3]
    group_rows = attended.shape[0]
    picks = routes_ref.shape[0]
    stripe = math.gcd(width, 512)
    far_steps = range(NEAR, ep_count)
    near_place = me % NEAR

    def peer(step):
        return (flip(me, step), head_index)

    def remote(source, target, send_sem, recv_sem, device):
        return pltpu.make_async_remote_copy(
            src_ref=source,
            dst_ref=target,
            send_sem=send_sem,
            recv_sem=recv_sem,
            device_id=device,
            device_id_type=MESH,
        )

    head_lanes = attended.shape[1]
    heads = head_lanes // VALUE
    fetch_list = []
    for side in range(2):
        side_index = (row if side == 0 else 1 - row) * 2 + core
        columns = pl.ds(pl.multiple_of(side_index * head_lanes, head_lanes), head_lanes)
        turn_columns = pl.ds(pl.multiple_of(side_index * heads * ROTARY // 128 * 128, 128), 128)
        fetch_list += [
            (query_content_hbm.at[:, columns], query_columns_ref.at[side, :, :head_lanes]),
            (query_rotary_hbm.at[:, turn_columns], query_columns_ref.at[side, :, head_lanes:]),
            (key_content_hbm.at[:, columns], latent_columns_ref.at[side, :, :head_lanes]),
            (value_weight_hbm.at[:, columns], latent_columns_ref.at[side, :, head_lanes:]),
        ]
    fetch_list += [
        (output_weight_hbm, output_weight_ref),
        (shared_gate_hbm, shared_gate_ref),
        (shared_up_hbm, shared_up_ref),
        (shared_down_hbm, shared_down_ref),
        (gate_hbm, gate_ref),
        (up_hbm, up_ref),
        (down_hbm, down_ref),
    ]
    fetches = [
        pltpu.make_async_copy(source, target, weight_sem.at[place])
        for place, (source, target) in enumerate(fetch_list)
    ]
    for fetch in fetches:
        fetch.start()

    def turn(entries, cosine, sine):
        lane = lax.broadcasted_iota(jnp.int32, entries.shape, 1)
        crossed = jnp.where(
            lane % 2 == 0, -pltpu.roll(entries, 127, 1), pltpu.roll(entries, 1, 1)
        )
        return narrow(entries * cosine + crossed * sine)

    rank_width = key_latent_ref.shape[1]
    latents[core, 0, :, :rank_width] = narrow(rms_rows(key_latent_ref[...], latent_gain_ref[...]))
    repeats = narrow(
        jnp.where(
            lax.broadcasted_iota(jnp.int32, (ROTARY, 128), 0)
            == lax.broadcasted_iota(jnp.int32, (ROTARY, 128), 1) % ROTARY,
            1.0,
            0.0,
        )
    )
    own_span = pl.ds(pl.multiple_of(head_index * own_rows, own_rows), own_rows)
    latents[core, 0, :, rank_width:] = turn(
        lax.dot_general(
            rotary_key_ref[...],
            repeats,
            (((0,), (0,)), ((), ())),
            preferred_element_type=jnp.float32,
        ),
        cosine_ref[own_span, :],
        sine_ref[own_span, :],
    )
    queries[row, core] = narrow(rms_rows(query_latent_ref[...], query_gain_ref[...]))
    info_ref[...] = jnp.zeros(info_ref.shape, jnp.float32)
    info_ref[:picks, :own_rows] = routes_ref[...].astype(jnp.float32)
    info_ref[picks : 2 * picks, :own_rows] = route_weight_ref[...]
    greet(ep_count, me, head_index)

    def latent_ep(step):
        if step % 2 == 0:
            return remote(
                latents.at[core, 0],
                latents.at[core, step],
                ep_send.at[1, step],
                ep_recv.at[1, step],
                peer(step),
            )
        return remote(
            latents.at[core, step - 1],
            latents.at[core, step],
            ep_send.at[1, step],
            ep_recv.at[1, step],
            peer(1),
        )

    def latent_core(step):
        return remote(
            latents.at[core, step],
            latents.at[core, step],
            core_send.at[1, step],
            core_recv.at[1, step],
            core_peer,
        )

    def slots_ep(step):
        return remote(
            slots_ref.at[flip(me, step)],
            rows.at[row, core, step],
            ep_send.at[0, step],
            ep_recv.at[0, step],
            peer(step),
        )

    def peer_slots_ep(step):
        return remote(
            peer_slots_ref.at[flip(near_place, step)],
            rows.at[1 - row, core, step],
            peer_send.at[0, step],
            peer_recv.at[0, step],
            peer(step),
        )

    routes_of = {
        "y": (row, y_send, y_recv, y_peer),
        "core": (row, core_send, core_recv, core_peer),
        "cross": (1 - row, cross_send, cross_recv, core_peer),
    }

    def moved_rows(step, route):
        origin_row, send_sem, recv_sem, device = routes_of[route]
        block = rows.at[origin_row, core, step]
        return remote(block, block, send_sem.at[0, step], recv_sem.at[0, step], device)

    def moved(buffer, place, route):
        origin_row, send_sem, recv_sem, device = routes_of[route]
        block = buffer.at[origin_row, core]
        return remote(
            block, block, send_sem.at[place, ep_count], recv_sem.at[place, ep_count], device
        )

    info_y = remote(
        info_ref, peer_info_ref, y_send.at[0, 0], y_recv.at[0, 0], y_peer
    )
    for step in range(1, ep_count):
        if step == 1 or step % 2 == 0:
            latent_ep(step).start()
    latent_core(0).start()
    info_y.start()
    for route in ("y", "core"):
        moved(queries, 1, route).start()
    expert_normed = narrow(rms_rows(expert_input_ref[...], norm_gain_ref[...]))
    tokens[row, core] = expert_normed
    for route in ("y", "core"):
        moved(tokens, 0, route).start()
    expert_total = local_experts * ep_count
    picker, weight = choose_slots(
        routes_ref[...].T, route_weight_ref[...].T, expert_total, capacity, 0, ep_count * slot_rows
    )
    store_split(weight_ref, weight)

    def fill(target, chooser, origin_row):
        for start in range(0, width, stripe):
            target[:, :, start : start + stripe] = narrow(
                jnp.dot(
                    chooser,
                    tokens[origin_row, core, :, start : start + stripe],
                    preferred_element_type=jnp.float32,
                )
            ).reshape(target.shape[0], slot_rows, stripe)

    fill(slots_ref, picker, row)
    for step in range(1, ep_count):
        slots_ep(step).start()
    own_slots = pltpu.make_async_copy(slots_ref.at[me], rows.at[row, core, 0], own_sem.at[0])
    own_slots.start()
    own_slots.wait()
    moved_rows(0, "core").start()

    def pass_latents(steps):
        for step in steps:
            latent_ep(step).wait_recv()
            if step % 2 == 0:
                latent_ep(step + 1).start()
            latent_core(step).start()

    pass_latents(range(2, ep_count, 2))
    moved(queries, 1, "y").wait_recv()
    moved(queries, 1, "cross").start()
    info_y.wait_recv()
    peer_picker, peer_weight = choose_slots(
        peer_info_ref[:picks, :own_rows].T.astype(jnp.int32),
        peer_info_ref[picks : 2 * picks, :own_rows].T,
        expert_total,
        capacity,
        me // NEAR * NEAR * slot_rows,
        NEAR * slot_rows,
    )
    store_split(peer_weight_ref, peer_weight)
    moved(tokens, 0, "y").wait_recv()
    moved(tokens, 0, "cross").start()
    fill(peer_slots_ref, peer_picker, 1 - row)
    for step in range(1, NEAR):
        peer_slots_ep(step).start()
    peer_own = pltpu.make_async_copy(
        peer_slots_ref.at[near_place], rows.at[1 - row, core, 0], own_sem.at[1]
    )
    peer_own.start()
    peer_own.wait()
    moved_rows(0, "cross").start()
    pass_latents(range(1, ep_count, 2))
    for route in ("core", "cross"):
        moved(queries, 1, route).wait_recv()
    for step in range(ep_count):
        latent_core(step).wait_recv()

    def project():
        for fetch in fetches[:8]:
            fetch.wait()
        query_rows = queries[...].reshape(group_rows, queries.shape[-1])
        for side in range(2):
            projected = jnp.dot(
                query_rows, query_columns_ref[side], preferred_element_type=jnp.float32
            )
            query_wide[side, :, :head_lanes] = narrow(projected[:, :head_lanes])
            query_wide[side, :, head_lanes:] = turn(
                projected[:, head_lanes:], cosine_ref[...], sine_ref[...]
            )
        for block in range(2):
            packed = latents[block].reshape(ep_count * own_rows, latents.shape[-1])
            span = slice(block * ep_count * own_rows, (block + 1) * ep_count * own_rows)
            for side in range(2):
                expanded = narrow(
                    jnp.dot(
                        packed[:, :rank_width],
                        latent_columns_ref[side],
                        preferred_element_type=jnp.float32,
                    )
                )
                keys[side, span, :head_lanes] = expanded[:, :head_lanes]
                keys[side, span, head_lanes:] = packed[:, rank_width:]
                values[side, span, :] = expanded[:, head_lanes:]

    block_rows = group_rows // 2

    def attend(side, block):
        span = slice(block * block_rows, (block + 1) * block_rows)
        query_block = query_wide[side, span, :]
        lane = lax.broadcasted_iota(jnp.int32, query_block.shape, 1)
        lane_head = jnp.where(
            lane < head_lanes,
            lane // CONTENT,
            (lane - head_lanes) // ROTARY - core * heads % (128 // ROTARY),
        )
        out_lane = lax.broadcasted_iota(jnp.int32, (block_rows, head_lanes), 1)
        result = jnp.zeros((block_rows, head_lanes), jnp.float32)
        stats = jnp.zeros((block_rows, head_lanes), jnp.float32)
        for head in range(heads):
            chosen = jnp.where(lane_head == head, query_block, jnp.zeros_like(query_block))
            scores = lax.dot_general(
                chosen, keys[side], (((1,), (1,)), ((), ())), preferred_element_type=jnp.float32
            ) * ((CONTENT + ROTARY) ** (-0.5))
            peak = jnp.max(scores, -1, keepdims=True)
            weights = jnp.exp(scores - peak)
            total = jnp.sum(weights, -1, keepdims=True)
            summed = jnp.dot(narrow(weights), values[side], preferred_element_type=jnp.float32)
            result = jnp.where(out_lane // VALUE == head, summed, result)
            stats = jnp.where(out_lane == 2 * head, peak, stats)
            stats = jnp.where(out_lane == 2 * head + 1, total, stats)
        if side == 0:
            own_sum[span, :] = result
            own_stats[span, :] = stats
        else:
            sent_sum[span, :] = result
            sent_sum[group_rows + 8 * block : group_rows + 8 * block + 8, :] = stats.T[:8]

    sum_y = remote(sent_sum, far_sum, y_send.at[1, 0], y_recv.at[1, 0], y_peer)

    def merge():
        sum_y.wait_recv()
        out_lane = lax.broadcasted_iota(jnp.int32, (block_rows, head_lanes), 1)
        for block in range(2):
            span = slice(block * block_rows, (block + 1) * block_rows)
            here = own_stats[span, :]
            there = far_sum[group_rows + 8 * block : group_rows + 8 * block + 8, :].T
            result = jnp.zeros((block_rows, head_lanes), jnp.float32)
            for head in range(heads):
                peak_here, total_here = here[:, 2 * head : 2 * head + 1], here[:, 2 * head + 1 : 2 * head + 2]
                peak_there, total_there = there[:, 2 * head : 2 * head + 1], there[:, 2 * head + 1 : 2 * head + 2]
                peak = jnp.maximum(peak_here, peak_there)
                factor_here = jnp.exp(peak_here - peak)
                factor_there = jnp.exp(peak_there - peak)
                total = total_here * factor_here + total_there * factor_there
                summed = own_sum[span, :] * factor_here + far_sum[span, :] * factor_there
                result = jnp.where(out_lane // VALUE == head, summed / total, result)
            attended[span, :] = narrow(result)

    def mix():
        fetches[8].wait()
        for start in range(0, width, stripe):
            product = narrow(
                jnp.dot(
                    attended[...],
                    output_weight_ref[:, start : start + stripe],
                    preferred_element_type=jnp.float32,
                )
            )
            mixed[:, :, :, start : start + stripe] = product.reshape(2, 2, own_rows, stripe)

    def share():
        for fetch in fetches[9:12]:
            fetch.wait()
        for route in ("core", "cross"):
            moved(tokens, 0, route).wait_recv()
        hidden = gated_rows(
            tokens[...].reshape(group_rows, width), shared_gate_ref[...], shared_up_ref[...]
        )
        for start in range(0, width, stripe):
            product = narrow(
                jnp.dot(
                    hidden,
                    shared_down_ref[:, start : start + stripe],
                    preferred_element_type=jnp.float32,
                )
            )
            shared[:, :, :, start : start + stripe] = product.reshape(2, 2, own_rows, stripe)

    shared_half = remote(
        shared.at[:, 1 - core], half_shared, side_send.at[0], side_recv.at[0], core_peer
    )
    mixed_half = remote(
        mixed.at[:, 1 - core], half_mixed, side_send.at[1], side_recv.at[1], core_peer
    )
    shared_y = remote(
        shared.at[1 - row, core], far_shared, side_send.at[2], side_recv.at[2], y_peer
    )
    mixed_y = remote(mixed.at[1 - row, core], far_mixed, side_send.at[3], side_recv.at[3], y_peer)

    def mixed_far():
        mixed_half.wait_recv()
        mixed[1 - row, core] = narrow(wide(mixed[1 - row, core]) + wide(half_mixed[1 - row]))
        mixed_y.start()

    def arrive(step):
        slots_ep(step).wait_recv()
        if step >= NEAR:
            moved_rows(step, "y").start()
        moved_rows(step, "core").start()

    def arrive_peer(step):
        if step >= NEAR:
            moved_rows(step, "y").wait_recv()
        else:
            peer_slots_ep(step).wait_recv()
        moved_rows(step, "cross").start()

    project()
    arrive(1)
    attend(1, 0)
    arrive(2)
    arrive(3)
    attend(1, 1)
    sum_y.start()
    arrive(4)
    attend(0, 0)
    arrive(5)
    arrive_peer(1)
    arrive_peer(4)
    attend(0, 1)
    arrive(6)
    arrive_peer(5)
    merge()
    mix()
    mixed_half.start()
    for step in range(7, ep_count):
        arrive(step)
    arrive_peer(2)
    arrive_peer(3)
    share()
    shared_half.start()
    for step in range(6, ep_count):
        arrive_peer(step)
    mixed_far()

    for fetch in fetches[12:]:
        fetch.wait()

    def spans(expert):
        return slice(expert * capacity, (expert + 1) * capacity)

    def compute(first, last, expert):
        span = spans(expert)
        block = rows[:, :, first:last, span, :].reshape(4 * (last - first) * capacity, width)
        hidden = gated_rows(block, gate_ref[expert], up_ref[expert])
        for start in range(0, width, stripe):
            product = narrow(
                jnp.dot(
                    hidden,
                    down_ref[expert, :, start : start + stripe],
                    preferred_element_type=jnp.float32,
                )
            )
            part[:, :, first:last, span, start : start + stripe] = product.reshape(
                2, 2, last - first, capacity, stripe
            )

    def near_half():
        return remote(
            part.at[:, 1 - core, :NEAR],
            half_rows.at[:, :NEAR],
            half_send.at[local_experts],
            half_recv.at[local_experts],
            core_peer,
        )

    def far_half(expert):
        return remote(
            part.at[:, 1 - core, NEAR:, spans(expert)],
            half_rows.at[:, NEAR:, spans(expert)],
            half_send.at[expert],
            half_recv.at[expert],
            core_peer,
        )

    def back_near(step):
        return remote(
            part.at[row, core, step],
            returned.at[me],
            back_send.at[0, step],
            back_recv.at[0, step],
            peer(step),
        )

    def back_peer(step):
        return remote(
            part.at[1 - row, core, step],
            returned_peer.at[near_place],
            peer_send.at[1, step],
            peer_recv.at[1, step],
            peer(step),
        )

    def back_far(step, expert):
        return remote(
            part.at[row, core, step, spans(expert)],
            returned.at[me, spans(expert)],
            back_send.at[expert, step],
            back_recv.at[expert, step],
            peer(step),
        )

    def y_copy(step, expert):
        return remote(
            part.at[1 - row, core, step, spans(expert)],
            far_rows.at[step - NEAR, spans(expert)],
            far_send.at[expert, step],
            far_recv.at[expert, step],
            y_peer,
        )

    def settle_near():
        near_half().wait_recv()
        for step in list(range(1, NEAR)) + [0]:
            outer = narrow(wide(part[1 - row, core, step]) + wide(half_rows[1 - row, step]))
            if step:
                part[1 - row, core, step] = outer
                back_peer(step).start()
            else:
                returned_peer[near_place] = outer
            total = narrow(wide(part[row, core, step]) + wide(half_rows[row, step]))
            if step:
                part[row, core, step] = total
                back_near(step).start()
            else:
                returned[me] = total

    def settle_outer(expert):
        far_half(expert).wait_recv()
        span = spans(expert)
        for step in far_steps:
            part[1 - row, core, step, span] = narrow(
                wide(part[1 - row, core, step, span]) + wide(half_rows[1 - row, step, span])
            )
            y_copy(step, expert).start()

    def settle_far(expert):
        span = spans(expert)
        for step in far_steps:
            y_copy(step, expert).wait_recv()
            part[row, core, step, span] = narrow(
                wide(part[row, core, step, span])
                + wide(half_rows[row, step, span])
                + wide(far_rows[step - NEAR, span])
            )
            back_far(step, expert).start()

    def wait_rows(steps):
        for step in steps:
            for route in ("core", "cross"):
                moved_rows(step, route).wait_recv()

    wait_rows(range(NEAR))
    for expert in range(local_experts):
        compute(0, NEAR, expert)
    near_half().start()
    wait_rows(far_steps)
    for expert in range(local_experts):
        compute(NEAR, ep_count, expert)
        far_half(expert).start()
        if expert == 0:
            settle_near()
        else:
            settle_outer(expert - 1)
    settle_outer(local_experts - 1)
    for step in range(1, NEAR):
        back_peer(step).wait_recv()
    shared_half.wait_recv()
    for start in range(0, width, stripe):
        cut = slice(start, start + stripe)
        shared[1 - row, core, :, cut] = narrow(
            weighted_rows(
                peer_weight_ref[...],
                returned_peer[:, :, cut].reshape(NEAR * slot_rows, stripe),
            )
            + wide(shared[1 - row, core, :, cut])
            + wide(half_shared[1 - row, :, cut])
        )
    shared_y.start()
    for expert in range(local_experts):
        settle_far(expert)
    mixed_y.wait_recv()
    both_out[0] = narrow(wide(mixed[row, core]) + wide(half_mixed[row]) + wide(far_mixed[...]))
    shared_y.wait_recv()
    for step in range(1, NEAR):
        back_near(step).wait_recv()
    for expert in range(local_experts):
        for step in far_steps:
            back_far(step, expert).wait_recv()
    for start in range(0, width, stripe):
        cut = slice(start, start + stripe)
        both_out[1, :, cut] = narrow(
            weighted_rows(
                weight_ref[...], returned[:, :, cut].reshape(ep_count * slot_rows, stripe)
            )
            + wide(shared[row, core, :, cut])
            + wide(half_shared[row, :, cut])
            + wide(far_shared[:, cut])
        )

    for step in range(1, ep_count):
        latent_ep(step).wait_send()
        slots_ep(step).wait_send()
    for step in range(ep_count):
        latent_core(step).wait_send()
        for route in ("core", "cross"):
            moved_rows(step, route).wait_send()
    for step in range(1, NEAR):
        peer_slots_ep(step).wait_send()
        back_near(step).wait_send()
        back_peer(step).wait_send()
    for step in far_steps:
        moved_rows(step, "y").wait_send()
        for expert in range(local_experts):
            back_far(step, expert).wait_send()
            y_copy(step, expert).wait_send()
    for route in ("y", "core", "cross"):
        moved(queries, 1, route).wait_send()
        moved(tokens, 0, route).wait_send()
    for expert in range(local_experts):
        far_half(expert).wait_send()
    for copy in (info_y, sum_y, near_half(), shared_half, mixed_half, shared_y, mixed_y):
        copy.wait_send()


def block_call(ep_count, capacity, *operands):
    query_latent, key_latent = operands[:2]
    own_rows, width = operands[5].shape
    head_lanes = operands[15].shape[0]
    local_experts = operands[16].shape[0]
    slot_rows = local_experts * capacity
    latent_shape = (own_rows, key_latent.shape[1] + 128)
    vmem = pl.BlockSpec(memory_space=pltpu.VMEM)
    anywhere = pl.BlockSpec(memory_space=pl.ANY)

    def held(*shape):
        return pltpu.VMEM(shape, jnp.bfloat16)

    def precise(*shape):
        return pltpu.VMEM(shape, jnp.float32)

    def sems(*shape):
        return pltpu.SemaphoreType.DMA(shape)

    group_rows = 4 * own_rows
    key_rows = 2 * ep_count * own_rows
    row_block = (slot_rows, width)
    side = (own_rows, width)
    return pl.pallas_call(
        lambda *refs: block_kernel(ep_count, capacity, *refs),
        out_shape=jax.ShapeDtypeStruct((2, own_rows, width), jnp.bfloat16),
        in_specs=[vmem] * 11 + [anywhere] * 11,
        out_specs=vmem,
        scratch_shapes=[
            held(ep_count, *row_block),
            held(NEAR, *row_block),
            held(2, query_latent.shape[1], head_lanes + 128),
            held(2, key_latent.shape[1], 2 * head_lanes),
            held(head_lanes, width),
            held(3 * own_rows, ep_count * slot_rows),
            held(3 * own_rows, NEAR * slot_rows),
            held(2, 2, ep_count, *row_block),
            held(2, ep_count, *latent_shape),
            held(2, 2, *side),
            held(2, 2, *query_latent.shape),
        ]
        + [held(*operand.shape) for operand in operands[16:]]
        + [
            held(2, key_rows, head_lanes + 128),
            held(2, key_rows, head_lanes),
            held(2, group_rows, head_lanes + 128),
            held(group_rows, head_lanes),
            held(2, 2, ep_count, *row_block),
            held(2, ep_count, *row_block),
            held(ep_count - NEAR, *row_block),
            held(ep_count, *row_block),
            held(NEAR, *row_block),
            held(2, 2, *side),
            held(2, *side),
            held(*side),
            held(2, 2, *side),
            held(2, *side),
            held(*side),
            precise(8, 128),
            precise(8, 128),
            precise(group_rows, head_lanes),
            precise(group_rows, head_lanes),
            precise(group_rows + 16, head_lanes),
            precise(group_rows + 16, head_lanes),
        ]
        + [sems(2, ep_count + 1)] * 8
        + [sems(2, NEAR)] * 2
        + [sems(local_experts, ep_count)] * 4
        + [sems(local_experts + 1)] * 2
        + [sems(4)] * 2
        + [sems(2), sems(15)],
        compiler_params=pltpu.CompilerParams(
            collective_id=0, has_side_effects=True, vmem_limit_bytes=VMEM_LIMIT
        ),
        name="block",
    )(*operands)


def shards(
    query_latent,
    key_latent,
    rotary_key,
    query_gain,
    latent_gain,
    query_content,
    query_rotary,
    key_content,
    value_weight,
    output_weight,
    expert_input,
    norm_gain,
    routes,
    route_weight,
    expert_gate,
    expert_up,
    expert_down,
    shared_gate,
    shared_up,
    shared_down,
):
    group_size = lax.axis_size("tp")
    expert_groups = lax.axis_size("ep")
    token_rows = expert_input.shape[0]
    picks = routes.shape[1]
    local_experts = expert_gate.shape[0]
    expert_total = local_experts * expert_groups
    capacity = 2 * token_rows * picks // expert_total
    if group_size != 4 or capacity % 16 or not fits_kernel(expert_groups, local_experts * capacity):
        return shards_plain(
            query_latent,
            key_latent,
            rotary_key,
            query_gain,
            latent_gain,
            query_content,
            query_rotary,
            key_content,
            value_weight,
            output_weight,
            expert_input,
            norm_gain,
            routes,
            route_weight,
            expert_gate,
            expert_up,
            expert_down,
            shared_gate,
            shared_up,
            shared_down,
        )
    group_rows_count = expert_input.shape[0] * group_size
    positions = lax.axis_index("ep") * group_rows_count + jnp.arange(
        group_rows_count, dtype=jnp.int32
    )
    frequency = rope_base ** (-jnp.arange(ROTARY // 2, dtype=jnp.float32) * 2.0 / ROTARY)
    angles = positions.astype(jnp.float32)[:, None] * jnp.tile(
        jnp.repeat(frequency, 2), 128 // ROTARY
    )[None, :]
    both = block_call(
        expert_groups,
        capacity,
        query_latent,
        key_latent,
        rotary_key.T,
        query_gain[None, :],
        latent_gain[None, :],
        expert_input,
        norm_gain[None, :],
        routes.T,
        route_weight.T,
        jnp.cos(angles),
        jnp.sin(angles),
        query_content,
        query_rotary,
        key_content,
        value_weight,
        output_weight,
        expert_gate,
        expert_up,
        expert_down,
        shared_gate,
        shared_up,
        shared_down,
    )
    return (both[0], both[1])


def solution(mesh):
    in_specs = (
        P(("ep", "tp"), None),
        P(("ep", "tp"), None),
        P(("ep", "tp"), None),
        P(),
        P(),
        P(),
        P(),
        P(),
        P(),
        P("tp", None),
        P(("ep", "tp"), None),
        P(),
        P(("ep", "tp"), None),
        P(("ep", "tp"), None),
        P("ep", None, "tp"),
        P("ep", None, "tp"),
        P("ep", "tp", None),
        P(None, "tp"),
        P(None, "tp"),
        P("tp", None),
    )
    out_specs = (P(("ep", "tp"), None), P(("ep", "tp"), None))
    return jax.shard_map(shards, mesh=mesh, in_specs=in_specs, out_specs=out_specs, check_vma=False)
```

```python
import math

import jax
import jax.numpy as jnp
import numpy as np
from jax import lax
from jax.experimental import pallas as pl
from jax.experimental.pallas import tpu as pltpu
from jax.sharding import PartitionSpec as P

HEADS = 8
CONTENT = 64
ROTARY = 32
VALUE = 64


norm_eps = 1e-06
rope_base = 10000.0


def rms_rows(entries, gain_row):
    widened = entries.astype(jnp.float32)
    return widened * lax.rsqrt(jnp.mean(widened * widened, -1, keepdims=True) + norm_eps) * gain_row


def turn_pairs(entries, positions):
    width_full = entries.shape[-1]
    frequency = rope_base ** (-jnp.arange(width_full // 2, dtype=jnp.float32) * 2.0 / width_full)
    angles = positions.astype(jnp.float32)[:, None] * frequency[None, :]
    cosine = jnp.cos(angles)[:, None, :]
    sine_part = jnp.sin(angles)[:, None, :]
    even_part = entries[..., 0::2]
    odd_part = entries[..., 1::2]
    joined = jnp.stack(
        [even_part * cosine - odd_part * sine_part, even_part * sine_part + odd_part * cosine], -1
    )
    return joined.reshape(entries.shape)


def absorb_block(carried, query_part, query_turn, key_part, key_turn, value_rows, score_scale):
    running_peak, running_total, summed = carried
    scores = jnp.einsum("qhc,khc->qhk", query_part, key_part, preferred_element_type=jnp.float32)
    scores = scores + jnp.einsum(
        "qhr,kr->qhk", query_turn, key_turn, preferred_element_type=jnp.float32
    )
    scores = scores * score_scale
    new_peak = jnp.maximum(running_peak, jnp.max(scores, -1))
    factor = jnp.exp(running_peak - new_peak)
    weights = jnp.exp(scores - new_peak[..., None])
    running_total = running_total * factor + jnp.sum(weights, -1)
    summed = summed * factor[..., None] + jnp.einsum(
        "qhk,khv->qhv", weights.astype(jnp.bfloat16), value_rows, preferred_element_type=jnp.float32
    )
    return (new_peak, running_total, summed)


def absorb_piece(carried, query_part, query_turn, key_part, key_turn, value_rows, score_scale):
    row_count = key_part.shape[0]
    key_block = math.gcd(row_count, 2048)
    if key_block == row_count:
        return absorb_block(
            carried, query_part, query_turn, key_part, key_turn, value_rows, score_scale
        )
    block_count = row_count // key_block

    def advance(state, pieces):
        return (
            absorb_block(
                state, query_part, query_turn, pieces[0], pieces[1], pieces[2], score_scale
            ),
            None,
        )

    stacked = (
        key_part.reshape((block_count, key_block) + key_part.shape[1:]),
        key_turn.reshape(block_count, key_block, key_turn.shape[1]),
        value_rows.reshape((block_count, key_block) + value_rows.shape[1:]),
    )
    carried, ignored = lax.scan(advance, carried, stacked)
    return carried


def expand_keys(latent_rows, key_columns, value_columns, head_local):
    row_count = latent_rows.shape[0]
    key_part = (
        jnp.dot(latent_rows, key_columns, preferred_element_type=jnp.float32)
        .astype(jnp.bfloat16)
        .reshape(row_count, head_local, CONTENT)
    )
    value_rows = (
        jnp.dot(latent_rows, value_columns, preferred_element_type=jnp.float32)
        .astype(jnp.bfloat16)
        .reshape(row_count, head_local, VALUE)
    )
    return (key_part, value_rows)


def expert_terms(row_block, gate_weight, up_weight, down_weight):
    gated = jnp.einsum("secd,edf->secf", row_block, gate_weight, preferred_element_type=jnp.float32)
    lifted = jnp.einsum("secd,edf->secf", row_block, up_weight, preferred_element_type=jnp.float32)
    hidden = (jax.nn.silu(gated) * lifted).astype(jnp.bfloat16)
    return jnp.einsum("secf,efd->secd", hidden, down_weight, preferred_element_type=jnp.float32)


def shared_terms(row_block, gate_weight, up_weight, down_weight):
    gated = jnp.dot(row_block, gate_weight, preferred_element_type=jnp.float32)
    lifted = jnp.dot(row_block, up_weight, preferred_element_type=jnp.float32)
    hidden = (jax.nn.silu(gated) * lifted).astype(jnp.bfloat16)
    return jnp.dot(hidden, down_weight, preferred_element_type=jnp.float32)


def shards_plain(
    query_latent,
    key_latent,
    rotary_key,
    query_gain,
    latent_gain,
    query_content,
    query_rotary,
    key_content,
    value_weight,
    output_weight,
    expert_input,
    norm_gain,
    routes,
    route_weight,
    expert_gate,
    expert_up,
    expert_down,
    shared_gate,
    shared_up,
    shared_down,
):
    group_size = lax.axis_size("tp")
    expert_groups = lax.axis_size("ep")
    own_rows = query_latent.shape[0]
    head_local = HEADS // group_size
    head_index = lax.axis_index("tp")
    group_rows_count = own_rows * group_size
    group_start = lax.axis_index("ep") * group_rows_count
    own_start = group_start + head_index * own_rows
    score_scale = (CONTENT + ROTARY) ** (-0.5)
    query_normed = rms_rows(query_latent, query_gain).astype(jnp.bfloat16)
    latent_normed = rms_rows(key_latent, latent_gain).astype(jnp.bfloat16)
    own_positions = own_start + jnp.arange(own_rows, dtype=jnp.int32)
    key_turned = turn_pairs(rotary_key.astype(jnp.float32)[:, None, :], own_positions)[
        :, 0, :
    ].astype(jnp.bfloat16)
    token_rows = expert_input.shape[0]
    picks = routes.shape[1]
    local_experts = expert_gate.shape[0]
    expert_total = local_experts * expert_groups
    capacity = 2 * token_rows * picks // expert_total
    slot_total = expert_total * capacity
    model_width = expert_input.shape[1]
    expert_normed = rms_rows(expert_input, norm_gain).astype(jnp.bfloat16)
    flat_routes = routes.reshape(-1)
    marks = (flat_routes[:, None] == jnp.arange(expert_total, dtype=jnp.int32)[None, :]).astype(
        jnp.int32
    )
    ranks = jnp.sum((jnp.cumsum(marks, 0) - marks) * marks, 1)
    targets = flat_routes * capacity + ranks
    picker = (jnp.arange(slot_total, dtype=jnp.int32)[:, None] == targets[None, :]).astype(
        jnp.int32
    )
    picker = jnp.sum(picker.reshape(slot_total, token_rows, picks), 2).astype(jnp.bfloat16)
    outgoing = jnp.dot(picker, expert_normed, preferred_element_type=jnp.float32).astype(
        jnp.bfloat16
    )
    outgoing = outgoing.reshape(expert_groups, local_experts, capacity, model_width)
    received = lax.all_to_all(outgoing, "ep", split_axis=0, concat_axis=0, tiled=True)
    group_query, group_latent, group_turn, gathered_rows, gathered_tokens = (
        lax.all_gather(query_normed, "tp", axis=0, tiled=True),
        lax.all_gather(latent_normed, "tp", axis=0, tiled=True),
        lax.all_gather(key_turned, "tp", axis=0, tiled=True),
        lax.all_gather(received, "tp", axis=0, tiled=True),
        lax.all_gather(expert_normed, "tp", axis=0, tiled=True),
    )
    positions = group_start + jnp.arange(group_rows_count, dtype=jnp.int32)
    content_columns = lax.dynamic_slice_in_dim(
        query_content, head_index * head_local * CONTENT, head_local * CONTENT, 1
    )
    rotary_columns = lax.dynamic_slice_in_dim(
        query_rotary, head_index * head_local * ROTARY, head_local * ROTARY, 1
    )
    query_part = (
        jnp.dot(group_query, content_columns, preferred_element_type=jnp.float32)
        .astype(jnp.bfloat16)
        .reshape(group_rows_count, head_local, CONTENT)
    )
    query_turn = turn_pairs(
        jnp.dot(group_query, rotary_columns, preferred_element_type=jnp.float32).reshape(
            group_rows_count, head_local, ROTARY
        ),
        positions,
    ).astype(jnp.bfloat16)
    key_columns = lax.dynamic_slice_in_dim(
        key_content, head_index * head_local * CONTENT, head_local * CONTENT, 1
    )
    value_columns = lax.dynamic_slice_in_dim(
        value_weight, head_index * head_local * VALUE, head_local * VALUE, 1
    )
    carry_start = (
        jnp.full((group_rows_count, head_local), -jnp.inf, jnp.float32),
        jnp.zeros((group_rows_count, head_local), jnp.float32),
        jnp.zeros((group_rows_count, head_local, VALUE), jnp.float32),
    )
    key_part, value_rows = expand_keys(
        lax.all_gather(group_latent, "ep", axis=0, tiled=True),
        key_columns,
        value_columns,
        head_local,
    )
    running_peak, running_total, summed = absorb_piece(
        carry_start,
        query_part,
        query_turn,
        key_part,
        lax.all_gather(group_turn, "ep", axis=0, tiled=True),
        value_rows,
        score_scale,
    )
    attended = (
        (summed / running_total[..., None])
        .astype(jnp.bfloat16)
        .reshape(group_rows_count, head_local * VALUE)
    )
    routed_term = expert_terms(gathered_rows, expert_gate, expert_up, expert_down)
    shared_term = shared_terms(gathered_tokens, shared_gate, shared_up, shared_down)
    mixer_term = jnp.dot(attended, output_weight, preferred_element_type=jnp.float32)
    mixer_sum, routed_sum, shared_sum = (
        lax.psum_scatter(
            mixer_term.astype(jnp.bfloat16), "tp", scatter_dimension=0, tiled=True
        ).astype(jnp.float32),
        lax.psum_scatter(
            routed_term.astype(jnp.bfloat16), "tp", scatter_dimension=0, tiled=True
        ).astype(jnp.float32),
        lax.psum_scatter(
            shared_term.astype(jnp.bfloat16), "tp", scatter_dimension=0, tiled=True
        ).astype(jnp.float32),
    )
    mixer_out = mixer_sum.astype(jnp.bfloat16)
    returned = lax.all_to_all(
        routed_sum.astype(jnp.bfloat16), "ep", split_axis=0, concat_axis=0, tiled=True
    )
    returned = returned.reshape(slot_total, model_width)
    picked = jnp.take(returned, targets, axis=0).reshape(token_rows, picks, model_width)
    combined = jnp.sum(route_weight[..., None] * picked.astype(jnp.float32), 1) + shared_sum
    expert_out = combined.astype(jnp.bfloat16)
    return (mixer_out, expert_out)


MESH = pl.DeviceIdType.MESH
VMEM_LIMIT = 60 * 1024 * 1024
NEAR = 4


def fits_kernel(ep_count, slot_rows):
    return ep_count == 2 * NEAR and NEAR * slot_rows % 128 == 0


def flip(place, bits):
    flipped = place
    bit = 1
    while bit <= bits:
        if bits & bit:
            flipped = flipped + bit * (1 - 2 * (place // bit % 2))
        bit *= 2
    return flipped


def greet(ep_count, me, head_index):
    barrier = pltpu.get_barrier_semaphore()
    for step in range(1, ep_count):
        pl.semaphore_signal(
            barrier, inc=1, device_id=(flip(me, step), head_index), device_id_type=MESH
        )
    row, core = head_index // 2, head_index % 2
    for other in ((1 - row) * 2 + core, row * 2 + 1 - core):
        pl.semaphore_signal(barrier, inc=1, device_id=(me, other), device_id_type=MESH)
    return lambda: pl.semaphore_wait(barrier, ep_count + 1)


def gated_rows(rows, gate_weight, up_weight):
    gated = jnp.dot(rows, gate_weight, preferred_element_type=jnp.float32)
    lifted = jnp.dot(rows, up_weight, preferred_element_type=jnp.float32)
    return (gated / (1.0 + jnp.exp(-gated)) * lifted).astype(jnp.bfloat16)


def wide(entries):
    return entries.astype(jnp.float32)


def narrow(entries):
    return entries.astype(jnp.bfloat16)


def choose_slots(routes, weights, expert_total, capacity, first_slot, slot_count):
    own_rows = routes.shape[0]
    expert_lane = lax.broadcasted_iota(jnp.int32, (own_rows, expert_total), 1)
    named = [
        jnp.where(routes[:, pick : pick + 1] == expert_lane, 1.0, 0.0)
        for pick in range(routes.shape[1])
    ]
    earlier = narrow(
        jnp.where(
            lax.broadcasted_iota(jnp.int32, (own_rows, own_rows), 0)
            > lax.broadcasted_iota(jnp.int32, (own_rows, own_rows), 1),
            1.0,
            0.0,
        )
    )
    ahead = jnp.dot(earlier, narrow(sum(named)), preferred_element_type=jnp.float32)
    slot_lane = lax.broadcasted_iota(jnp.int32, (own_rows, slot_count), 1) + first_slot
    picker = jnp.zeros(slot_lane.shape, jnp.float32)
    weight = jnp.zeros(slot_lane.shape, jnp.float32)
    for pick, marks in enumerate(named):
        rank = jnp.sum(ahead * marks, 1, keepdims=True).astype(jnp.int32)
        chosen = slot_lane == routes[:, pick : pick + 1] * capacity + rank
        picker = jnp.where(chosen, 1.0, picker)
        weight = jnp.where(chosen, weights[:, pick : pick + 1], weight)
    return narrow(picker.T), weight


def store_split(target, weight):
    own_rows = weight.shape[0]
    high = narrow(weight)
    rest = weight - wide(high)
    middle = narrow(rest)
    target[:own_rows] = high
    target[own_rows : 2 * own_rows] = middle
    target[2 * own_rows :] = narrow(rest - wide(middle))


def weighted_rows(split_weight, entries):
    picked = jnp.dot(split_weight, entries, preferred_element_type=jnp.float32)
    own_rows = picked.shape[0] // 3
    return picked[:own_rows] + picked[own_rows : 2 * own_rows] + picked[2 * own_rows :]


def block_kernel(
    ep_count,
    capacity,
    query_latent_hbm,
    key_latent_hbm,
    rotary_key_hbm,
    query_gain_hbm,
    latent_gain_hbm,
    expert_input_hbm,
    norm_gain_hbm,
    routes_hbm,
    route_weight_hbm,
    frequency_hbm,
    query_content_hbm,
    query_rotary_hbm,
    key_content_hbm,
    value_weight_hbm,
    output_weight_hbm,
    gate_hbm,
    up_hbm,
    down_hbm,
    shared_gate_hbm,
    shared_up_hbm,
    shared_down_hbm,
    mixer_out,
    expert_out,
    query_latent_ref,
    key_latent_ref,
    rotary_key_ref,
    query_gain_ref,
    latent_gain_ref,
    expert_input_ref,
    norm_gain_ref,
    routes_ref,
    route_weight_ref,
    frequency_ref,
    cosine_ref,
    sine_ref,
    mixer_rows,
    expert_rows,
    slots_ref,
    peer_slots_ref,
    query_columns_ref,
    latent_columns_ref,
    output_weight_ref,
    weight_ref,
    peer_weight_ref,
    rows,
    latents,
    tokens,
    queries,
    gate_ref,
    up_ref,
    down_ref,
    shared_gate_ref,
    shared_up_ref,
    shared_down_ref,
    keys,
    values,
    query_wide,
    attended,
    part,
    half_rows,
    far_rows,
    returned,
    returned_peer,
    mixed,
    half_mixed,
    far_mixed,
    shared,
    half_shared,
    far_shared,
    info_ref,
    peer_info_ref,
    own_sum,
    own_stats,
    sent_sum,
    far_sum,
    ep_send,
    ep_recv,
    y_send,
    y_recv,
    core_send,
    core_recv,
    cross_send,
    cross_recv,
    peer_send,
    peer_recv,
    back_send,
    back_recv,
    far_send,
    far_recv,
    half_send,
    half_recv,
    side_send,
    side_recv,
    own_sem,
    weight_sem,
    input_sem,
    out_sem,
):
    me = lax.axis_index("ep")
    head_index = lax.axis_index("tp")
    row, core = head_index // 2, head_index % 2
    y_peer = (me, (1 - row) * 2 + core)
    core_peer = (me, row * 2 + 1 - core)
    local_experts = gate_ref.shape[0]
    width = rows.shape[-1]
    own_rows = tokens.shape[2]
    slot_rows = rows.shape[3]
    group_rows = attended.shape[0]
    picks = routes_ref.shape[0]
    stripe = math.gcd(width, 512)
    far_steps = range(NEAR, ep_count)
    chunks = ((NEAR + 2, ep_count), (NEAR, NEAR + 2))
    greeted = greet(ep_count, me, head_index)
    arguments = [
        pltpu.make_async_copy(source, target, input_sem.at[place])
        for place, (source, target) in enumerate(
            (
                (key_latent_hbm, key_latent_ref),
                (rotary_key_hbm, rotary_key_ref),
                (latent_gain_hbm, latent_gain_ref),
                (frequency_hbm, frequency_ref),
                (expert_input_hbm, expert_input_ref),
                (norm_gain_hbm, norm_gain_ref),
                (routes_hbm, routes_ref),
                (route_weight_hbm, route_weight_ref),
                (query_latent_hbm, query_latent_ref),
                (query_gain_hbm, query_gain_ref),
            )
        )
    ]
    for argument in arguments:
        argument.start()
    near_place = me % NEAR

    def peer(step):
        return (flip(me, step), head_index)

    def remote(source, target, send_sem, recv_sem, device):
        return pltpu.make_async_remote_copy(
            src_ref=source,
            dst_ref=target,
            send_sem=send_sem,
            recv_sem=recv_sem,
            device_id=device,
            device_id_type=MESH,
        )

    head_lanes = attended.shape[1]
    heads = head_lanes // VALUE
    fetch_list = []
    for side in range(2):
        side_index = (row if side == 0 else 1 - row) * 2 + core
        columns = pl.ds(pl.multiple_of(side_index * head_lanes, head_lanes), head_lanes)
        turn_columns = pl.ds(pl.multiple_of(side_index * heads * ROTARY // 128 * 128, 128), 128)
        fetch_list += [
            (query_content_hbm.at[:, columns], query_columns_ref.at[side, :, :head_lanes]),
            (query_rotary_hbm.at[:, turn_columns], query_columns_ref.at[side, :, head_lanes:]),
            (key_content_hbm.at[:, columns], latent_columns_ref.at[side, :, :head_lanes]),
            (value_weight_hbm.at[:, columns], latent_columns_ref.at[side, :, head_lanes:]),
        ]
    fetch_list += [
        (output_weight_hbm, output_weight_ref),
        (shared_gate_hbm, shared_gate_ref),
        (shared_up_hbm, shared_up_ref),
        (shared_down_hbm, shared_down_ref),
        (gate_hbm, gate_ref),
        (up_hbm, up_ref),
        (down_hbm, down_ref),
    ]
    fetches = [
        pltpu.make_async_copy(source, target, weight_sem.at[place])
        for place, (source, target) in enumerate(fetch_list)
    ]
    for fetch in fetches:
        fetch.start()

    def turn(entries, cosine, sine):
        lane = lax.broadcasted_iota(jnp.int32, entries.shape, 1)
        crossed = jnp.where(
            lane % 2 == 0, -pltpu.roll(entries, 127, 1), pltpu.roll(entries, 1, 1)
        )
        return narrow(entries * cosine + crossed * sine)

    def angles(first, count):
        places = first + lax.broadcasted_iota(jnp.int32, (count, 128), 0)
        return places.astype(jnp.float32) * frequency_ref[...]

    for argument in arguments[:4]:
        argument.wait()
    rank_width = key_latent_ref.shape[1]
    latents[core, 0, :, :rank_width] = narrow(rms_rows(key_latent_ref[...], latent_gain_ref[...]))
    repeats = narrow(
        jnp.where(
            lax.broadcasted_iota(jnp.int32, (ROTARY, 128), 0)
            == lax.broadcasted_iota(jnp.int32, (ROTARY, 128), 1) % ROTARY,
            1.0,
            0.0,
        )
    )
    own_angles = angles((me * 4 + head_index) * own_rows, own_rows)
    latents[core, 0, :, rank_width:] = turn(
        lax.dot_general(
            rotary_key_ref[...],
            repeats,
            (((0,), (0,)), ((), ())),
            preferred_element_type=jnp.float32,
        ),
        jnp.cos(own_angles),
        jnp.sin(own_angles),
    )
    for argument in arguments[4:]:
        argument.wait()
    expert_normed = narrow(rms_rows(expert_input_ref[...], norm_gain_ref[...]))
    tokens[row, core] = expert_normed
    queries[row, core] = narrow(rms_rows(query_latent_ref[...], query_gain_ref[...]))
    info_ref[...] = jnp.zeros(info_ref.shape, jnp.float32)
    info_ref[:picks, :own_rows] = routes_ref[...].astype(jnp.float32)
    info_ref[picks : 2 * picks, :own_rows] = route_weight_ref[...]
    greeted()

    def latent_ep(step):
        if step % 2 == 0:
            return remote(
                latents.at[core, 0],
                latents.at[core, step],
                ep_send.at[1, step],
                ep_recv.at[1, step],
                peer(step),
            )
        return remote(
            latents.at[core, step - 1],
            latents.at[core, step],
            ep_send.at[1, step],
            ep_recv.at[1, step],
            peer(1),
        )

    def latent_core(step):
        return remote(
            latents.at[core, step],
            latents.at[core, step],
            core_send.at[1, step],
            core_recv.at[1, step],
            core_peer,
        )

    def slots_ep(step):
        return remote(
            slots_ref.at[flip(me, step)],
            rows.at[row, core, step],
            ep_send.at[0, step],
            ep_recv.at[0, step],
            peer(step),
        )

    def peer_slots_ep(step):
        return remote(
            peer_slots_ref.at[flip(near_place, step)],
            rows.at[1 - row, core, step],
            peer_send.at[0, step],
            peer_recv.at[0, step],
            peer(step),
        )

    routes_of = {
        "y": (row, y_send, y_recv, y_peer),
        "core": (row, core_send, core_recv, core_peer),
        "cross": (1 - row, cross_send, cross_recv, core_peer),
    }

    def moved_rows(step, route):
        origin_row, send_sem, recv_sem, device = routes_of[route]
        block = rows.at[origin_row, core, step]
        source = block
        if step == 0:
            source = peer_slots_ref.at[near_place] if route == "cross" else slots_ref.at[me]
        return remote(source, block, send_sem.at[0, step], recv_sem.at[0, step], device)

    def moved(buffer, place, route):
        origin_row, send_sem, recv_sem, device = routes_of[route]
        block = buffer.at[origin_row, core]
        return remote(
            block, block, send_sem.at[place, ep_count], recv_sem.at[place, ep_count], device
        )

    info_y = remote(
        info_ref, peer_info_ref, y_send.at[0, 0], y_recv.at[0, 0], y_peer
    )
    for step in range(1, ep_count):
        if step == 1 or step % 2 == 0:
            latent_ep(step).start()
    latent_core(0).start()
    info_y.start()
    for route in ("y", "core"):
        moved(tokens, 0, route).start()
    for route in ("y", "core"):
        moved(queries, 1, route).start()
    expert_total = local_experts * ep_count
    picker, weight = choose_slots(
        routes_ref[...].T, route_weight_ref[...].T, expert_total, capacity, 0, ep_count * slot_rows
    )
    store_split(weight_ref, weight)

    def fill(target, chooser, origin_row):
        for start in range(0, width, stripe):
            target[:, :, start : start + stripe] = narrow(
                jnp.dot(
                    chooser,
                    tokens[origin_row, core, :, start : start + stripe],
                    preferred_element_type=jnp.float32,
                )
            ).reshape(target.shape[0], slot_rows, stripe)

    fill(slots_ref, picker, row)
    for step in (6, 7, 1, 2, 3):
        slots_ep(step).start()
    own_slots = pltpu.make_async_copy(slots_ref.at[me], rows.at[row, core, 0], own_sem.at[0])
    own_slots.start()
    moved_rows(0, "core").start()
    group_angles = angles(me * group_rows, group_rows)
    cosine_ref[...] = jnp.cos(group_angles)
    sine_ref[...] = jnp.sin(group_angles)

    def pass_latents(steps):
        for step in steps:
            latent_ep(step).wait_recv()
            if step % 2 == 0:
                latent_ep(step + 1).start()
            latent_core(step).start()

    info_y.wait_recv()
    peer_picker, peer_weight = choose_slots(
        peer_info_ref[:picks, :own_rows].T.astype(jnp.int32),
        peer_info_ref[picks : 2 * picks, :own_rows].T,
        expert_total,
        capacity,
        me // NEAR * NEAR * slot_rows,
        NEAR * slot_rows,
    )
    store_split(peer_weight_ref, peer_weight)
    pass_latents(range(2, ep_count, 2))
    moved(tokens, 0, "y").wait_recv()
    moved(tokens, 0, "cross").start()
    fill(peer_slots_ref, peer_picker, 1 - row)
    for step in range(1, NEAR):
        peer_slots_ep(step).start()
    for step in (4, 5):
        slots_ep(step).start()
    peer_own = pltpu.make_async_copy(
        peer_slots_ref.at[near_place], rows.at[1 - row, core, 0], own_sem.at[1]
    )
    peer_own.start()
    moved_rows(0, "cross").start()
    moved(queries, 1, "y").wait_recv()
    moved(queries, 1, "cross").start()
    pass_latents(range(1, ep_count, 2))
    for route in ("core", "cross"):
        moved(queries, 1, route).wait_recv()
    for step in range(ep_count):
        latent_core(step).wait_recv()

    def project():
        for fetch in fetches[:8]:
            fetch.wait()
        query_rows = queries[...].reshape(group_rows, queries.shape[-1])
        for side in range(2):
            projected = jnp.dot(
                query_rows, query_columns_ref[side], preferred_element_type=jnp.float32
            )
            query_wide[side, :, :head_lanes] = narrow(projected[:, :head_lanes])
            query_wide[side, :, head_lanes:] = turn(
                projected[:, head_lanes:], cosine_ref[...], sine_ref[...]
            )
        for block in range(2):
            packed = latents[block].reshape(ep_count * own_rows, latents.shape[-1])
            span = slice(block * ep_count * own_rows, (block + 1) * ep_count * own_rows)
            for side in range(2):
                expanded = narrow(
                    jnp.dot(
                        packed[:, :rank_width],
                        latent_columns_ref[side],
                        preferred_element_type=jnp.float32,
                    )
                )
                keys[side, span, :head_lanes] = expanded[:, :head_lanes]
                keys[side, span, head_lanes:] = packed[:, rank_width:]
                values[side, span, :] = expanded[:, head_lanes:]

    block_rows = group_rows // 2

    def attend(side, block):
        span = slice(block * block_rows, (block + 1) * block_rows)
        query_block = query_wide[side, span, :]
        lane = lax.broadcasted_iota(jnp.int32, query_block.shape, 1)
        lane_head = jnp.where(
            lane < head_lanes,
            lane // CONTENT,
            (lane - head_lanes) // ROTARY - core * heads % (128 // ROTARY),
        )
        out_lane = lax.broadcasted_iota(jnp.int32, (block_rows, head_lanes), 1)
        result = jnp.zeros((block_rows, head_lanes), jnp.float32)
        stats = jnp.zeros((block_rows, head_lanes), jnp.float32)
        for head in range(heads):
            chosen = jnp.where(lane_head == head, query_block, jnp.zeros_like(query_block))
            scores = lax.dot_general(
                chosen, keys[side], (((1,), (1,)), ((), ())), preferred_element_type=jnp.float32
            ) * ((CONTENT + ROTARY) ** (-0.5))
            peak = jnp.max(scores, -1, keepdims=True)
            weights = jnp.exp(scores - peak)
            total = jnp.sum(weights, -1, keepdims=True)
            summed = jnp.dot(narrow(weights), values[side], preferred_element_type=jnp.float32)
            result = jnp.where(out_lane // VALUE == head, summed, result)
            stats = jnp.where(out_lane == 2 * head, peak, stats)
            stats = jnp.where(out_lane == 2 * head + 1, total, stats)
        if side == 0:
            own_sum[span, :] = result
            own_stats[span, :] = stats
        else:
            sent_sum[span, :] = result
            sent_sum[group_rows + 8 * block : group_rows + 8 * block + 8, :] = stats.T[:8]

    sum_y = remote(sent_sum, far_sum, y_send.at[1, 0], y_recv.at[1, 0], y_peer)

    def merge():
        sum_y.wait_recv()
        out_lane = lax.broadcasted_iota(jnp.int32, (block_rows, head_lanes), 1)
        for block in range(2):
            span = slice(block * block_rows, (block + 1) * block_rows)
            here = own_stats[span, :]
            there = far_sum[group_rows + 8 * block : group_rows + 8 * block + 8, :].T
            result = jnp.zeros((block_rows, head_lanes), jnp.float32)
            for head in range(heads):
                peak_here, total_here = here[:, 2 * head : 2 * head + 1], here[:, 2 * head + 1 : 2 * head + 2]
                peak_there, total_there = there[:, 2 * head : 2 * head + 1], there[:, 2 * head + 1 : 2 * head + 2]
                peak = jnp.maximum(peak_here, peak_there)
                factor_here = jnp.exp(peak_here - peak)
                factor_there = jnp.exp(peak_there - peak)
                total = total_here * factor_here + total_there * factor_there
                summed = own_sum[span, :] * factor_here + far_sum[span, :] * factor_there
                result = jnp.where(out_lane // VALUE == head, summed / total, result)
            attended[span, :] = narrow(result)

    def mix():
        fetches[8].wait()
        for start in range(0, width, stripe):
            product = narrow(
                jnp.dot(
                    attended[...],
                    output_weight_ref[:, start : start + stripe],
                    preferred_element_type=jnp.float32,
                )
            )
            mixed[:, :, :, start : start + stripe] = product.reshape(2, 2, own_rows, stripe)

    def share():
        for fetch in fetches[9:12]:
            fetch.wait()
        for route in ("core", "cross"):
            moved(tokens, 0, route).wait_recv()
        hidden = gated_rows(
            tokens[...].reshape(group_rows, width), shared_gate_ref[...], shared_up_ref[...]
        )
        for start in range(0, width, stripe):
            product = narrow(
                jnp.dot(
                    hidden,
                    shared_down_ref[:, start : start + stripe],
                    preferred_element_type=jnp.float32,
                )
            )
            shared[:, :, :, start : start + stripe] = product.reshape(2, 2, own_rows, stripe)

    shared_half = remote(
        shared.at[:, 1 - core], half_shared, side_send.at[0], side_recv.at[0], core_peer
    )
    mixed_half = remote(
        mixed.at[:, 1 - core], half_mixed, side_send.at[1], side_recv.at[1], core_peer
    )
    shared_y = remote(
        shared.at[1 - row, core], far_shared, side_send.at[2], side_recv.at[2], y_peer
    )
    mixed_y = remote(mixed.at[1 - row, core], far_mixed, side_send.at[3], side_recv.at[3], y_peer)

    def mixed_far():
        mixed_half.wait_recv()
        mixed[1 - row, core] = narrow(wide(mixed[1 - row, core]) + wide(half_mixed[1 - row]))
        mixed_y.start()

    def arrive(step):
        slots_ep(step).wait_recv()
        if step >= NEAR:
            moved_rows(step, "y").start()
        moved_rows(step, "core").start()

    def arrive_peer(step):
        if step >= NEAR:
            moved_rows(step, "y").wait_recv()
        else:
            peer_slots_ep(step).wait_recv()
        moved_rows(step, "cross").start()

    def spans(expert):
        return slice(expert * capacity, (expert + 1) * capacity)

    def compute(first, last, expert):
        span = spans(expert)
        block = rows[:, :, first:last, span, :].reshape(4 * (last - first) * capacity, width)
        hidden = gated_rows(block, gate_ref[expert], up_ref[expert])
        for start in range(0, width, stripe):
            product = narrow(
                jnp.dot(
                    hidden,
                    down_ref[expert, :, start : start + stripe],
                    preferred_element_type=jnp.float32,
                )
            )
            part[:, :, first:last, span, start : start + stripe] = product.reshape(
                2, 2, last - first, capacity, stripe
            )

    def near_half():
        return remote(
            part.at[:, 1 - core, :NEAR],
            half_rows.at[:, :NEAR],
            half_send.at[2, 0],
            half_recv.at[2, 0],
            core_peer,
        )

    def far_half(chunk, expert):
        first, last = chunks[chunk]
        return remote(
            part.at[:, 1 - core, first:last, spans(expert)],
            half_rows.at[:, first:last, spans(expert)],
            half_send.at[chunk, expert],
            half_recv.at[chunk, expert],
            core_peer,
        )

    def back_near(step):
        return remote(
            part.at[row, core, step],
            returned.at[me],
            back_send.at[0, step],
            back_recv.at[0, step],
            peer(step),
        )

    def back_peer(step):
        return remote(
            part.at[1 - row, core, step],
            returned_peer.at[near_place],
            peer_send.at[1, step],
            peer_recv.at[1, step],
            peer(step),
        )

    def back_far(step, expert):
        return remote(
            part.at[row, core, step, spans(expert)],
            returned.at[me, spans(expert)],
            back_send.at[expert, step],
            back_recv.at[expert, step],
            peer(step),
        )

    def y_copy(step, expert):
        return remote(
            part.at[1 - row, core, step, spans(expert)],
            far_rows.at[step - NEAR, spans(expert)],
            far_send.at[expert, step],
            far_recv.at[expert, step],
            y_peer,
        )

    def settle_near():
        near_half().wait_recv()
        order = list(range(1, NEAR)) + [0]
        for step in order:
            outer = narrow(wide(part[1 - row, core, step]) + wide(half_rows[1 - row, step]))
            if step:
                part[1 - row, core, step] = outer
                back_peer(step).start()
            else:
                returned_peer[near_place] = outer
        for step in order:
            total = narrow(wide(part[row, core, step]) + wide(half_rows[row, step]))
            if step:
                part[row, core, step] = total
                back_near(step).start()
            else:
                returned[me] = total

    def settle_outer(chunk, expert):
        far_half(chunk, expert).wait_recv()
        span = spans(expert)
        for step in range(*chunks[chunk]):
            part[1 - row, core, step, span] = narrow(
                wide(part[1 - row, core, step, span]) + wide(half_rows[1 - row, step, span])
            )
            y_copy(step, expert).start()

    def settle_far(chunk, expert):
        span = spans(expert)
        for step in range(*chunks[chunk]):
            y_copy(step, expert).wait_recv()
            part[row, core, step, span] = narrow(
                wide(part[row, core, step, span])
                + wide(half_rows[row, step, span])
                + wide(far_rows[step - NEAR, span])
            )
            back_far(step, expert).start()

    def wait_rows(steps):
        for step in steps:
            for route in ("core", "cross"):
                moved_rows(step, route).wait_recv()

    def far_chunk(chunk):
        wait_rows(range(*chunks[chunk]))
        for expert in range(local_experts):
            compute(*chunks[chunk], expert)
            far_half(chunk, expert).start()

    project()
    attend(1, 0)
    attend(1, 1)
    sum_y.start()
    arrive(6)
    arrive(7)
    attend(0, 0)
    for step in range(1, NEAR):
        arrive(step)
    arrive_peer(1)
    attend(0, 1)
    arrive_peer(6)
    arrive_peer(7)
    merge()
    mix()
    mixed_half.start()
    for fetch in fetches[12:]:
        fetch.wait()
    far_chunk(0)
    share()
    shared_half.start()
    for expert in range(local_experts):
        settle_outer(0, expert)
    mixed_far()
    arrive(4)
    settle_far(0, 0)
    arrive(5)
    for expert in range(1, local_experts):
        settle_far(0, expert)
    arrive_peer(2)
    arrive_peer(3)
    arrive_peer(4)
    own_slots.wait()
    peer_own.wait()
    wait_rows(range(NEAR))
    for expert in range(local_experts):
        compute(0, NEAR, expert)
    near_half().start()
    arrive_peer(5)
    far_chunk(1)
    settle_near()
    for expert in range(local_experts):
        settle_outer(1, expert)
    for expert in range(local_experts):
        settle_far(1, expert)
    mixed_y.wait_recv()
    mixer_rows[...] = narrow(
        wide(mixed[row, core]) + wide(half_mixed[row]) + wide(far_mixed[...])
    )
    mixer_copy = pltpu.make_async_copy(mixer_rows, mixer_out, out_sem.at[0])
    mixer_copy.start()
    for step in range(1, NEAR):
        back_peer(step).wait_recv()
    shared_half.wait_recv()
    for start in range(0, width, stripe):
        cut = slice(start, start + stripe)
        shared[1 - row, core, :, cut] = narrow(
            weighted_rows(
                peer_weight_ref[...],
                returned_peer[:, :, cut].reshape(NEAR * slot_rows, stripe),
            )
            + wide(shared[1 - row, core, :, cut])
            + wide(half_shared[1 - row, :, cut])
        )
    shared_y.start()
    for step in range(1, NEAR):
        back_near(step).wait_recv()
    for chunk in range(2):
        for expert in range(local_experts):
            for step in range(*chunks[chunk]):
                back_far(step, expert).wait_recv()
    shared_y.wait_recv()
    out_copies = []
    for place, start in enumerate(range(0, width, stripe)):
        cut = slice(start, start + stripe)
        expert_rows[:, cut] = narrow(
            weighted_rows(
                weight_ref[...], returned[:, :, cut].reshape(ep_count * slot_rows, stripe)
            )
            + wide(shared[row, core, :, cut])
            + wide(half_shared[row, :, cut])
            + wide(far_shared[:, cut])
        )
        out_copies.append(
            pltpu.make_async_copy(
                expert_rows.at[:, cut], expert_out.at[:, cut], out_sem.at[1 + place]
            )
        )
        out_copies[-1].start()

    for step in range(1, ep_count):
        latent_ep(step).wait_send()
        slots_ep(step).wait_send()
    for step in range(ep_count):
        latent_core(step).wait_send()
        for route in ("core", "cross"):
            moved_rows(step, route).wait_send()
    for step in range(1, NEAR):
        peer_slots_ep(step).wait_send()
        back_near(step).wait_send()
        back_peer(step).wait_send()
    for step in far_steps:
        moved_rows(step, "y").wait_send()
        for expert in range(local_experts):
            back_far(step, expert).wait_send()
            y_copy(step, expert).wait_send()
    for route in ("y", "core", "cross"):
        moved(queries, 1, route).wait_send()
        moved(tokens, 0, route).wait_send()
    for chunk in range(2):
        for expert in range(local_experts):
            far_half(chunk, expert).wait_send()
    for copy in (info_y, sum_y, near_half(), shared_half, mixed_half, shared_y, mixed_y):
        copy.wait_send()
    for copy in [mixer_copy] + out_copies:
        copy.wait()


def block_call(ep_count, capacity, *operands):
    query_latent, key_latent = operands[:2]
    own_rows, width = operands[5].shape
    head_lanes = operands[14].shape[0]
    local_experts = operands[15].shape[0]
    slot_rows = local_experts * capacity
    latent_shape = (own_rows, key_latent.shape[1] + 128)
    anywhere = pl.BlockSpec(memory_space=pl.ANY)

    def held(*shape):
        return pltpu.VMEM(shape, jnp.bfloat16)

    def precise(*shape):
        return pltpu.VMEM(shape, jnp.float32)

    def sems(*shape):
        return pltpu.SemaphoreType.DMA(shape)

    group_rows = 4 * own_rows
    key_rows = 2 * ep_count * own_rows
    row_block = (slot_rows, width)
    side = (own_rows, width)
    return pl.pallas_call(
        lambda *refs: block_kernel(ep_count, capacity, *refs),
        out_shape=[jax.ShapeDtypeStruct(side, jnp.bfloat16)] * 2,
        in_specs=[anywhere] * 21,
        out_specs=[anywhere] * 2,
        scratch_shapes=[pltpu.VMEM(operand.shape, operand.dtype) for operand in operands[:10]]
        + [
            precise(group_rows, 128),
            precise(group_rows, 128),
            held(*side),
            held(*side),
            held(ep_count, *row_block),
            held(NEAR, *row_block),
            held(2, query_latent.shape[1], head_lanes + 128),
            held(2, key_latent.shape[1], 2 * head_lanes),
            held(head_lanes, width),
            held(3 * own_rows, ep_count * slot_rows),
            held(3 * own_rows, NEAR * slot_rows),
            held(2, 2, ep_count, *row_block),
            held(2, ep_count, *latent_shape),
            held(2, 2, *side),
            held(2, 2, *query_latent.shape),
        ]
        + [held(*operand.shape) for operand in operands[15:]]
        + [
            held(2, key_rows, head_lanes + 128),
            held(2, key_rows, head_lanes),
            held(2, group_rows, head_lanes + 128),
            held(group_rows, head_lanes),
            held(2, 2, ep_count, *row_block),
            held(2, ep_count, *row_block),
            held(ep_count - NEAR, *row_block),
            held(ep_count, *row_block),
            held(NEAR, *row_block),
            held(2, 2, *side),
            held(2, *side),
            held(*side),
            held(2, 2, *side),
            held(2, *side),
            held(*side),
            precise(8, 128),
            precise(8, 128),
            precise(group_rows, head_lanes),
            precise(group_rows, head_lanes),
            precise(group_rows + 16, head_lanes),
            precise(group_rows + 16, head_lanes),
        ]
        + [sems(2, ep_count + 1)] * 8
        + [sems(2, NEAR)] * 2
        + [sems(local_experts, ep_count)] * 4
        + [sems(3, local_experts)] * 2
        + [sems(4)] * 2
        + [sems(2), sems(15), sems(10), sems(1 + width // math.gcd(width, 512))],
        compiler_params=pltpu.CompilerParams(
            collective_id=0, has_side_effects=True, vmem_limit_bytes=VMEM_LIMIT
        ),
        name="block",
    )(*operands)


def shards(
    query_latent,
    key_latent,
    rotary_key,
    query_gain,
    latent_gain,
    query_content,
    query_rotary,
    key_content,
    value_weight,
    output_weight,
    expert_input,
    norm_gain,
    routes,
    route_weight,
    expert_gate,
    expert_up,
    expert_down,
    shared_gate,
    shared_up,
    shared_down,
):
    group_size = lax.axis_size("tp")
    expert_groups = lax.axis_size("ep")
    token_rows = expert_input.shape[0]
    picks = routes.shape[1]
    local_experts = expert_gate.shape[0]
    expert_total = local_experts * expert_groups
    capacity = 2 * token_rows * picks // expert_total
    if group_size != 4 or capacity % 16 or not fits_kernel(expert_groups, local_experts * capacity):
        return shards_plain(
            query_latent,
            key_latent,
            rotary_key,
            query_gain,
            latent_gain,
            query_content,
            query_rotary,
            key_content,
            value_weight,
            output_weight,
            expert_input,
            norm_gain,
            routes,
            route_weight,
            expert_gate,
            expert_up,
            expert_down,
            shared_gate,
            shared_up,
            shared_down,
        )
    frequency = rope_base ** (-np.arange(ROTARY // 2) * 2.0 / ROTARY)
    return block_call(
        expert_groups,
        capacity,
        query_latent,
        key_latent,
        rotary_key.T,
        query_gain[None, :],
        latent_gain[None, :],
        expert_input,
        norm_gain[None, :],
        routes.T,
        route_weight.T,
        jnp.asarray(np.tile(np.repeat(frequency, 2), 128 // ROTARY)[None, :], jnp.float32),
        query_content,
        query_rotary,
        key_content,
        value_weight,
        output_weight,
        expert_gate,
        expert_up,
        expert_down,
        shared_gate,
        shared_up,
        shared_down,
    )


def solution(mesh):
    in_specs = (
        P(("ep", "tp"), None),
        P(("ep", "tp"), None),
        P(("ep", "tp"), None),
        P(),
        P(),
        P(),
        P(),
        P(),
        P(),
        P("tp", None),
        P(("ep", "tp"), None),
        P(),
        P(("ep", "tp"), None),
        P(("ep", "tp"), None),
        P("ep", None, "tp"),
        P("ep", None, "tp"),
        P("ep", "tp", None),
        P(None, "tp"),
        P(None, "tp"),
        P("tp", None),
    )
    out_specs = (P(("ep", "tp"), None), P(("ep", "tp"), None))
    return jax.shard_map(shards, mesh=mesh, in_specs=in_specs, out_specs=out_specs, check_vma=False)
```

```python
import math

import jax
import jax.numpy as jnp
import numpy as np
from jax import lax
from jax.experimental import pallas as pl
from jax.experimental.pallas import tpu as pltpu
from jax.sharding import PartitionSpec as P

HEADS = 8
CONTENT = 64
ROTARY = 32
VALUE = 64


norm_eps = 1e-06
rope_base = 10000.0


def rms_rows(entries, gain_row):
    widened = entries.astype(jnp.float32)
    return widened * lax.rsqrt(jnp.mean(widened * widened, -1, keepdims=True) + norm_eps) * gain_row


def turn_pairs(entries, positions):
    width_full = entries.shape[-1]
    frequency = rope_base ** (-jnp.arange(width_full // 2, dtype=jnp.float32) * 2.0 / width_full)
    angles = positions.astype(jnp.float32)[:, None] * frequency[None, :]
    cosine = jnp.cos(angles)[:, None, :]
    sine_part = jnp.sin(angles)[:, None, :]
    even_part = entries[..., 0::2]
    odd_part = entries[..., 1::2]
    joined = jnp.stack(
        [even_part * cosine - odd_part * sine_part, even_part * sine_part + odd_part * cosine], -1
    )
    return joined.reshape(entries.shape)


def absorb_block(carried, query_part, query_turn, key_part, key_turn, value_rows, score_scale):
    running_peak, running_total, summed = carried
    scores = jnp.einsum("qhc,khc->qhk", query_part, key_part, preferred_element_type=jnp.float32)
    scores = scores + jnp.einsum(
        "qhr,kr->qhk", query_turn, key_turn, preferred_element_type=jnp.float32
    )
    scores = scores * score_scale
    new_peak = jnp.maximum(running_peak, jnp.max(scores, -1))
    factor = jnp.exp(running_peak - new_peak)
    weights = jnp.exp(scores - new_peak[..., None])
    running_total = running_total * factor + jnp.sum(weights, -1)
    summed = summed * factor[..., None] + jnp.einsum(
        "qhk,khv->qhv", weights.astype(jnp.bfloat16), value_rows, preferred_element_type=jnp.float32
    )
    return (new_peak, running_total, summed)


def absorb_piece(carried, query_part, query_turn, key_part, key_turn, value_rows, score_scale):
    row_count = key_part.shape[0]
    key_block = math.gcd(row_count, 2048)
    if key_block == row_count:
        return absorb_block(
            carried, query_part, query_turn, key_part, key_turn, value_rows, score_scale
        )
    block_count = row_count // key_block

    def advance(state, pieces):
        return (
            absorb_block(
                state, query_part, query_turn, pieces[0], pieces[1], pieces[2], score_scale
            ),
            None,
        )

    stacked = (
        key_part.reshape((block_count, key_block) + key_part.shape[1:]),
        key_turn.reshape(block_count, key_block, key_turn.shape[1]),
        value_rows.reshape((block_count, key_block) + value_rows.shape[1:]),
    )
    carried, ignored = lax.scan(advance, carried, stacked)
    return carried


def expand_keys(latent_rows, key_columns, value_columns, head_local):
    row_count = latent_rows.shape[0]
    key_part = (
        jnp.dot(latent_rows, key_columns, preferred_element_type=jnp.float32)
        .astype(jnp.bfloat16)
        .reshape(row_count, head_local, CONTENT)
    )
    value_rows = (
        jnp.dot(latent_rows, value_columns, preferred_element_type=jnp.float32)
        .astype(jnp.bfloat16)
        .reshape(row_count, head_local, VALUE)
    )
    return (key_part, value_rows)


def expert_terms(row_block, gate_weight, up_weight, down_weight):
    gated = jnp.einsum("secd,edf->secf", row_block, gate_weight, preferred_element_type=jnp.float32)
    lifted = jnp.einsum("secd,edf->secf", row_block, up_weight, preferred_element_type=jnp.float32)
    hidden = (jax.nn.silu(gated) * lifted).astype(jnp.bfloat16)
    return jnp.einsum("secf,efd->secd", hidden, down_weight, preferred_element_type=jnp.float32)


def shared_terms(row_block, gate_weight, up_weight, down_weight):
    gated = jnp.dot(row_block, gate_weight, preferred_element_type=jnp.float32)
    lifted = jnp.dot(row_block, up_weight, preferred_element_type=jnp.float32)
    hidden = (jax.nn.silu(gated) * lifted).astype(jnp.bfloat16)
    return jnp.dot(hidden, down_weight, preferred_element_type=jnp.float32)


def shards_plain(
    query_latent,
    key_latent,
    rotary_key,
    query_gain,
    latent_gain,
    query_content,
    query_rotary,
    key_content,
    value_weight,
    output_weight,
    expert_input,
    norm_gain,
    routes,
    route_weight,
    expert_gate,
    expert_up,
    expert_down,
    shared_gate,
    shared_up,
    shared_down,
):
    group_size = lax.axis_size("tp")
    expert_groups = lax.axis_size("ep")
    own_rows = query_latent.shape[0]
    head_local = HEADS // group_size
    head_index = lax.axis_index("tp")
    group_rows_count = own_rows * group_size
    group_start = lax.axis_index("ep") * group_rows_count
    own_start = group_start + head_index * own_rows
    score_scale = (CONTENT + ROTARY) ** (-0.5)
    query_normed = rms_rows(query_latent, query_gain).astype(jnp.bfloat16)
    latent_normed = rms_rows(key_latent, latent_gain).astype(jnp.bfloat16)
    own_positions = own_start + jnp.arange(own_rows, dtype=jnp.int32)
    key_turned = turn_pairs(rotary_key.astype(jnp.float32)[:, None, :], own_positions)[
        :, 0, :
    ].astype(jnp.bfloat16)
    token_rows = expert_input.shape[0]
    picks = routes.shape[1]
    local_experts = expert_gate.shape[0]
    expert_total = local_experts * expert_groups
    capacity = 2 * token_rows * picks // expert_total
    slot_total = expert_total * capacity
    model_width = expert_input.shape[1]
    expert_normed = rms_rows(expert_input, norm_gain).astype(jnp.bfloat16)
    flat_routes = routes.reshape(-1)
    marks = (flat_routes[:, None] == jnp.arange(expert_total, dtype=jnp.int32)[None, :]).astype(
        jnp.int32
    )
    ranks = jnp.sum((jnp.cumsum(marks, 0) - marks) * marks, 1)
    targets = flat_routes * capacity + ranks
    picker = (jnp.arange(slot_total, dtype=jnp.int32)[:, None] == targets[None, :]).astype(
        jnp.int32
    )
    picker = jnp.sum(picker.reshape(slot_total, token_rows, picks), 2).astype(jnp.bfloat16)
    outgoing = jnp.dot(picker, expert_normed, preferred_element_type=jnp.float32).astype(
        jnp.bfloat16
    )
    outgoing = outgoing.reshape(expert_groups, local_experts, capacity, model_width)
    received = lax.all_to_all(outgoing, "ep", split_axis=0, concat_axis=0, tiled=True)
    group_query, group_latent, group_turn, gathered_rows, gathered_tokens = (
        lax.all_gather(query_normed, "tp", axis=0, tiled=True),
        lax.all_gather(latent_normed, "tp", axis=0, tiled=True),
        lax.all_gather(key_turned, "tp", axis=0, tiled=True),
        lax.all_gather(received, "tp", axis=0, tiled=True),
        lax.all_gather(expert_normed, "tp", axis=0, tiled=True),
    )
    positions = group_start + jnp.arange(group_rows_count, dtype=jnp.int32)
    content_columns = lax.dynamic_slice_in_dim(
        query_content, head_index * head_local * CONTENT, head_local * CONTENT, 1
    )
    rotary_columns = lax.dynamic_slice_in_dim(
        query_rotary, head_index * head_local * ROTARY, head_local * ROTARY, 1
    )
    query_part = (
        jnp.dot(group_query, content_columns, preferred_element_type=jnp.float32)
        .astype(jnp.bfloat16)
        .reshape(group_rows_count, head_local, CONTENT)
    )
    query_turn = turn_pairs(
        jnp.dot(group_query, rotary_columns, preferred_element_type=jnp.float32).reshape(
            group_rows_count, head_local, ROTARY
        ),
        positions,
    ).astype(jnp.bfloat16)
    key_columns = lax.dynamic_slice_in_dim(
        key_content, head_index * head_local * CONTENT, head_local * CONTENT, 1
    )
    value_columns = lax.dynamic_slice_in_dim(
        value_weight, head_index * head_local * VALUE, head_local * VALUE, 1
    )
    carry_start = (
        jnp.full((group_rows_count, head_local), -jnp.inf, jnp.float32),
        jnp.zeros((group_rows_count, head_local), jnp.float32),
        jnp.zeros((group_rows_count, head_local, VALUE), jnp.float32),
    )
    key_part, value_rows = expand_keys(
        lax.all_gather(group_latent, "ep", axis=0, tiled=True),
        key_columns,
        value_columns,
        head_local,
    )
    running_peak, running_total, summed = absorb_piece(
        carry_start,
        query_part,
        query_turn,
        key_part,
        lax.all_gather(group_turn, "ep", axis=0, tiled=True),
        value_rows,
        score_scale,
    )
    attended = (
        (summed / running_total[..., None])
        .astype(jnp.bfloat16)
        .reshape(group_rows_count, head_local * VALUE)
    )
    routed_term = expert_terms(gathered_rows, expert_gate, expert_up, expert_down)
    shared_term = shared_terms(gathered_tokens, shared_gate, shared_up, shared_down)
    mixer_term = jnp.dot(attended, output_weight, preferred_element_type=jnp.float32)
    mixer_sum, routed_sum, shared_sum = (
        lax.psum_scatter(
            mixer_term.astype(jnp.bfloat16), "tp", scatter_dimension=0, tiled=True
        ).astype(jnp.float32),
        lax.psum_scatter(
            routed_term.astype(jnp.bfloat16), "tp", scatter_dimension=0, tiled=True
        ).astype(jnp.float32),
        lax.psum_scatter(
            shared_term.astype(jnp.bfloat16), "tp", scatter_dimension=0, tiled=True
        ).astype(jnp.float32),
    )
    mixer_out = mixer_sum.astype(jnp.bfloat16)
    returned = lax.all_to_all(
        routed_sum.astype(jnp.bfloat16), "ep", split_axis=0, concat_axis=0, tiled=True
    )
    returned = returned.reshape(slot_total, model_width)
    picked = jnp.take(returned, targets, axis=0).reshape(token_rows, picks, model_width)
    combined = jnp.sum(route_weight[..., None] * picked.astype(jnp.float32), 1) + shared_sum
    expert_out = combined.astype(jnp.bfloat16)
    return (mixer_out, expert_out)


MESH = pl.DeviceIdType.MESH
VMEM_LIMIT = 60 * 1024 * 1024
NEAR = 4


def fits_kernel(ep_count, slot_rows):
    return ep_count == 2 * NEAR and NEAR * slot_rows % 128 == 0


def flip(place, bits, width=3):
    flipped = place
    for power in range(width):
        bit = 2**power
        flipped = flipped + bit * (bits // bit % 2) * (1 - 2 * (place // bit % 2))
    return flipped


def greet(ep_count, me, head_index):
    barrier = pltpu.get_barrier_semaphore()
    for step in range(1, ep_count):
        pl.semaphore_signal(
            barrier, inc=1, device_id=(flip(me, step), head_index), device_id_type=MESH
        )
    row, core = head_index // 2, head_index % 2
    for other in ((1 - row) * 2 + core, row * 2 + 1 - core):
        pl.semaphore_signal(barrier, inc=1, device_id=(me, other), device_id_type=MESH)
    return lambda: pl.semaphore_wait(barrier, ep_count + 1)


def gated_rows(rows, gate_weight, up_weight):
    gated = jnp.dot(rows, gate_weight, preferred_element_type=jnp.float32)
    lifted = jnp.dot(rows, up_weight, preferred_element_type=jnp.float32)
    return (gated / (1.0 + jnp.exp(-gated)) * lifted).astype(jnp.bfloat16)


def wide(entries):
    return entries.astype(jnp.float32)


def narrow(entries):
    return entries.astype(jnp.bfloat16)


def choose_slots(routes, weights, expert_total, capacity, first_slot, slot_count):
    own_rows = routes.shape[0]
    expert_lane = lax.broadcasted_iota(jnp.int32, (own_rows, expert_total), 1)
    named = [
        jnp.where(routes[:, pick : pick + 1] == expert_lane, 1.0, 0.0)
        for pick in range(routes.shape[1])
    ]
    earlier = narrow(
        jnp.where(
            lax.broadcasted_iota(jnp.int32, (own_rows, own_rows), 0)
            > lax.broadcasted_iota(jnp.int32, (own_rows, own_rows), 1),
            1.0,
            0.0,
        )
    )
    ahead = jnp.dot(earlier, narrow(sum(named)), preferred_element_type=jnp.float32)
    slot_lane = lax.broadcasted_iota(jnp.int32, (own_rows, slot_count), 1) + first_slot
    picker = jnp.zeros(slot_lane.shape, jnp.float32)
    weight = jnp.zeros(slot_lane.shape, jnp.float32)
    for pick, marks in enumerate(named):
        rank = jnp.sum(ahead * marks, 1, keepdims=True).astype(jnp.int32)
        chosen = slot_lane == routes[:, pick : pick + 1] * capacity + rank
        picker = jnp.where(chosen, 1.0, picker)
        weight = jnp.where(chosen, weights[:, pick : pick + 1], weight)
    return narrow(picker.T), weight


def store_split(target, weight):
    own_rows = weight.shape[0]
    high = narrow(weight)
    rest = weight - wide(high)
    middle = narrow(rest)
    target[:own_rows] = high
    target[own_rows : 2 * own_rows] = middle
    target[2 * own_rows :] = narrow(rest - wide(middle))


def weighted_rows(split_weight, entries):
    picked = jnp.dot(split_weight, entries, preferred_element_type=jnp.float32)
    own_rows = picked.shape[0] // 3
    return picked[:own_rows] + picked[own_rows : 2 * own_rows] + picked[2 * own_rows :]


def block_kernel(
    ep_count,
    capacity,
    query_latent_hbm,
    key_latent_hbm,
    rotary_key_hbm,
    query_gain_hbm,
    latent_gain_hbm,
    expert_input_hbm,
    norm_gain_hbm,
    routes_hbm,
    route_weight_hbm,
    frequency_hbm,
    query_content_hbm,
    query_rotary_hbm,
    key_content_hbm,
    value_weight_hbm,
    output_weight_hbm,
    gate_hbm,
    up_hbm,
    down_hbm,
    shared_gate_hbm,
    shared_up_hbm,
    shared_down_hbm,
    both_out,
    query_latent_ref,
    key_latent_ref,
    rotary_key_ref,
    query_gain_ref,
    latent_gain_ref,
    expert_input_ref,
    norm_gain_ref,
    routes_ref,
    route_weight_ref,
    frequency_ref,
    cosine_ref,
    sine_ref,
    slots_ref,
    peer_slots_ref,
    query_columns_ref,
    latent_columns_ref,
    output_weight_ref,
    weight_ref,
    peer_weight_ref,
    rows,
    latents,
    tokens,
    queries,
    gate_ref,
    up_ref,
    down_ref,
    shared_gate_ref,
    shared_up_ref,
    shared_down_ref,
    keys,
    values,
    query_wide,
    attended,
    part,
    half_rows,
    far_rows,
    returned,
    returned_peer,
    mixed,
    half_mixed,
    far_mixed,
    shared,
    half_shared,
    far_shared,
    info_ref,
    peer_info_ref,
    own_sum,
    own_stats,
    sent_sum,
    far_sum,
    ep_send,
    ep_recv,
    y_send,
    y_recv,
    core_send,
    core_recv,
    cross_send,
    cross_recv,
    peer_send,
    peer_recv,
    back_send,
    back_recv,
    far_send,
    far_recv,
    half_send,
    half_recv,
    side_send,
    side_recv,
    own_sem,
    weight_sem,
    input_sem,
):
    me = lax.axis_index("ep")
    head_index = lax.axis_index("tp")
    row, core = head_index // 2, head_index % 2
    y_peer = (me, (1 - row) * 2 + core)
    core_peer = (me, row * 2 + 1 - core)
    local_experts = gate_ref.shape[0]
    width = rows.shape[-1]
    own_rows = tokens.shape[2]
    slot_rows = rows.shape[3]
    group_rows = attended.shape[0]
    picks = routes_ref.shape[0]
    stripe = math.gcd(width, 512)
    far_steps = range(NEAR, ep_count)
    outermost = 1 - (me // 2 + me // 4) % 2
    chunks = (NEAR + 2 * (1 - outermost), NEAR + 2 * outermost)
    greeted = greet(ep_count, me, head_index)
    arguments = [
        pltpu.make_async_copy(source, target, input_sem.at[place])
        for place, (source, target) in enumerate(
            (
                (key_latent_hbm, key_latent_ref),
                (rotary_key_hbm, rotary_key_ref),
                (latent_gain_hbm, latent_gain_ref),
                (frequency_hbm, frequency_ref),
                (expert_input_hbm, expert_input_ref),
                (norm_gain_hbm, norm_gain_ref),
                (routes_hbm, routes_ref),
                (route_weight_hbm, route_weight_ref),
                (query_latent_hbm, query_latent_ref),
                (query_gain_hbm, query_gain_ref),
            )
        )
    ]
    for argument in arguments:
        argument.start()
    near_place = me % NEAR

    def peer(step):
        return (flip(me, step), head_index)

    def remote(source, target, send_sem, recv_sem, device):
        return pltpu.make_async_remote_copy(
            src_ref=source,
            dst_ref=target,
            send_sem=send_sem,
            recv_sem=recv_sem,
            device_id=device,
            device_id_type=MESH,
        )

    head_lanes = attended.shape[1]
    heads = head_lanes // VALUE
    fetch_list = []
    for side in range(2):
        side_index = (row if side == 0 else 1 - row) * 2 + core
        columns = pl.ds(pl.multiple_of(side_index * head_lanes, head_lanes), head_lanes)
        turn_columns = pl.ds(pl.multiple_of(side_index * heads * ROTARY // 128 * 128, 128), 128)
        fetch_list += [
            (query_content_hbm.at[:, columns], query_columns_ref.at[side, :, :head_lanes]),
            (query_rotary_hbm.at[:, turn_columns], query_columns_ref.at[side, :, head_lanes:]),
            (key_content_hbm.at[:, columns], latent_columns_ref.at[side, :, :head_lanes]),
            (value_weight_hbm.at[:, columns], latent_columns_ref.at[side, :, head_lanes:]),
        ]
    fetch_list += [
        (output_weight_hbm, output_weight_ref),
        (shared_gate_hbm, shared_gate_ref),
        (shared_up_hbm, shared_up_ref),
        (shared_down_hbm, shared_down_ref),
        (gate_hbm, gate_ref),
        (up_hbm, up_ref),
        (down_hbm, down_ref),
    ]
    fetches = [
        pltpu.make_async_copy(source, target, weight_sem.at[place])
        for place, (source, target) in enumerate(fetch_list)
    ]
    for fetch in fetches:
        fetch.start()

    def turn(entries, cosine, sine):
        lane = lax.broadcasted_iota(jnp.int32, entries.shape, 1)
        crossed = jnp.where(
            lane % 2 == 0, -pltpu.roll(entries, 127, 1), pltpu.roll(entries, 1, 1)
        )
        return narrow(entries * cosine + crossed * sine)

    def angles(first, count):
        places = first + lax.broadcasted_iota(jnp.int32, (count, 128), 0)
        return places.astype(jnp.float32) * frequency_ref[...]

    for argument in arguments[:4]:
        argument.wait()
    rank_width = key_latent_ref.shape[1]
    latents[core, 0, :, :rank_width] = narrow(rms_rows(key_latent_ref[...], latent_gain_ref[...]))
    repeats = narrow(
        jnp.where(
            lax.broadcasted_iota(jnp.int32, (ROTARY, 128), 0)
            == lax.broadcasted_iota(jnp.int32, (ROTARY, 128), 1) % ROTARY,
            1.0,
            0.0,
        )
    )
    own_angles = angles((me * 4 + head_index) * own_rows, own_rows)
    latents[core, 0, :, rank_width:] = turn(
        lax.dot_general(
            rotary_key_ref[...],
            repeats,
            (((0,), (0,)), ((), ())),
            preferred_element_type=jnp.float32,
        ),
        jnp.cos(own_angles),
        jnp.sin(own_angles),
    )
    for argument in arguments[4:]:
        argument.wait()
    expert_normed = narrow(rms_rows(expert_input_ref[...], norm_gain_ref[...]))
    tokens[row, core] = expert_normed
    queries[row, core] = narrow(rms_rows(query_latent_ref[...], query_gain_ref[...]))
    info_ref[...] = jnp.zeros(info_ref.shape, jnp.float32)
    info_ref[:picks, :own_rows] = routes_ref[...].astype(jnp.float32)
    info_ref[picks : 2 * picks, :own_rows] = route_weight_ref[...]
    greeted()

    def latent_ep(step):
        if step % 2 == 0:
            return remote(
                latents.at[core, 0],
                latents.at[core, step],
                ep_send.at[1, step],
                ep_recv.at[1, step],
                peer(step),
            )
        return remote(
            latents.at[core, step - 1],
            latents.at[core, step],
            ep_send.at[1, step],
            ep_recv.at[1, step],
            peer(1),
        )

    def latent_core(step):
        return remote(
            latents.at[core, step],
            latents.at[core, step],
            core_send.at[1, step],
            core_recv.at[1, step],
            core_peer,
        )

    def slots_ep(step):
        return remote(
            slots_ref.at[flip(me, step)],
            rows.at[row, core, step],
            ep_send.at[0, step],
            ep_recv.at[0, step],
            peer(step),
        )

    def peer_slots_ep(step):
        return remote(
            peer_slots_ref.at[flip(near_place, step)],
            rows.at[1 - row, core, step],
            peer_send.at[0, step],
            peer_recv.at[0, step],
            peer(step),
        )

    routes_of = {
        "y": (row, y_send, y_recv, y_peer),
        "core": (row, core_send, core_recv, core_peer),
        "cross": (1 - row, cross_send, cross_recv, core_peer),
    }

    def moved_rows(step, route):
        origin_row, send_sem, recv_sem, device = routes_of[route]
        block = rows.at[origin_row, core, step]
        source = block
        if isinstance(step, int) and step == 0:
            source = peer_slots_ref.at[near_place] if route == "cross" else slots_ref.at[me]
        return remote(source, block, send_sem.at[0, step], recv_sem.at[0, step], device)

    def moved(buffer, place, route):
        origin_row, send_sem, recv_sem, device = routes_of[route]
        block = buffer.at[origin_row, core]
        return remote(
            block, block, send_sem.at[place, ep_count], recv_sem.at[place, ep_count], device
        )

    info_y = remote(
        info_ref, peer_info_ref, y_send.at[0, 0], y_recv.at[0, 0], y_peer
    )
    for step in (6, 4, 2, 1):
        latent_ep(step).start()
    latent_core(0).start()
    info_y.start()
    for route in ("y", "core"):
        moved(tokens, 0, route).start()
    for route in ("y", "core"):
        moved(queries, 1, route).start()
    expert_total = local_experts * ep_count
    picker, weight = choose_slots(
        routes_ref[...].T, route_weight_ref[...].T, expert_total, capacity, 0, ep_count * slot_rows
    )
    store_split(weight_ref, weight)

    def fill(target, chooser, origin_row):
        for start in range(0, width, stripe):
            target[:, :, start : start + stripe] = narrow(
                jnp.dot(
                    chooser,
                    tokens[origin_row, core, :, start : start + stripe],
                    preferred_element_type=jnp.float32,
                )
            ).reshape(target.shape[0], slot_rows, stripe)

    fill(slots_ref, picker, row)
    @pl.when(outermost == 0)
    def _():
        for step in (6, 4, 7, 5):
            slots_ep(step).start()

    for step in (2, 3):
        slots_ep(step).start()
    own_slots = pltpu.make_async_copy(slots_ref.at[me], rows.at[row, core, 0], own_sem.at[0])
    own_slots.start()
    moved_rows(0, "core").start()
    group_angles = angles(me * group_rows, group_rows)
    cosine_ref[...] = jnp.cos(group_angles)
    sine_ref[...] = jnp.sin(group_angles)

    def pass_latents(steps):
        for step in steps:
            latent_ep(step).wait_recv()
            if step % 2 == 0:
                latent_ep(step + 1).start()
            latent_core(step).start()

    info_y.wait_recv()
    peer_picker, peer_weight = choose_slots(
        peer_info_ref[:picks, :own_rows].T.astype(jnp.int32),
        peer_info_ref[picks : 2 * picks, :own_rows].T,
        expert_total,
        capacity,
        me // NEAR * NEAR * slot_rows,
        NEAR * slot_rows,
    )
    store_split(peer_weight_ref, peer_weight)
    pass_latents(range(2, ep_count, 2))
    slots_ep(1).start()
    moved(tokens, 0, "y").wait_recv()
    moved(tokens, 0, "cross").start()
    fill(peer_slots_ref, peer_picker, 1 - row)
    for step in range(1, NEAR):
        peer_slots_ep(step).start()
    peer_own = pltpu.make_async_copy(
        peer_slots_ref.at[near_place], rows.at[1 - row, core, 0], own_sem.at[1]
    )
    peer_own.start()
    moved_rows(0, "cross").start()
    def project():
        for fetch in fetches[:8]:
            fetch.wait()
        query_rows = queries[...].reshape(group_rows, queries.shape[-1])
        for side in range(2):
            projected = jnp.dot(
                query_rows, query_columns_ref[side], preferred_element_type=jnp.float32
            )
            query_wide[side, :, :head_lanes] = narrow(projected[:, :head_lanes])
            query_wide[side, :, head_lanes:] = turn(
                projected[:, head_lanes:], cosine_ref[...], sine_ref[...]
            )
        for block in range(2):
            packed = latents[block].reshape(ep_count * own_rows, latents.shape[-1])
            span = slice(block * ep_count * own_rows, (block + 1) * ep_count * own_rows)
            for side in range(2):
                expanded = narrow(
                    jnp.dot(
                        packed[:, :rank_width],
                        latent_columns_ref[side],
                        preferred_element_type=jnp.float32,
                    )
                )
                keys[side, span, :head_lanes] = expanded[:, :head_lanes]
                keys[side, span, head_lanes:] = packed[:, rank_width:]
                values[side, span, :] = expanded[:, head_lanes:]

    block_rows = group_rows // 2

    def attend(side, block):
        span = slice(block * block_rows, (block + 1) * block_rows)
        query_block = query_wide[side, span, :]
        lane = lax.broadcasted_iota(jnp.int32, query_block.shape, 1)
        lane_head = jnp.where(
            lane < head_lanes,
            lane // CONTENT,
            (lane - head_lanes) // ROTARY - core * heads % (128 // ROTARY),
        )
        out_lane = lax.broadcasted_iota(jnp.int32, (block_rows, head_lanes), 1)
        result = jnp.zeros((block_rows, head_lanes), jnp.float32)
        stats = jnp.zeros((block_rows, head_lanes), jnp.float32)
        for head in range(heads):
            chosen = jnp.where(lane_head == head, query_block, jnp.zeros_like(query_block))
            scores = lax.dot_general(
                chosen, keys[side], (((1,), (1,)), ((), ())), preferred_element_type=jnp.float32
            ) * ((CONTENT + ROTARY) ** (-0.5))
            peak = jnp.max(scores, -1, keepdims=True)
            weights = jnp.exp(scores - peak)
            total = jnp.sum(weights, -1, keepdims=True)
            summed = jnp.dot(narrow(weights), values[side], preferred_element_type=jnp.float32)
            result = jnp.where(out_lane // VALUE == head, summed, result)
            stats = jnp.where(out_lane == 2 * head, peak, stats)
            stats = jnp.where(out_lane == 2 * head + 1, total, stats)
        if side == 0:
            own_sum[span, :] = result
            own_stats[span, :] = stats
        else:
            sent_sum[span, :] = result
            sent_sum[group_rows + 8 * block : group_rows + 8 * block + 8, :] = stats.T[:8]

    sum_y = remote(sent_sum, far_sum, y_send.at[1, 0], y_recv.at[1, 0], y_peer)

    def merge():
        sum_y.wait_recv()
        out_lane = lax.broadcasted_iota(jnp.int32, (block_rows, head_lanes), 1)
        for block in range(2):
            span = slice(block * block_rows, (block + 1) * block_rows)
            here = own_stats[span, :]
            there = far_sum[group_rows + 8 * block : group_rows + 8 * block + 8, :].T
            result = jnp.zeros((block_rows, head_lanes), jnp.float32)
            for head in range(heads):
                peak_here, total_here = here[:, 2 * head : 2 * head + 1], here[:, 2 * head + 1 : 2 * head + 2]
                peak_there, total_there = there[:, 2 * head : 2 * head + 1], there[:, 2 * head + 1 : 2 * head + 2]
                peak = jnp.maximum(peak_here, peak_there)
                factor_here = jnp.exp(peak_here - peak)
                factor_there = jnp.exp(peak_there - peak)
                total = total_here * factor_here + total_there * factor_there
                summed = own_sum[span, :] * factor_here + far_sum[span, :] * factor_there
                result = jnp.where(out_lane // VALUE == head, summed / total, result)
            attended[span, :] = narrow(result)

    def mix():
        fetches[8].wait()
        for start in range(0, width, stripe):
            product = narrow(
                jnp.dot(
                    attended[...],
                    output_weight_ref[:, start : start + stripe],
                    preferred_element_type=jnp.float32,
                )
            )
            mixed[:, :, :, start : start + stripe] = product.reshape(2, 2, own_rows, stripe)

    def share():
        for fetch in fetches[9:12]:
            fetch.wait()
        for route in ("core", "cross"):
            moved(tokens, 0, route).wait_recv()
        hidden = gated_rows(
            tokens[...].reshape(group_rows, width), shared_gate_ref[...], shared_up_ref[...]
        )
        for start in range(0, width, stripe):
            product = narrow(
                jnp.dot(
                    hidden,
                    shared_down_ref[:, start : start + stripe],
                    preferred_element_type=jnp.float32,
                )
            )
            shared[:, :, :, start : start + stripe] = product.reshape(2, 2, own_rows, stripe)

    shared_half = remote(
        shared.at[:, 1 - core], half_shared, side_send.at[0], side_recv.at[0], core_peer
    )
    mixed_half = remote(
        mixed.at[:, 1 - core], half_mixed, side_send.at[1], side_recv.at[1], core_peer
    )
    shared_y = remote(
        shared.at[1 - row, core], far_shared, side_send.at[2], side_recv.at[2], y_peer
    )
    mixed_y = remote(mixed.at[1 - row, core], far_mixed, side_send.at[3], side_recv.at[3], y_peer)

    def mixed_far():
        mixed_half.wait_recv()
        mixed[1 - row, core] = narrow(wide(mixed[1 - row, core]) + wide(half_mixed[1 - row]))
        mixed_y.start()

    def arrive(step):
        slots_ep(step).wait_recv()
        moved_rows(step, "core").start()

    def arrive_peer(step):
        peer_slots_ep(step).wait_recv()
        moved_rows(step, "cross").start()

    def arrive_far(chunk, place):
        step = chunks[chunk] + place
        slots_ep(step).wait_recv()
        moved_rows(step, "y").start()
        moved_rows(step, "core").start()

    def arrive_far_peer(chunk, place):
        step = chunks[chunk] + place
        moved_rows(step, "y").wait_recv()
        moved_rows(step, "cross").start()

    def spans(expert):
        return slice(expert * capacity, (expert + 1) * capacity)

    def compute(first, count, expert):
        span = spans(expert)
        block = rows[:, :, pl.ds(first, count), span, :].reshape(4 * count * capacity, width)
        hidden = gated_rows(block, gate_ref[expert], up_ref[expert])
        for start in range(0, width, stripe):
            product = narrow(
                jnp.dot(
                    hidden,
                    down_ref[expert, :, start : start + stripe],
                    preferred_element_type=jnp.float32,
                )
            )
            part[:, :, pl.ds(first, count), span, start : start + stripe] = product.reshape(
                2, 2, count, capacity, stripe
            )

    def near_half():
        return remote(
            part.at[:, 1 - core, :NEAR],
            half_rows.at[:, :NEAR],
            half_send.at[2, 0],
            half_recv.at[2, 0],
            core_peer,
        )

    def far_half(chunk, expert):
        steps = pl.ds(chunks[chunk], 2)
        return remote(
            part.at[:, 1 - core, steps, spans(expert)],
            half_rows.at[:, steps, spans(expert)],
            half_send.at[chunk, expert],
            half_recv.at[chunk, expert],
            core_peer,
        )

    def back_near(step):
        return remote(
            part.at[row, core, step],
            returned.at[me],
            back_send.at[0, step],
            back_recv.at[0, step],
            peer(step),
        )

    def back_peer(step):
        return remote(
            part.at[1 - row, core, step],
            returned_peer.at[near_place],
            peer_send.at[1, step],
            peer_recv.at[1, step],
            peer(step),
        )

    def back_far(step, expert):
        return remote(
            part.at[row, core, step, spans(expert)],
            returned.at[me, spans(expert)],
            back_send.at[expert, step],
            back_recv.at[expert, step],
            peer(step),
        )

    def y_copy(step, expert):
        return remote(
            part.at[1 - row, core, step, spans(expert)],
            far_rows.at[step - NEAR, spans(expert)],
            far_send.at[expert, step],
            far_recv.at[expert, step],
            y_peer,
        )

    def settle_near():
        near_half().wait_recv()
        order = list(range(1, NEAR)) + [0]
        for step in order:
            outer = narrow(wide(part[1 - row, core, step]) + wide(half_rows[1 - row, step]))
            if step:
                part[1 - row, core, step] = outer
                back_peer(step).start()
            else:
                returned_peer[near_place] = outer
        for step in order:
            total = narrow(wide(part[row, core, step]) + wide(half_rows[row, step]))
            if step:
                part[row, core, step] = total
                back_near(step).start()
            else:
                returned[me] = total

    def settle_outer(chunk, expert):
        far_half(chunk, expert).wait_recv()
        span = spans(expert)
        for step in (chunks[chunk], chunks[chunk] + 1):
            part[1 - row, core, step, span] = narrow(
                wide(part[1 - row, core, step, span]) + wide(half_rows[1 - row, step, span])
            )
            y_copy(step, expert).start()

    def settle_far(chunk, expert):
        span = spans(expert)
        for step in (chunks[chunk], chunks[chunk] + 1):
            y_copy(step, expert).wait_recv()
            part[row, core, step, span] = narrow(
                wide(part[row, core, step, span])
                + wide(half_rows[row, step, span])
                + wide(far_rows[step - NEAR, span])
            )
            back_far(step, expert).start()

    def wait_rows(steps):
        for step in steps:
            for route in ("core", "cross"):
                moved_rows(step, route).wait_recv()

    def far_chunk(chunk):
        wait_rows((chunks[chunk], chunks[chunk] + 1))
        for expert in range(local_experts):
            compute(chunks[chunk], 2, expert)
            far_half(chunk, expert).start()

    def gather_latents():
        moved(queries, 1, "y").wait_recv()
        moved(queries, 1, "cross").start()
        pass_latents(range(1, ep_count, 2))

    def finish_latents():
        for route in ("core", "cross"):
            moved(queries, 1, route).wait_recv()
        for step in range(ep_count):
            latent_core(step).wait_recv()

    def near_compute():
        own_slots.wait()
        peer_own.wait()
        wait_rows(range(NEAR))
        for expert in range(local_experts):
            compute(0, NEAR, expert)
        near_half().start()

    def inner(work):
        pl.when(outermost == 0)(work)

    def outer(work):
        pl.when(outermost == 1)(work)

    def attend_peer():
        gather_latents()
        finish_latents()
        project()
        attend(1, 0)
        attend(1, 1)
        sum_y.start()

    def attend_own():
        attend(0, 0)
        attend(0, 1)
        merge()
        mix()
        mixed_half.start()

    def send_far():
        for step in (6, 4, 7, 5):
            slots_ep(step).start()

    arrive_far(0, 0)
    outer(attend_peer)
    arrive_far(0, 1)
    outer(send_far)
    outer(attend_own)
    for fetch in fetches[12:]:
        fetch.wait()
    for place in range(2):
        arrive_far_peer(0, place)
    far_chunk(0)
    for step in range(1, NEAR):
        arrive(step)
    for expert in range(local_experts):
        settle_outer(0, expert)
    for step in range(1, NEAR):
        arrive_peer(step)
    inner(attend_peer)
    inner(near_compute)
    arrive_far(1, 0)
    arrive_far(1, 1)
    outer(near_compute)
    settle_far(0, 0)
    settle_far(0, 1)
    settle_near()
    inner(attend_own)
    share()
    shared_half.start()
    for place in range(2):
        arrive_far_peer(1, place)
    mixed_far()
    far_chunk(1)
    for expert in range(local_experts):
        settle_outer(1, expert)
    for expert in range(local_experts):
        settle_far(1, expert)
    mixed_y.wait_recv()
    both_out[0] = narrow(wide(mixed[row, core]) + wide(half_mixed[row]) + wide(far_mixed[...]))
    for step in range(1, NEAR):
        back_peer(step).wait_recv()
    shared_half.wait_recv()
    for start in range(0, width, stripe):
        cut = slice(start, start + stripe)
        shared[1 - row, core, :, cut] = narrow(
            weighted_rows(
                peer_weight_ref[...],
                returned_peer[:, :, cut].reshape(NEAR * slot_rows, stripe),
            )
            + wide(shared[1 - row, core, :, cut])
            + wide(half_shared[1 - row, :, cut])
        )
    shared_y.start()
    for step in range(1, NEAR):
        back_near(step).wait_recv()
    for step in far_steps:
        for expert in range(local_experts):
            back_far(step, expert).wait_recv()
    shared_y.wait_recv()
    for start in range(0, width, stripe):
        cut = slice(start, start + stripe)
        both_out[1, :, cut] = narrow(
            weighted_rows(
                weight_ref[...], returned[:, :, cut].reshape(ep_count * slot_rows, stripe)
            )
            + wide(shared[row, core, :, cut])
            + wide(half_shared[row, :, cut])
            + wide(far_shared[:, cut])
        )

    for step in range(1, ep_count):
        latent_ep(step).wait_send()
        slots_ep(step).wait_send()
    for step in range(ep_count):
        latent_core(step).wait_send()
        for route in ("core", "cross"):
            moved_rows(step, route).wait_send()
    for step in range(1, NEAR):
        peer_slots_ep(step).wait_send()
        back_near(step).wait_send()
        back_peer(step).wait_send()
    for step in far_steps:
        moved_rows(step, "y").wait_send()
        for expert in range(local_experts):
            back_far(step, expert).wait_send()
            y_copy(step, expert).wait_send()
    for route in ("y", "core", "cross"):
        moved(queries, 1, route).wait_send()
        moved(tokens, 0, route).wait_send()
    for chunk in range(2):
        for expert in range(local_experts):
            far_half(chunk, expert).wait_send()
    for copy in (info_y, sum_y, near_half(), shared_half, mixed_half, shared_y, mixed_y):
        copy.wait_send()


def block_call(ep_count, capacity, *operands):
    query_latent, key_latent = operands[:2]
    own_rows, width = operands[5].shape
    head_lanes = operands[14].shape[0]
    local_experts = operands[15].shape[0]
    slot_rows = local_experts * capacity
    latent_shape = (own_rows, key_latent.shape[1] + 128)
    anywhere = pl.BlockSpec(memory_space=pl.ANY)

    def held(*shape):
        return pltpu.VMEM(shape, jnp.bfloat16)

    def precise(*shape):
        return pltpu.VMEM(shape, jnp.float32)

    def sems(*shape):
        return pltpu.SemaphoreType.DMA(shape)

    group_rows = 4 * own_rows
    key_rows = 2 * ep_count * own_rows
    row_block = (slot_rows, width)
    side = (own_rows, width)
    return pl.pallas_call(
        lambda *refs: block_kernel(ep_count, capacity, *refs),
        out_shape=jax.ShapeDtypeStruct((2,) + side, jnp.bfloat16),
        in_specs=[anywhere] * 21,
        out_specs=pl.BlockSpec(memory_space=pltpu.VMEM),
        scratch_shapes=[pltpu.VMEM(operand.shape, operand.dtype) for operand in operands[:10]]
        + [
            precise(group_rows, 128),
            precise(group_rows, 128),
            held(ep_count, *row_block),
            held(NEAR, *row_block),
            held(2, query_latent.shape[1], head_lanes + 128),
            held(2, key_latent.shape[1], 2 * head_lanes),
            held(head_lanes, width),
            held(3 * own_rows, ep_count * slot_rows),
            held(3 * own_rows, NEAR * slot_rows),
            held(2, 2, ep_count, *row_block),
            held(2, ep_count, *latent_shape),
            held(2, 2, *side),
            held(2, 2, *query_latent.shape),
        ]
        + [held(*operand.shape) for operand in operands[15:]]
        + [
            held(2, key_rows, head_lanes + 128),
            held(2, key_rows, head_lanes),
            held(2, group_rows, head_lanes + 128),
            held(group_rows, head_lanes),
            held(2, 2, ep_count, *row_block),
            held(2, ep_count, *row_block),
            held(ep_count - NEAR, *row_block),
            held(ep_count, *row_block),
            held(NEAR, *row_block),
            held(2, 2, *side),
            held(2, *side),
            held(*side),
            held(2, 2, *side),
            held(2, *side),
            held(*side),
            precise(8, 128),
            precise(8, 128),
            precise(group_rows, head_lanes),
            precise(group_rows, head_lanes),
            precise(group_rows + 16, head_lanes),
            precise(group_rows + 16, head_lanes),
        ]
        + [sems(2, ep_count + 1)] * 8
        + [sems(2, NEAR)] * 2
        + [sems(local_experts, ep_count)] * 4
        + [sems(3, local_experts)] * 2
        + [sems(4)] * 2
        + [sems(2), sems(15), sems(10)],
        compiler_params=pltpu.CompilerParams(
            collective_id=0, has_side_effects=True, vmem_limit_bytes=VMEM_LIMIT
        ),
        name="block",
    )(*operands)


def shards(
    query_latent,
    key_latent,
    rotary_key,
    query_gain,
    latent_gain,
    query_content,
    query_rotary,
    key_content,
    value_weight,
    output_weight,
    expert_input,
    norm_gain,
    routes,
    route_weight,
    expert_gate,
    expert_up,
    expert_down,
    shared_gate,
    shared_up,
    shared_down,
):
    group_size = lax.axis_size("tp")
    expert_groups = lax.axis_size("ep")
    token_rows = expert_input.shape[0]
    picks = routes.shape[1]
    local_experts = expert_gate.shape[0]
    expert_total = local_experts * expert_groups
    capacity = 2 * token_rows * picks // expert_total
    if group_size != 4 or capacity % 16 or not fits_kernel(expert_groups, local_experts * capacity):
        return shards_plain(
            query_latent,
            key_latent,
            rotary_key,
            query_gain,
            latent_gain,
            query_content,
            query_rotary,
            key_content,
            value_weight,
            output_weight,
            expert_input,
            norm_gain,
            routes,
            route_weight,
            expert_gate,
            expert_up,
            expert_down,
            shared_gate,
            shared_up,
            shared_down,
        )
    frequency = rope_base ** (-np.arange(ROTARY // 2) * 2.0 / ROTARY)
    both = block_call(
        expert_groups,
        capacity,
        query_latent,
        key_latent,
        rotary_key.T,
        query_gain[None, :],
        latent_gain[None, :],
        expert_input,
        norm_gain[None, :],
        routes.T,
        route_weight.T,
        jnp.asarray(np.tile(np.repeat(frequency, 2), 128 // ROTARY)[None, :], jnp.float32),
        query_content,
        query_rotary,
        key_content,
        value_weight,
        output_weight,
        expert_gate,
        expert_up,
        expert_down,
        shared_gate,
        shared_up,
        shared_down,
    )
    return (both[0], both[1])


def solution(mesh):
    in_specs = (
        P(("ep", "tp"), None),
        P(("ep", "tp"), None),
        P(("ep", "tp"), None),
        P(),
        P(),
        P(),
        P(),
        P(),
        P(),
        P("tp", None),
        P(("ep", "tp"), None),
        P(),
        P(("ep", "tp"), None),
        P(("ep", "tp"), None),
        P("ep", None, "tp"),
        P("ep", None, "tp"),
        P("ep", "tp", None),
        P(None, "tp"),
        P(None, "tp"),
        P("tp", None),
    )
    out_specs = (P(("ep", "tp"), None), P(("ep", "tp"), None))
    return jax.shard_map(shards, mesh=mesh, in_specs=in_specs, out_specs=out_specs, check_vma=False)
```

```python
import math

import jax
import jax.numpy as jnp
import numpy as np
from jax import lax
from jax.experimental import pallas as pl
from jax.experimental.pallas import tpu as pltpu
from jax.sharding import PartitionSpec as P

HEADS = 8
CONTENT = 64
ROTARY = 32
VALUE = 64


norm_eps = 1e-06
rope_base = 10000.0


def rms_rows(entries, gain_row):
    widened = entries.astype(jnp.float32)
    return widened * lax.rsqrt(jnp.mean(widened * widened, -1, keepdims=True) + norm_eps) * gain_row


def turn_pairs(entries, positions):
    width_full = entries.shape[-1]
    frequency = rope_base ** (-jnp.arange(width_full // 2, dtype=jnp.float32) * 2.0 / width_full)
    angles = positions.astype(jnp.float32)[:, None] * frequency[None, :]
    cosine = jnp.cos(angles)[:, None, :]
    sine_part = jnp.sin(angles)[:, None, :]
    even_part = entries[..., 0::2]
    odd_part = entries[..., 1::2]
    joined = jnp.stack(
        [even_part * cosine - odd_part * sine_part, even_part * sine_part + odd_part * cosine], -1
    )
    return joined.reshape(entries.shape)


def absorb_block(carried, query_part, query_turn, key_part, key_turn, value_rows, score_scale):
    running_peak, running_total, summed = carried
    scores = jnp.einsum("qhc,khc->qhk", query_part, key_part, preferred_element_type=jnp.float32)
    scores = scores + jnp.einsum(
        "qhr,kr->qhk", query_turn, key_turn, preferred_element_type=jnp.float32
    )
    scores = scores * score_scale
    new_peak = jnp.maximum(running_peak, jnp.max(scores, -1))
    factor = jnp.exp(running_peak - new_peak)
    weights = jnp.exp(scores - new_peak[..., None])
    running_total = running_total * factor + jnp.sum(weights, -1)
    summed = summed * factor[..., None] + jnp.einsum(
        "qhk,khv->qhv", weights.astype(jnp.bfloat16), value_rows, preferred_element_type=jnp.float32
    )
    return (new_peak, running_total, summed)


def absorb_piece(carried, query_part, query_turn, key_part, key_turn, value_rows, score_scale):
    row_count = key_part.shape[0]
    key_block = math.gcd(row_count, 2048)
    if key_block == row_count:
        return absorb_block(
            carried, query_part, query_turn, key_part, key_turn, value_rows, score_scale
        )
    block_count = row_count // key_block

    def advance(state, pieces):
        return (
            absorb_block(
                state, query_part, query_turn, pieces[0], pieces[1], pieces[2], score_scale
            ),
            None,
        )

    stacked = (
        key_part.reshape((block_count, key_block) + key_part.shape[1:]),
        key_turn.reshape(block_count, key_block, key_turn.shape[1]),
        value_rows.reshape((block_count, key_block) + value_rows.shape[1:]),
    )
    carried, ignored = lax.scan(advance, carried, stacked)
    return carried


def expand_keys(latent_rows, key_columns, value_columns, head_local):
    row_count = latent_rows.shape[0]
    key_part = (
        jnp.dot(latent_rows, key_columns, preferred_element_type=jnp.float32)
        .astype(jnp.bfloat16)
        .reshape(row_count, head_local, CONTENT)
    )
    value_rows = (
        jnp.dot(latent_rows, value_columns, preferred_element_type=jnp.float32)
        .astype(jnp.bfloat16)
        .reshape(row_count, head_local, VALUE)
    )
    return (key_part, value_rows)


def expert_terms(row_block, gate_weight, up_weight, down_weight):
    gated = jnp.einsum("secd,edf->secf", row_block, gate_weight, preferred_element_type=jnp.float32)
    lifted = jnp.einsum("secd,edf->secf", row_block, up_weight, preferred_element_type=jnp.float32)
    hidden = (jax.nn.silu(gated) * lifted).astype(jnp.bfloat16)
    return jnp.einsum("secf,efd->secd", hidden, down_weight, preferred_element_type=jnp.float32)


def shared_terms(row_block, gate_weight, up_weight, down_weight):
    gated = jnp.dot(row_block, gate_weight, preferred_element_type=jnp.float32)
    lifted = jnp.dot(row_block, up_weight, preferred_element_type=jnp.float32)
    hidden = (jax.nn.silu(gated) * lifted).astype(jnp.bfloat16)
    return jnp.dot(hidden, down_weight, preferred_element_type=jnp.float32)


def shards_plain(
    query_latent,
    key_latent,
    rotary_key,
    query_gain,
    latent_gain,
    query_content,
    query_rotary,
    key_content,
    value_weight,
    output_weight,
    expert_input,
    norm_gain,
    routes,
    route_weight,
    expert_gate,
    expert_up,
    expert_down,
    shared_gate,
    shared_up,
    shared_down,
):
    group_size = lax.axis_size("tp")
    expert_groups = lax.axis_size("ep")
    own_rows = query_latent.shape[0]
    head_local = HEADS // group_size
    head_index = lax.axis_index("tp")
    group_rows_count = own_rows * group_size
    group_start = lax.axis_index("ep") * group_rows_count
    own_start = group_start + head_index * own_rows
    score_scale = (CONTENT + ROTARY) ** (-0.5)
    query_normed = rms_rows(query_latent, query_gain).astype(jnp.bfloat16)
    latent_normed = rms_rows(key_latent, latent_gain).astype(jnp.bfloat16)
    own_positions = own_start + jnp.arange(own_rows, dtype=jnp.int32)
    key_turned = turn_pairs(rotary_key.astype(jnp.float32)[:, None, :], own_positions)[
        :, 0, :
    ].astype(jnp.bfloat16)
    token_rows = expert_input.shape[0]
    picks = routes.shape[1]
    local_experts = expert_gate.shape[0]
    expert_total = local_experts * expert_groups
    capacity = 2 * token_rows * picks // expert_total
    slot_total = expert_total * capacity
    model_width = expert_input.shape[1]
    expert_normed = rms_rows(expert_input, norm_gain).astype(jnp.bfloat16)
    flat_routes = routes.reshape(-1)
    marks = (flat_routes[:, None] == jnp.arange(expert_total, dtype=jnp.int32)[None, :]).astype(
        jnp.int32
    )
    ranks = jnp.sum((jnp.cumsum(marks, 0) - marks) * marks, 1)
    targets = flat_routes * capacity + ranks
    picker = (jnp.arange(slot_total, dtype=jnp.int32)[:, None] == targets[None, :]).astype(
        jnp.int32
    )
    picker = jnp.sum(picker.reshape(slot_total, token_rows, picks), 2).astype(jnp.bfloat16)
    outgoing = jnp.dot(picker, expert_normed, preferred_element_type=jnp.float32).astype(
        jnp.bfloat16
    )
    outgoing = outgoing.reshape(expert_groups, local_experts, capacity, model_width)
    received = lax.all_to_all(outgoing, "ep", split_axis=0, concat_axis=0, tiled=True)
    group_query, group_latent, group_turn, gathered_rows, gathered_tokens = (
        lax.all_gather(query_normed, "tp", axis=0, tiled=True),
        lax.all_gather(latent_normed, "tp", axis=0, tiled=True),
        lax.all_gather(key_turned, "tp", axis=0, tiled=True),
        lax.all_gather(received, "tp", axis=0, tiled=True),
        lax.all_gather(expert_normed, "tp", axis=0, tiled=True),
    )
    positions = group_start + jnp.arange(group_rows_count, dtype=jnp.int32)
    content_columns = lax.dynamic_slice_in_dim(
        query_content, head_index * head_local * CONTENT, head_local * CONTENT, 1
    )
    rotary_columns = lax.dynamic_slice_in_dim(
        query_rotary, head_index * head_local * ROTARY, head_local * ROTARY, 1
    )
    query_part = (
        jnp.dot(group_query, content_columns, preferred_element_type=jnp.float32)
        .astype(jnp.bfloat16)
        .reshape(group_rows_count, head_local, CONTENT)
    )
    query_turn = turn_pairs(
        jnp.dot(group_query, rotary_columns, preferred_element_type=jnp.float32).reshape(
            group_rows_count, head_local, ROTARY
        ),
        positions,
    ).astype(jnp.bfloat16)
    key_columns = lax.dynamic_slice_in_dim(
        key_content, head_index * head_local * CONTENT, head_local * CONTENT, 1
    )
    value_columns = lax.dynamic_slice_in_dim(
        value_weight, head_index * head_local * VALUE, head_local * VALUE, 1
    )
    carry_start = (
        jnp.full((group_rows_count, head_local), -jnp.inf, jnp.float32),
        jnp.zeros((group_rows_count, head_local), jnp.float32),
        jnp.zeros((group_rows_count, head_local, VALUE), jnp.float32),
    )
    key_part, value_rows = expand_keys(
        lax.all_gather(group_latent, "ep", axis=0, tiled=True),
        key_columns,
        value_columns,
        head_local,
    )
    running_peak, running_total, summed = absorb_piece(
        carry_start,
        query_part,
        query_turn,
        key_part,
        lax.all_gather(group_turn, "ep", axis=0, tiled=True),
        value_rows,
        score_scale,
    )
    attended = (
        (summed / running_total[..., None])
        .astype(jnp.bfloat16)
        .reshape(group_rows_count, head_local * VALUE)
    )
    routed_term = expert_terms(gathered_rows, expert_gate, expert_up, expert_down)
    shared_term = shared_terms(gathered_tokens, shared_gate, shared_up, shared_down)
    mixer_term = jnp.dot(attended, output_weight, preferred_element_type=jnp.float32)
    mixer_sum, routed_sum, shared_sum = (
        lax.psum_scatter(
            mixer_term.astype(jnp.bfloat16), "tp", scatter_dimension=0, tiled=True
        ).astype(jnp.float32),
        lax.psum_scatter(
            routed_term.astype(jnp.bfloat16), "tp", scatter_dimension=0, tiled=True
        ).astype(jnp.float32),
        lax.psum_scatter(
            shared_term.astype(jnp.bfloat16), "tp", scatter_dimension=0, tiled=True
        ).astype(jnp.float32),
    )
    mixer_out = mixer_sum.astype(jnp.bfloat16)
    returned = lax.all_to_all(
        routed_sum.astype(jnp.bfloat16), "ep", split_axis=0, concat_axis=0, tiled=True
    )
    returned = returned.reshape(slot_total, model_width)
    picked = jnp.take(returned, targets, axis=0).reshape(token_rows, picks, model_width)
    combined = jnp.sum(route_weight[..., None] * picked.astype(jnp.float32), 1) + shared_sum
    expert_out = combined.astype(jnp.bfloat16)
    return (mixer_out, expert_out)


MESH = pl.DeviceIdType.MESH
VMEM_LIMIT = 60 * 1024 * 1024
NEAR = 4


def fits_kernel(ep_count, slot_rows):
    return ep_count == 2 * NEAR and NEAR * slot_rows % 128 == 0


def flip(place, bits, width=3):
    flipped = place
    for power in range(width):
        bit = 2**power
        flipped = flipped + bit * (bits // bit % 2) * (1 - 2 * (place // bit % 2))
    return flipped


def greet(ep_count, me, head_index):
    barrier = pltpu.get_barrier_semaphore()
    for step in range(1, ep_count):
        pl.semaphore_signal(
            barrier, inc=1, device_id=(flip(me, step), head_index), device_id_type=MESH
        )
    row, core = head_index // 2, head_index % 2
    for other in ((1 - row) * 2 + core, row * 2 + 1 - core):
        pl.semaphore_signal(barrier, inc=1, device_id=(me, other), device_id_type=MESH)
    return lambda: pl.semaphore_wait(barrier, ep_count + 1)


def gated_rows(rows, gate_weight, up_weight):
    gated = jnp.dot(rows, gate_weight, preferred_element_type=jnp.float32)
    lifted = jnp.dot(rows, up_weight, preferred_element_type=jnp.float32)
    return (gated / (1.0 + jnp.exp(-gated)) * lifted).astype(jnp.bfloat16)


def wide(entries):
    return entries.astype(jnp.float32)


def narrow(entries):
    return entries.astype(jnp.bfloat16)


def choose_slots(routes, weights, expert_total, capacity, first_slot, slot_count):
    own_rows = routes.shape[0]
    expert_lane = lax.broadcasted_iota(jnp.int32, (own_rows, expert_total), 1)
    named = [
        jnp.where(routes[:, pick : pick + 1] == expert_lane, 1.0, 0.0)
        for pick in range(routes.shape[1])
    ]
    earlier = narrow(
        jnp.where(
            lax.broadcasted_iota(jnp.int32, (own_rows, own_rows), 0)
            > lax.broadcasted_iota(jnp.int32, (own_rows, own_rows), 1),
            1.0,
            0.0,
        )
    )
    ahead = jnp.dot(earlier, narrow(sum(named)), preferred_element_type=jnp.float32)
    slot_lane = lax.broadcasted_iota(jnp.int32, (own_rows, slot_count), 1) + first_slot
    picker = jnp.zeros(slot_lane.shape, jnp.float32)
    weight = jnp.zeros(slot_lane.shape, jnp.float32)
    for pick, marks in enumerate(named):
        rank = jnp.sum(ahead * marks, 1, keepdims=True).astype(jnp.int32)
        chosen = slot_lane == routes[:, pick : pick + 1] * capacity + rank
        picker = jnp.where(chosen, 1.0, picker)
        weight = jnp.where(chosen, weights[:, pick : pick + 1], weight)
    return narrow(picker.T), weight


def store_split(target, weight):
    own_rows = weight.shape[0]
    high = narrow(weight)
    rest = weight - wide(high)
    middle = narrow(rest)
    target[:own_rows] = high
    target[own_rows : 2 * own_rows] = middle
    target[2 * own_rows :] = narrow(rest - wide(middle))


def weighted_rows(split_weight, entries):
    picked = jnp.dot(split_weight, entries, preferred_element_type=jnp.float32)
    own_rows = picked.shape[0] // 3
    return picked[:own_rows] + picked[own_rows : 2 * own_rows] + picked[2 * own_rows :]


def block_kernel(
    ep_count,
    capacity,
    query_latent_hbm,
    key_latent_hbm,
    rotary_key_hbm,
    query_gain_hbm,
    latent_gain_hbm,
    expert_input_hbm,
    norm_gain_hbm,
    routes_hbm,
    route_weight_hbm,
    frequency_hbm,
    query_content_hbm,
    query_rotary_hbm,
    key_content_hbm,
    value_weight_hbm,
    output_weight_hbm,
    gate_hbm,
    up_hbm,
    down_hbm,
    shared_gate_hbm,
    shared_up_hbm,
    shared_down_hbm,
    both_out,
    query_latent_ref,
    key_latent_ref,
    rotary_key_ref,
    query_gain_ref,
    latent_gain_ref,
    expert_input_ref,
    norm_gain_ref,
    routes_ref,
    route_weight_ref,
    frequency_ref,
    cosine_ref,
    sine_ref,
    slots_ref,
    peer_slots_ref,
    query_columns_ref,
    latent_columns_ref,
    output_weight_ref,
    weight_ref,
    peer_weight_ref,
    rows,
    latents,
    tokens,
    queries,
    gate_ref,
    up_ref,
    down_ref,
    shared_gate_ref,
    shared_up_ref,
    shared_down_ref,
    keys,
    values,
    query_wide,
    attended,
    part,
    half_rows,
    far_rows,
    returned,
    returned_peer,
    mixed,
    half_mixed,
    far_mixed,
    shared,
    half_shared,
    far_shared,
    info_ref,
    peer_info_ref,
    own_sum,
    own_stats,
    sent_sum,
    far_sum,
    sent_stats,
    far_stats,
    ep_send,
    ep_recv,
    y_send,
    y_recv,
    core_send,
    core_recv,
    cross_send,
    cross_recv,
    peer_send,
    peer_recv,
    back_send,
    back_recv,
    far_send,
    far_recv,
    half_send,
    half_recv,
    side_send,
    side_recv,
    own_sem,
    weight_sem,
    input_sem,
):
    me = lax.axis_index("ep")
    head_index = lax.axis_index("tp")
    row, core = head_index // 2, head_index % 2
    y_peer = (me, (1 - row) * 2 + core)
    core_peer = (me, row * 2 + 1 - core)
    local_experts = gate_ref.shape[0]
    width = rows.shape[-1]
    own_rows = tokens.shape[2]
    slot_rows = rows.shape[3]
    group_rows = attended.shape[0]
    picks = routes_ref.shape[0]
    stripe = math.gcd(width, 512)
    far_steps = range(NEAR, ep_count)
    outermost = 1 - (me // 2 + me // 4) % 2
    chunks = (NEAR + 2 * (1 - outermost), NEAR + 2 * outermost)
    greeted = greet(ep_count, me, head_index)
    arguments = [
        pltpu.make_async_copy(source, target, input_sem.at[place])
        for place, (source, target) in enumerate(
            (
                (key_latent_hbm, key_latent_ref),
                (rotary_key_hbm, rotary_key_ref),
                (latent_gain_hbm, latent_gain_ref),
                (frequency_hbm, frequency_ref),
                (expert_input_hbm, expert_input_ref),
                (norm_gain_hbm, norm_gain_ref),
                (routes_hbm, routes_ref),
                (route_weight_hbm, route_weight_ref),
                (query_latent_hbm, query_latent_ref),
                (query_gain_hbm, query_gain_ref),
            )
        )
    ]
    for argument in arguments:
        argument.start()
    near_place = me % NEAR

    def peer(step):
        return (flip(me, step), head_index)

    def remote(source, target, send_sem, recv_sem, device):
        return pltpu.make_async_remote_copy(
            src_ref=source,
            dst_ref=target,
            send_sem=send_sem,
            recv_sem=recv_sem,
            device_id=device,
            device_id_type=MESH,
        )

    head_lanes = attended.shape[1]
    heads = head_lanes // VALUE
    fetch_list = []
    for side in range(2):
        side_index = (row if side == 0 else 1 - row) * 2 + core
        columns = pl.ds(pl.multiple_of(side_index * head_lanes, head_lanes), head_lanes)
        turn_columns = pl.ds(pl.multiple_of(side_index * heads * ROTARY // 128 * 128, 128), 128)
        fetch_list += [
            (query_content_hbm.at[:, columns], query_columns_ref.at[side, :, :head_lanes]),
            (query_rotary_hbm.at[:, turn_columns], query_columns_ref.at[side, :, head_lanes:]),
            (key_content_hbm.at[:, columns], latent_columns_ref.at[side, :, :head_lanes]),
            (value_weight_hbm.at[:, columns], latent_columns_ref.at[side, :, head_lanes:]),
        ]
    fetch_list += [
        (output_weight_hbm, output_weight_ref),
        (shared_gate_hbm, shared_gate_ref),
        (shared_up_hbm, shared_up_ref),
        (shared_down_hbm, shared_down_ref),
        (gate_hbm, gate_ref),
        (up_hbm, up_ref),
        (down_hbm, down_ref),
    ]
    fetches = [
        pltpu.make_async_copy(
            source, target, weight_sem.at[place % 4 // 2 if place < 8 else place - 6]
        )
        for place, (source, target) in enumerate(fetch_list)
    ]
    for fetch in fetches:
        fetch.start()

    def turn(entries, cosine, sine):
        lane = lax.broadcasted_iota(jnp.int32, entries.shape, 1)
        crossed = jnp.where(
            lane % 2 == 0, -pltpu.roll(entries, 127, 1), pltpu.roll(entries, 1, 1)
        )
        return narrow(entries * cosine + crossed * sine)

    def angles(first, count):
        places = first + lax.broadcasted_iota(jnp.int32, (count, 128), 0)
        return places.astype(jnp.float32) * frequency_ref[...]

    for argument in arguments[:4]:
        argument.wait()
    rank_width = key_latent_ref.shape[1]
    latents[core, 0, :, :rank_width] = narrow(rms_rows(key_latent_ref[...], latent_gain_ref[...]))
    repeats = narrow(
        jnp.where(
            lax.broadcasted_iota(jnp.int32, (ROTARY, 128), 0)
            == lax.broadcasted_iota(jnp.int32, (ROTARY, 128), 1) % ROTARY,
            1.0,
            0.0,
        )
    )
    own_angles = angles((me * 4 + head_index) * own_rows, own_rows)
    latents[core, 0, :, rank_width:] = turn(
        lax.dot_general(
            rotary_key_ref[...],
            repeats,
            (((0,), (0,)), ((), ())),
            preferred_element_type=jnp.float32,
        ),
        jnp.cos(own_angles),
        jnp.sin(own_angles),
    )
    for argument in arguments[4:]:
        argument.wait()
    expert_normed = narrow(rms_rows(expert_input_ref[...], norm_gain_ref[...]))
    tokens[row, core] = expert_normed
    queries[row, core] = narrow(rms_rows(query_latent_ref[...], query_gain_ref[...]))
    info_ref[...] = jnp.zeros(info_ref.shape, jnp.float32)
    info_ref[:picks, :own_rows] = routes_ref[...].astype(jnp.float32)
    info_ref[picks : 2 * picks, :own_rows] = route_weight_ref[...]
    greeted()

    def latent_ep(step):
        if step % 2 == 0:
            return remote(
                latents.at[core, 0],
                latents.at[core, step],
                ep_send.at[1],
                ep_recv.at[1, step],
                peer(step),
            )
        return remote(
            latents.at[core, step - 1],
            latents.at[core, step],
            ep_send.at[1],
            ep_recv.at[1, step],
            peer(1),
        )

    def latent_core(step):
        return remote(
            latents.at[core, step],
            latents.at[core, step],
            core_send.at[1],
            core_recv.at[1],
            core_peer,
        )

    def slots_ep(step):
        return remote(
            slots_ref.at[flip(me, step)],
            rows.at[row, core, step],
            ep_send.at[0],
            ep_recv.at[0, step],
            peer(step),
        )

    def peer_slots_ep(step):
        return remote(
            peer_slots_ref.at[flip(near_place, step)],
            rows.at[1 - row, core, step],
            peer_send.at[0],
            peer_recv.at[step],
            peer(step),
        )

    routes_of = {
        "y": (row, y_send, y_recv, y_peer),
        "core": (row, core_send, core_recv, core_peer),
        "cross": (1 - row, cross_send, cross_recv, core_peer),
    }

    def moved_rows(step, route, group=0):
        origin_row, send_sem, recv_sem, device = routes_of[route]
        block = rows.at[origin_row, core, step]
        source = block
        if isinstance(step, int) and step == 0:
            source = peer_slots_ref.at[near_place] if route == "cross" else slots_ref.at[me]
        place = 4 + step - NEAR if route == "y" else 4 + group
        return remote(source, block, send_sem.at[0], recv_sem.at[place], device)

    def moved(buffer, place, route):
        origin_row, send_sem, recv_sem, device = routes_of[route]
        block = buffer.at[origin_row, core]
        return remote(block, block, send_sem.at[2 + place], recv_sem.at[2 + place], device)

    info_y = remote(
        info_ref, peer_info_ref, y_send.at[1], y_recv.at[0], y_peer
    )
    for step in (6, 4, 2, 1):
        latent_ep(step).start()
    latent_core(0).start()
    info_y.start()
    for route in ("y", "core"):
        moved(tokens, 0, route).start()
    for route in ("y", "core"):
        moved(queries, 1, route).start()
    expert_total = local_experts * ep_count
    picker, weight = choose_slots(
        routes_ref[...].T, route_weight_ref[...].T, expert_total, capacity, 0, ep_count * slot_rows
    )
    store_split(weight_ref, weight)

    def fill(target, chooser, origin_row):
        for start in range(0, width, stripe):
            target[:, :, start : start + stripe] = narrow(
                jnp.dot(
                    chooser,
                    tokens[origin_row, core, :, start : start + stripe],
                    preferred_element_type=jnp.float32,
                )
            ).reshape(target.shape[0], slot_rows, stripe)

    fill(slots_ref, picker, row)
    @pl.when(outermost == 0)
    def _():
        for step in (6, 4, 7, 5):
            slots_ep(step).start()

    for step in (2, 3):
        slots_ep(step).start()
    own_slots = pltpu.make_async_copy(slots_ref.at[me], rows.at[row, core, 0], own_sem.at[0])
    own_slots.start()
    moved_rows(0, "core").start()
    group_angles = angles(me * group_rows, group_rows)
    cosine_ref[...] = jnp.cos(group_angles)
    sine_ref[...] = jnp.sin(group_angles)

    def pass_latents(steps):
        for step in steps:
            latent_ep(step).wait_recv()
            if step % 2 == 0:
                latent_ep(step + 1).start()
            latent_core(step).start()

    info_y.wait_recv()
    peer_picker, peer_weight = choose_slots(
        peer_info_ref[:picks, :own_rows].T.astype(jnp.int32),
        peer_info_ref[picks : 2 * picks, :own_rows].T,
        expert_total,
        capacity,
        me // NEAR * NEAR * slot_rows,
        NEAR * slot_rows,
    )
    store_split(peer_weight_ref, peer_weight)
    pass_latents(range(2, ep_count, 2))
    slots_ep(1).start()
    moved(tokens, 0, "y").wait_recv()
    moved(tokens, 0, "cross").start()
    fill(peer_slots_ref, peer_picker, 1 - row)
    for step in range(1, NEAR):
        peer_slots_ep(step).start()
    peer_own = pltpu.make_async_copy(
        peer_slots_ref.at[near_place], rows.at[1 - row, core, 0], own_sem.at[1]
    )
    peer_own.start()
    moved_rows(0, "cross").start()
    def project():
        for place, target in enumerate((query_columns_ref, latent_columns_ref)):
            pltpu.make_async_copy(target, target, weight_sem.at[place]).wait()
        query_rows = queries[...].reshape(group_rows, queries.shape[-1])
        for side in range(2):
            projected = jnp.dot(
                query_rows, query_columns_ref[side], preferred_element_type=jnp.float32
            )
            query_wide[side, :, :head_lanes] = narrow(projected[:, :head_lanes])
            query_wide[side, :, head_lanes:] = turn(
                projected[:, head_lanes:], cosine_ref[...], sine_ref[...]
            )
        for block in range(2):
            packed = latents[block].reshape(ep_count * own_rows, latents.shape[-1])
            span = slice(block * ep_count * own_rows, (block + 1) * ep_count * own_rows)
            for side in range(2):
                expanded = narrow(
                    jnp.dot(
                        packed[:, :rank_width],
                        latent_columns_ref[side],
                        preferred_element_type=jnp.float32,
                    )
                )
                keys[side, span, :head_lanes] = expanded[:, :head_lanes]
                keys[side, span, head_lanes:] = packed[:, rank_width:]
                values[side, span, :] = expanded[:, head_lanes:]

    block_rows = group_rows // 2

    def attend(side, block):
        span = slice(block * block_rows, (block + 1) * block_rows)
        query_block = query_wide[side, span, :]
        lane = lax.broadcasted_iota(jnp.int32, query_block.shape, 1)
        lane_head = jnp.where(
            lane < head_lanes,
            lane // CONTENT,
            (lane - head_lanes) // ROTARY - core * heads % (128 // ROTARY),
        )
        out_lane = lax.broadcasted_iota(jnp.int32, (block_rows, head_lanes), 1)
        result = jnp.zeros((block_rows, head_lanes), jnp.float32)
        stats = jnp.zeros((block_rows, head_lanes), jnp.float32)
        for head in range(heads):
            chosen = jnp.where(lane_head == head, query_block, jnp.zeros_like(query_block))
            scores = lax.dot_general(
                chosen, keys[side], (((1,), (1,)), ((), ())), preferred_element_type=jnp.float32
            ) * ((CONTENT + ROTARY) ** (-0.5))
            peak = jnp.max(scores, -1, keepdims=True)
            weights = jnp.exp(scores - peak)
            total = jnp.sum(weights, -1, keepdims=True)
            summed = jnp.dot(narrow(weights), values[side], preferred_element_type=jnp.float32)
            result = jnp.where(out_lane // VALUE == head, summed, result)
            stats = jnp.where(out_lane == 2 * head, peak, stats)
            stats = jnp.where(out_lane == 2 * head + 1, total, stats)
        if side == 0:
            own_sum[span, :] = result
            own_stats[span, :] = stats
        else:
            sent_sum[span, :] = narrow(result)
            sent_stats[8 * block : 8 * block + 8, :] = stats.T[:8]

    sum_y = remote(sent_sum, far_sum, y_send.at[4], y_recv.at[1], y_peer)
    stats_y = remote(sent_stats, far_stats, y_send.at[5], y_recv.at[8], y_peer)

    def merge():
        stats_y.wait_recv()
        sum_y.wait_recv()
        out_lane = lax.broadcasted_iota(jnp.int32, (block_rows, head_lanes), 1)
        for block in range(2):
            span = slice(block * block_rows, (block + 1) * block_rows)
            here = own_stats[span, :]
            there = far_stats[8 * block : 8 * block + 8, :].T
            result = jnp.zeros((block_rows, head_lanes), jnp.float32)
            for head in range(heads):
                peak_here, total_here = here[:, 2 * head : 2 * head + 1], here[:, 2 * head + 1 : 2 * head + 2]
                peak_there, total_there = there[:, 2 * head : 2 * head + 1], there[:, 2 * head + 1 : 2 * head + 2]
                peak = jnp.maximum(peak_here, peak_there)
                factor_here = jnp.exp(peak_here - peak)
                factor_there = jnp.exp(peak_there - peak)
                total = total_here * factor_here + total_there * factor_there
                summed = own_sum[span, :] * factor_here + wide(far_sum[span, :]) * factor_there
                result = jnp.where(out_lane // VALUE == head, summed / total, result)
            attended[span, :] = narrow(result)

    def mix():
        fetches[8].wait()
        for start in range(0, width, stripe):
            product = narrow(
                jnp.dot(
                    attended[...],
                    output_weight_ref[:, start : start + stripe],
                    preferred_element_type=jnp.float32,
                )
            )
            mixed[:, :, :, start : start + stripe] = product.reshape(2, 2, own_rows, stripe)

    def share():
        for fetch in fetches[9:12]:
            fetch.wait()
        for route in ("core", "cross"):
            moved(tokens, 0, route).wait_recv()
        hidden = gated_rows(
            tokens[...].reshape(group_rows, width), shared_gate_ref[...], shared_up_ref[...]
        )
        for start in range(0, width, stripe):
            product = narrow(
                jnp.dot(
                    hidden,
                    shared_down_ref[:, start : start + stripe],
                    preferred_element_type=jnp.float32,
                )
            )
            shared[:, :, :, start : start + stripe] = product.reshape(2, 2, own_rows, stripe)

    shared_half = remote(
        shared.at[:, 1 - core], half_shared, side_send.at[0], side_recv.at[0], core_peer
    )
    mixed_half = remote(
        mixed.at[:, 1 - core], half_mixed, side_send.at[1], side_recv.at[1], core_peer
    )
    shared_y = remote(
        shared.at[1 - row, core], far_shared, side_send.at[2], side_recv.at[2], y_peer
    )
    mixed_y = remote(mixed.at[1 - row, core], far_mixed, side_send.at[3], side_recv.at[3], y_peer)

    def mixed_far():
        mixed_half.wait_recv()
        mixed[1 - row, core] = narrow(wide(mixed[1 - row, core]) + wide(half_mixed[1 - row]))
        mixed_y.start()

    def arrive(step):
        slots_ep(step).wait_recv()
        moved_rows(step, "core").start()

    def arrive_peer(step):
        peer_slots_ep(step).wait_recv()
        moved_rows(step, "cross").start()

    def arrive_far(chunk, place):
        step = chunks[chunk] + place
        slots_ep(step).wait_recv()
        moved_rows(step, "y").start()
        moved_rows(step, "core", 1 + chunk).start()

    def arrive_far_peer(chunk, place):
        step = chunks[chunk] + place
        moved_rows(step, "y").wait_recv()
        moved_rows(step, "cross", 1 + chunk).start()

    def spans(expert):
        return slice(expert * capacity, (expert + 1) * capacity)

    def compute(first, count, expert):
        span = spans(expert)
        block = rows[:, :, pl.ds(first, count), span, :].reshape(4 * count * capacity, width)
        hidden = gated_rows(block, gate_ref[expert], up_ref[expert])
        for start in range(0, width, stripe):
            product = narrow(
                jnp.dot(
                    hidden,
                    down_ref[expert, :, start : start + stripe],
                    preferred_element_type=jnp.float32,
                )
            )
            part[:, :, pl.ds(first, count), span, start : start + stripe] = product.reshape(
                2, 2, count, capacity, stripe
            )

    def near_half():
        return remote(
            part.at[:, 1 - core, :NEAR],
            half_rows.at[:, :NEAR],
            half_send.at[0],
            half_recv.at[0],
            core_peer,
        )

    def far_half(chunk, expert):
        steps = pl.ds(chunks[chunk], 2)
        return remote(
            part.at[:, 1 - core, steps, spans(expert)],
            half_rows.at[:, steps, spans(expert)],
            half_send.at[0],
            half_recv.at[1 + chunk * local_experts + expert],
            core_peer,
        )

    def back_near(step):
        return remote(
            part.at[row, core, step],
            returned.at[me],
            back_send.at[0],
            back_recv.at[0],
            peer(step),
        )

    def back_peer(step):
        return remote(
            part.at[1 - row, core, step],
            returned_peer.at[near_place],
            peer_send.at[1],
            peer_recv.at[0],
            peer(step),
        )

    def back_far(step, expert):
        return remote(
            part.at[row, core, step, spans(expert)],
            returned.at[me, spans(expert)],
            back_send.at[0],
            back_recv.at[0],
            peer(step),
        )

    def y_copy(step, expert):
        return remote(
            part.at[1 - row, core, step, spans(expert)],
            far_rows.at[step - NEAR, spans(expert)],
            far_send.at[0],
            far_recv.at[expert, step - NEAR],
            y_peer,
        )

    def settle_near():
        near_half().wait_recv()
        order = list(range(1, NEAR)) + [0]
        for step in order:
            outer = narrow(wide(part[1 - row, core, step]) + wide(half_rows[1 - row, step]))
            if step:
                part[1 - row, core, step] = outer
                back_peer(step).start()
            else:
                returned_peer[near_place] = outer
        for step in order:
            total = narrow(wide(part[row, core, step]) + wide(half_rows[row, step]))
            if step:
                part[row, core, step] = total
                back_near(step).start()
            else:
                returned[me] = total

    def settle_outer(chunk, expert):
        far_half(chunk, expert).wait_recv()
        span = spans(expert)
        for step in (chunks[chunk], chunks[chunk] + 1):
            part[1 - row, core, step, span] = narrow(
                wide(part[1 - row, core, step, span]) + wide(half_rows[1 - row, step, span])
            )
            y_copy(step, expert).start()

    def settle_far(chunk, expert):
        span = spans(expert)
        for step in (chunks[chunk], chunks[chunk] + 1):
            y_copy(step, expert).wait_recv()
            part[row, core, step, span] = narrow(
                wide(part[row, core, step, span])
                + wide(half_rows[row, step, span])
                + wide(far_rows[step - NEAR, span])
            )
            back_far(step, expert).start()

    def wait_rows(first, count, group):
        for route in ("core", "cross"):
            origin_row, send_sem, recv_sem, device = routes_of[route]
            block = rows.at[origin_row, 1 - core, pl.ds(first, count)]
            remote(block, block, send_sem.at[0], recv_sem.at[4 + group], device).wait_recv()

    def far_chunk(chunk):
        wait_rows(chunks[chunk], 2, 1 + chunk)
        for expert in range(local_experts):
            compute(chunks[chunk], 2, expert)
            far_half(chunk, expert).start()

    def gather_latents():
        moved(queries, 1, "y").wait_recv()
        moved(queries, 1, "cross").start()
        pass_latents(range(1, ep_count, 2))

    def finish_latents():
        for route in ("core", "cross"):
            moved(queries, 1, route).wait_recv()
        arrived = latents.at[1 - core]
        remote(arrived, arrived, core_send.at[1], core_recv.at[1], core_peer).wait_recv()

    def near_compute():
        own_slots.wait()
        peer_own.wait()
        wait_rows(0, NEAR, 0)
        for expert in range(local_experts):
            compute(0, NEAR, expert)
        near_half().start()

    def inner(work):
        pl.when(outermost == 0)(work)

    def outer(work):
        pl.when(outermost == 1)(work)

    def attend_peer():
        gather_latents()
        finish_latents()
        project()
        attend(1, 0)
        attend(1, 1)
        stats_y.start()
        sum_y.start()

    def mix_own():
        merge()
        mix()
        mixed_half.start()

    def send_far():
        for step in (6, 4, 7, 5):
            slots_ep(step).start()

    arrive_far(0, 0)
    outer(attend_peer)
    arrive_far(0, 1)
    outer(send_far)
    outer(lambda: attend(0, 0))
    outer(lambda: attend(0, 1))
    outer(mix_own)
    for fetch in fetches[12:]:
        fetch.wait()
    for place in range(2):
        arrive_far_peer(0, place)
    outer(mixed_far)
    far_chunk(0)
    for step in range(1, NEAR):
        arrive(step)
    for expert in range(local_experts):
        settle_outer(0, expert)
    for step in range(1, NEAR):
        arrive_peer(step)
    inner(attend_peer)
    inner(near_compute)
    arrive_far(1, 0)
    inner(lambda: attend(0, 0))
    arrive_far(1, 1)
    inner(lambda: attend(0, 1))
    outer(near_compute)
    settle_far(0, 0)
    settle_far(0, 1)
    inner(mix_own)
    settle_near()
    inner(mixed_far)
    share()
    shared_half.start()
    for place in range(2):
        arrive_far_peer(1, place)
    far_chunk(1)
    for expert in range(local_experts):
        settle_outer(1, expert)
    for expert in range(local_experts):
        settle_far(1, expert)
    mixed_y.wait_recv()
    both_out[0] = narrow(wide(mixed[row, core]) + wide(half_mixed[row]) + wide(far_mixed[...]))
    returns = returned_peer.at[: NEAR - 1]
    remote(returns, returns, peer_send.at[1], peer_recv.at[0], core_peer).wait_recv()
    shared_half.wait_recv()
    for start in range(0, width, stripe):
        cut = slice(start, start + stripe)
        shared[1 - row, core, :, cut] = narrow(
            weighted_rows(
                peer_weight_ref[...],
                returned_peer[:, :, cut].reshape(NEAR * slot_rows, stripe),
            )
            + wide(shared[1 - row, core, :, cut])
            + wide(half_shared[1 - row, :, cut])
        )
    shared_y.start()
    returns = returned.at[: ep_count - 1]
    remote(returns, returns, back_send.at[0], back_recv.at[0], core_peer).wait_recv()
    shared_y.wait_recv()
    for start in range(0, width, stripe):
        cut = slice(start, start + stripe)
        both_out[1, :, cut] = narrow(
            weighted_rows(
                weight_ref[...], returned[:, :, cut].reshape(ep_count * slot_rows, stripe)
            )
            + wide(shared[row, core, :, cut])
            + wide(half_shared[row, :, cut])
            + wide(far_shared[:, cut])
        )

    blocks = rows.at[0, 0]
    for source, sem in (
        (slots_ref.at[: ep_count - 1], ep_send.at[0]),
        (latents.at[0, : ep_count - 1], ep_send.at[1]),
        (blocks, core_send.at[0]),
        (latents.at[0], core_send.at[1]),
        (blocks, cross_send.at[0]),
        (rows.at[0, 0, NEAR:], y_send.at[0]),
        (rows.at[0, 0, : NEAR - 1], peer_send.at[0]),
        (rows.at[0, 0, : NEAR - 1], peer_send.at[1]),
        (rows.at[0, 0, : ep_count - 1], back_send.at[0]),
        (rows.at[0, 0, NEAR:], far_send.at[0]),
        (part.at[0], half_send.at[0]),
    ):
        remote(source, source, sem, core_recv.at[0], core_peer).wait_send()
    for route in ("y", "core", "cross"):
        moved(queries, 1, route).wait_send()
        moved(tokens, 0, route).wait_send()
    for copy in (info_y, sum_y, stats_y, shared_half, mixed_half, shared_y, mixed_y):
        copy.wait_send()


def block_call(ep_count, capacity, *operands):
    query_latent, key_latent = operands[:2]
    own_rows, width = operands[5].shape
    head_lanes = operands[14].shape[0]
    local_experts = operands[15].shape[0]
    slot_rows = local_experts * capacity
    latent_shape = (own_rows, key_latent.shape[1] + 128)
    anywhere = pl.BlockSpec(memory_space=pl.ANY)

    def held(*shape):
        return pltpu.VMEM(shape, jnp.bfloat16)

    def precise(*shape):
        return pltpu.VMEM(shape, jnp.float32)

    def sems(*shape):
        return pltpu.SemaphoreType.DMA(shape)

    group_rows = 4 * own_rows
    key_rows = 2 * ep_count * own_rows
    row_block = (slot_rows, width)
    side = (own_rows, width)
    return pl.pallas_call(
        lambda *refs: block_kernel(ep_count, capacity, *refs),
        out_shape=jax.ShapeDtypeStruct((2,) + side, jnp.bfloat16),
        in_specs=[anywhere] * 21,
        out_specs=pl.BlockSpec(memory_space=pltpu.VMEM),
        scratch_shapes=[pltpu.VMEM(operand.shape, operand.dtype) for operand in operands[:10]]
        + [
            precise(group_rows, 128),
            precise(group_rows, 128),
            held(ep_count, *row_block),
            held(NEAR, *row_block),
            held(2, query_latent.shape[1], head_lanes + 128),
            held(2, key_latent.shape[1], 2 * head_lanes),
            held(head_lanes, width),
            held(3 * own_rows, ep_count * slot_rows),
            held(3 * own_rows, NEAR * slot_rows),
            held(2, 2, ep_count, *row_block),
            held(2, ep_count, *latent_shape),
            held(2, 2, *side),
            held(2, 2, *query_latent.shape),
        ]
        + [held(*operand.shape) for operand in operands[15:]]
        + [
            held(2, key_rows, head_lanes + 128),
            held(2, key_rows, head_lanes),
            held(2, group_rows, head_lanes + 128),
            held(group_rows, head_lanes),
            held(2, 2, ep_count, *row_block),
            held(2, ep_count, *row_block),
            held(ep_count - NEAR, *row_block),
            held(ep_count, *row_block),
            held(NEAR, *row_block),
            held(2, 2, *side),
            held(2, *side),
            held(*side),
            held(2, 2, *side),
            held(2, *side),
            held(*side),
            precise(8, 128),
            precise(8, 128),
            precise(group_rows, head_lanes),
            precise(group_rows, head_lanes),
            held(group_rows, head_lanes),
            held(group_rows, head_lanes),
            precise(16, head_lanes),
            precise(16, head_lanes),
        ]
        + [
            sems(2),
            sems(2, ep_count),
            sems(6),
            sems(9),
            sems(4),
            sems(7),
            sems(4),
            sems(7),
            sems(2),
            sems(NEAR),
            sems(1),
            sems(1),
            sems(1),
            sems(local_experts, ep_count - NEAR),
            sems(1),
            sems(1 + 2 * local_experts),
            sems(4),
            sems(4),
            sems(2),
            sems(9),
            sems(10),
        ],
        compiler_params=pltpu.CompilerParams(
            collective_id=0, has_side_effects=True, vmem_limit_bytes=VMEM_LIMIT
        ),
        name="block",
    )(*operands)


def shards(
    query_latent,
    key_latent,
    rotary_key,
    query_gain,
    latent_gain,
    query_content,
    query_rotary,
    key_content,
    value_weight,
    output_weight,
    expert_input,
    norm_gain,
    routes,
    route_weight,
    expert_gate,
    expert_up,
    expert_down,
    shared_gate,
    shared_up,
    shared_down,
):
    group_size = lax.axis_size("tp")
    expert_groups = lax.axis_size("ep")
    token_rows = expert_input.shape[0]
    picks = routes.shape[1]
    local_experts = expert_gate.shape[0]
    expert_total = local_experts * expert_groups
    capacity = 2 * token_rows * picks // expert_total
    if group_size != 4 or capacity % 16 or not fits_kernel(expert_groups, local_experts * capacity):
        return shards_plain(
            query_latent,
            key_latent,
            rotary_key,
            query_gain,
            latent_gain,
            query_content,
            query_rotary,
            key_content,
            value_weight,
            output_weight,
            expert_input,
            norm_gain,
            routes,
            route_weight,
            expert_gate,
            expert_up,
            expert_down,
            shared_gate,
            shared_up,
            shared_down,
        )
    frequency = rope_base ** (-np.arange(ROTARY // 2) * 2.0 / ROTARY)
    both = block_call(
        expert_groups,
        capacity,
        query_latent,
        key_latent,
        rotary_key.T,
        query_gain[None, :],
        latent_gain[None, :],
        expert_input,
        norm_gain[None, :],
        routes.T,
        route_weight.T,
        jnp.asarray(np.tile(np.repeat(frequency, 2), 128 // ROTARY)[None, :], jnp.float32),
        query_content,
        query_rotary,
        key_content,
        value_weight,
        output_weight,
        expert_gate,
        expert_up,
        expert_down,
        shared_gate,
        shared_up,
        shared_down,
    )
    return (both[0], both[1])


def solution(mesh):
    in_specs = (
        P(("ep", "tp"), None),
        P(("ep", "tp"), None),
        P(("ep", "tp"), None),
        P(),
        P(),
        P(),
        P(),
        P(),
        P(),
        P("tp", None),
        P(("ep", "tp"), None),
        P(),
        P(("ep", "tp"), None),
        P(("ep", "tp"), None),
        P("ep", None, "tp"),
        P("ep", None, "tp"),
        P("ep", "tp", None),
        P(None, "tp"),
        P(None, "tp"),
        P("tp", None),
    )
    out_specs = (P(("ep", "tp"), None), P(("ep", "tp"), None))
    return jax.shard_map(shards, mesh=mesh, in_specs=in_specs, out_specs=out_specs, check_vma=False)
```

```python
import math

import jax
import jax.numpy as jnp
import numpy as np
from jax import lax
from jax.experimental import pallas as pl
from jax.experimental.pallas import tpu as pltpu
from jax.sharding import PartitionSpec as P

HEADS = 8
CONTENT = 64
ROTARY = 32
VALUE = 64


norm_eps = 1e-06
rope_base = 10000.0


def rms_rows(entries, gain_row):
    widened = entries.astype(jnp.float32)
    return widened * lax.rsqrt(jnp.mean(widened * widened, -1, keepdims=True) + norm_eps) * gain_row


def turn_pairs(entries, positions):
    width_full = entries.shape[-1]
    frequency = rope_base ** (-jnp.arange(width_full // 2, dtype=jnp.float32) * 2.0 / width_full)
    angles = positions.astype(jnp.float32)[:, None] * frequency[None, :]
    cosine = jnp.cos(angles)[:, None, :]
    sine_part = jnp.sin(angles)[:, None, :]
    even_part = entries[..., 0::2]
    odd_part = entries[..., 1::2]
    joined = jnp.stack(
        [even_part * cosine - odd_part * sine_part, even_part * sine_part + odd_part * cosine], -1
    )
    return joined.reshape(entries.shape)


def absorb_block(carried, query_part, query_turn, key_part, key_turn, value_rows, score_scale):
    running_peak, running_total, summed = carried
    scores = jnp.einsum("qhc,khc->qhk", query_part, key_part, preferred_element_type=jnp.float32)
    scores = scores + jnp.einsum(
        "qhr,kr->qhk", query_turn, key_turn, preferred_element_type=jnp.float32
    )
    scores = scores * score_scale
    new_peak = jnp.maximum(running_peak, jnp.max(scores, -1))
    factor = jnp.exp(running_peak - new_peak)
    weights = jnp.exp(scores - new_peak[..., None])
    running_total = running_total * factor + jnp.sum(weights, -1)
    summed = summed * factor[..., None] + jnp.einsum(
        "qhk,khv->qhv", weights.astype(jnp.bfloat16), value_rows, preferred_element_type=jnp.float32
    )
    return (new_peak, running_total, summed)


def absorb_piece(carried, query_part, query_turn, key_part, key_turn, value_rows, score_scale):
    row_count = key_part.shape[0]
    key_block = math.gcd(row_count, 2048)
    if key_block == row_count:
        return absorb_block(
            carried, query_part, query_turn, key_part, key_turn, value_rows, score_scale
        )
    block_count = row_count // key_block

    def advance(state, pieces):
        return (
            absorb_block(
                state, query_part, query_turn, pieces[0], pieces[1], pieces[2], score_scale
            ),
            None,
        )

    stacked = (
        key_part.reshape((block_count, key_block) + key_part.shape[1:]),
        key_turn.reshape(block_count, key_block, key_turn.shape[1]),
        value_rows.reshape((block_count, key_block) + value_rows.shape[1:]),
    )
    carried, ignored = lax.scan(advance, carried, stacked)
    return carried


def expand_keys(latent_rows, key_columns, value_columns, head_local):
    row_count = latent_rows.shape[0]
    key_part = (
        jnp.dot(latent_rows, key_columns, preferred_element_type=jnp.float32)
        .astype(jnp.bfloat16)
        .reshape(row_count, head_local, CONTENT)
    )
    value_rows = (
        jnp.dot(latent_rows, value_columns, preferred_element_type=jnp.float32)
        .astype(jnp.bfloat16)
        .reshape(row_count, head_local, VALUE)
    )
    return (key_part, value_rows)


def expert_terms(row_block, gate_weight, up_weight, down_weight):
    gated = jnp.einsum("secd,edf->secf", row_block, gate_weight, preferred_element_type=jnp.float32)
    lifted = jnp.einsum("secd,edf->secf", row_block, up_weight, preferred_element_type=jnp.float32)
    hidden = (jax.nn.silu(gated) * lifted).astype(jnp.bfloat16)
    return jnp.einsum("secf,efd->secd", hidden, down_weight, preferred_element_type=jnp.float32)


def shared_terms(row_block, gate_weight, up_weight, down_weight):
    gated = jnp.dot(row_block, gate_weight, preferred_element_type=jnp.float32)
    lifted = jnp.dot(row_block, up_weight, preferred_element_type=jnp.float32)
    hidden = (jax.nn.silu(gated) * lifted).astype(jnp.bfloat16)
    return jnp.dot(hidden, down_weight, preferred_element_type=jnp.float32)


def shards_plain(
    query_latent,
    key_latent,
    rotary_key,
    query_gain,
    latent_gain,
    query_content,
    query_rotary,
    key_content,
    value_weight,
    output_weight,
    expert_input,
    norm_gain,
    routes,
    route_weight,
    expert_gate,
    expert_up,
    expert_down,
    shared_gate,
    shared_up,
    shared_down,
):
    group_size = lax.axis_size("tp")
    expert_groups = lax.axis_size("ep")
    own_rows = query_latent.shape[0]
    head_local = HEADS // group_size
    head_index = lax.axis_index("tp")
    group_rows_count = own_rows * group_size
    group_start = lax.axis_index("ep") * group_rows_count
    own_start = group_start + head_index * own_rows
    score_scale = (CONTENT + ROTARY) ** (-0.5)
    query_normed = rms_rows(query_latent, query_gain).astype(jnp.bfloat16)
    latent_normed = rms_rows(key_latent, latent_gain).astype(jnp.bfloat16)
    own_positions = own_start + jnp.arange(own_rows, dtype=jnp.int32)
    key_turned = turn_pairs(rotary_key.astype(jnp.float32)[:, None, :], own_positions)[
        :, 0, :
    ].astype(jnp.bfloat16)
    token_rows = expert_input.shape[0]
    picks = routes.shape[1]
    local_experts = expert_gate.shape[0]
    expert_total = local_experts * expert_groups
    capacity = 2 * token_rows * picks // expert_total
    slot_total = expert_total * capacity
    model_width = expert_input.shape[1]
    expert_normed = rms_rows(expert_input, norm_gain).astype(jnp.bfloat16)
    flat_routes = routes.reshape(-1)
    marks = (flat_routes[:, None] == jnp.arange(expert_total, dtype=jnp.int32)[None, :]).astype(
        jnp.int32
    )
    ranks = jnp.sum((jnp.cumsum(marks, 0) - marks) * marks, 1)
    targets = flat_routes * capacity + ranks
    picker = (jnp.arange(slot_total, dtype=jnp.int32)[:, None] == targets[None, :]).astype(
        jnp.int32
    )
    picker = jnp.sum(picker.reshape(slot_total, token_rows, picks), 2).astype(jnp.bfloat16)
    outgoing = jnp.dot(picker, expert_normed, preferred_element_type=jnp.float32).astype(
        jnp.bfloat16
    )
    outgoing = outgoing.reshape(expert_groups, local_experts, capacity, model_width)
    received = lax.all_to_all(outgoing, "ep", split_axis=0, concat_axis=0, tiled=True)
    group_query, group_latent, group_turn, gathered_rows, gathered_tokens = (
        lax.all_gather(query_normed, "tp", axis=0, tiled=True),
        lax.all_gather(latent_normed, "tp", axis=0, tiled=True),
        lax.all_gather(key_turned, "tp", axis=0, tiled=True),
        lax.all_gather(received, "tp", axis=0, tiled=True),
        lax.all_gather(expert_normed, "tp", axis=0, tiled=True),
    )
    positions = group_start + jnp.arange(group_rows_count, dtype=jnp.int32)
    content_columns = lax.dynamic_slice_in_dim(
        query_content, head_index * head_local * CONTENT, head_local * CONTENT, 1
    )
    rotary_columns = lax.dynamic_slice_in_dim(
        query_rotary, head_index * head_local * ROTARY, head_local * ROTARY, 1
    )
    query_part = (
        jnp.dot(group_query, content_columns, preferred_element_type=jnp.float32)
        .astype(jnp.bfloat16)
        .reshape(group_rows_count, head_local, CONTENT)
    )
    query_turn = turn_pairs(
        jnp.dot(group_query, rotary_columns, preferred_element_type=jnp.float32).reshape(
            group_rows_count, head_local, ROTARY
        ),
        positions,
    ).astype(jnp.bfloat16)
    key_columns = lax.dynamic_slice_in_dim(
        key_content, head_index * head_local * CONTENT, head_local * CONTENT, 1
    )
    value_columns = lax.dynamic_slice_in_dim(
        value_weight, head_index * head_local * VALUE, head_local * VALUE, 1
    )
    carry_start = (
        jnp.full((group_rows_count, head_local), -jnp.inf, jnp.float32),
        jnp.zeros((group_rows_count, head_local), jnp.float32),
        jnp.zeros((group_rows_count, head_local, VALUE), jnp.float32),
    )
    key_part, value_rows = expand_keys(
        lax.all_gather(group_latent, "ep", axis=0, tiled=True),
        key_columns,
        value_columns,
        head_local,
    )
    running_peak, running_total, summed = absorb_piece(
        carry_start,
        query_part,
        query_turn,
        key_part,
        lax.all_gather(group_turn, "ep", axis=0, tiled=True),
        value_rows,
        score_scale,
    )
    attended = (
        (summed / running_total[..., None])
        .astype(jnp.bfloat16)
        .reshape(group_rows_count, head_local * VALUE)
    )
    routed_term = expert_terms(gathered_rows, expert_gate, expert_up, expert_down)
    shared_term = shared_terms(gathered_tokens, shared_gate, shared_up, shared_down)
    mixer_term = jnp.dot(attended, output_weight, preferred_element_type=jnp.float32)
    mixer_sum, routed_sum, shared_sum = (
        lax.psum_scatter(
            mixer_term.astype(jnp.bfloat16), "tp", scatter_dimension=0, tiled=True
        ).astype(jnp.float32),
        lax.psum_scatter(
            routed_term.astype(jnp.bfloat16), "tp", scatter_dimension=0, tiled=True
        ).astype(jnp.float32),
        lax.psum_scatter(
            shared_term.astype(jnp.bfloat16), "tp", scatter_dimension=0, tiled=True
        ).astype(jnp.float32),
    )
    mixer_out = mixer_sum.astype(jnp.bfloat16)
    returned = lax.all_to_all(
        routed_sum.astype(jnp.bfloat16), "ep", split_axis=0, concat_axis=0, tiled=True
    )
    returned = returned.reshape(slot_total, model_width)
    picked = jnp.take(returned, targets, axis=0).reshape(token_rows, picks, model_width)
    combined = jnp.sum(route_weight[..., None] * picked.astype(jnp.float32), 1) + shared_sum
    expert_out = combined.astype(jnp.bfloat16)
    return (mixer_out, expert_out)


MESH = pl.DeviceIdType.MESH
VMEM_LIMIT = 60 * 1024 * 1024
NEAR = 4


def fits_kernel(ep_count, slot_rows):
    return ep_count == 2 * NEAR and NEAR * slot_rows % 128 == 0


def flip(place, bits, width=3):
    flipped = place
    for power in range(width):
        bit = 2**power
        flipped = flipped + bit * (bits // bit % 2) * (1 - 2 * (place // bit % 2))
    return flipped


def greet(ep_count, me, head_index):
    barrier = pltpu.get_barrier_semaphore()
    for step in range(1, ep_count):
        pl.semaphore_signal(
            barrier, inc=1, device_id=(flip(me, step), head_index), device_id_type=MESH
        )
    row, core = head_index // 2, head_index % 2
    for other in ((1 - row) * 2 + core, row * 2 + 1 - core):
        pl.semaphore_signal(barrier, inc=1, device_id=(me, other), device_id_type=MESH)
    return lambda: pl.semaphore_wait(barrier, ep_count + 1)


def gated_rows(rows, gate_weight, up_weight):
    gated = jnp.dot(rows, gate_weight, preferred_element_type=jnp.float32)
    lifted = jnp.dot(rows, up_weight, preferred_element_type=jnp.float32)
    return (gated / (1.0 + jnp.exp(-gated)) * lifted).astype(jnp.bfloat16)


def wide(entries):
    return entries.astype(jnp.float32)


def narrow(entries):
    return entries.astype(jnp.bfloat16)


def choose_slots(routes, weights, expert_total, capacity, first_slot, slot_count):
    own_rows = routes.shape[0]
    expert_lane = lax.broadcasted_iota(jnp.int32, (own_rows, expert_total), 1)
    named = [
        jnp.where(routes[:, pick : pick + 1] == expert_lane, 1.0, 0.0)
        for pick in range(routes.shape[1])
    ]
    earlier = narrow(
        jnp.where(
            lax.broadcasted_iota(jnp.int32, (own_rows, own_rows), 0)
            > lax.broadcasted_iota(jnp.int32, (own_rows, own_rows), 1),
            1.0,
            0.0,
        )
    )
    ahead = jnp.dot(earlier, narrow(sum(named)), preferred_element_type=jnp.float32)
    slot_lane = lax.broadcasted_iota(jnp.int32, (own_rows, slot_count), 1) + first_slot
    picker = jnp.zeros(slot_lane.shape, jnp.float32)
    weight = jnp.zeros(slot_lane.shape, jnp.float32)
    for pick, marks in enumerate(named):
        rank = jnp.sum(ahead * marks, 1, keepdims=True).astype(jnp.int32)
        chosen = slot_lane == routes[:, pick : pick + 1] * capacity + rank
        picker = jnp.where(chosen, 1.0, picker)
        weight = jnp.where(chosen, weights[:, pick : pick + 1], weight)
    return narrow(picker.T), weight


def store_split(target, weight):
    own_rows = weight.shape[0]
    high = narrow(weight)
    rest = weight - wide(high)
    middle = narrow(rest)
    target[:own_rows] = high
    target[own_rows : 2 * own_rows] = middle
    target[2 * own_rows :] = narrow(rest - wide(middle))


def weighted_rows(split_weight, entries):
    picked = jnp.dot(split_weight, entries, preferred_element_type=jnp.float32)
    own_rows = picked.shape[0] // 3
    return picked[:own_rows] + picked[own_rows : 2 * own_rows] + picked[2 * own_rows :]


def block_kernel(
    ep_count,
    capacity,
    query_latent_hbm,
    key_latent_hbm,
    rotary_key_hbm,
    query_gain_hbm,
    latent_gain_hbm,
    expert_input_hbm,
    norm_gain_hbm,
    routes_hbm,
    route_weight_hbm,
    frequency_hbm,
    query_content_hbm,
    query_rotary_hbm,
    key_content_hbm,
    value_weight_hbm,
    output_weight_hbm,
    gate_hbm,
    up_hbm,
    down_hbm,
    shared_gate_hbm,
    shared_up_hbm,
    shared_down_hbm,
    both_out,
    query_latent_ref,
    key_latent_ref,
    rotary_key_ref,
    query_gain_ref,
    latent_gain_ref,
    expert_input_ref,
    norm_gain_ref,
    routes_ref,
    route_weight_ref,
    frequency_ref,
    cosine_ref,
    sine_ref,
    slots_ref,
    peer_slots_ref,
    query_columns_ref,
    latent_columns_ref,
    output_weight_ref,
    weight_ref,
    peer_weight_ref,
    rows,
    latents,
    tokens,
    queries,
    gate_ref,
    up_ref,
    down_ref,
    shared_gate_ref,
    shared_up_ref,
    shared_down_ref,
    keys,
    values,
    query_wide,
    attended,
    part,
    half_rows,
    far_rows,
    returned,
    returned_peer,
    mixed,
    half_mixed,
    far_mixed,
    shared,
    half_shared,
    far_shared,
    info_ref,
    peer_info_ref,
    own_sum,
    own_stats,
    sent_sum,
    far_sum,
    sent_stats,
    far_stats,
    ep_send,
    ep_recv,
    y_send,
    y_recv,
    core_send,
    core_recv,
    cross_send,
    cross_recv,
    peer_send,
    peer_recv,
    back_send,
    back_recv,
    far_send,
    far_recv,
    half_send,
    half_recv,
    side_send,
    side_recv,
    own_sem,
    weight_sem,
    input_sem,
):
    me = lax.axis_index("ep")
    head_index = lax.axis_index("tp")
    row, core = head_index // 2, head_index % 2
    y_peer = (me, (1 - row) * 2 + core)
    core_peer = (me, row * 2 + 1 - core)
    local_experts = gate_ref.shape[0]
    width = rows.shape[-1]
    own_rows = tokens.shape[2]
    slot_rows = rows.shape[3]
    group_rows = attended.shape[0]
    picks = routes_ref.shape[0]
    stripe = math.gcd(width, 512)
    far_steps = range(NEAR, ep_count)
    outermost = 1 - (me // 2 + me // 4) % 2
    chunks = (NEAR + 2 * (1 - outermost), NEAR + 2 * outermost)
    greeted = greet(ep_count, me, head_index)
    arguments = [
        pltpu.make_async_copy(source, target, input_sem.at[place])
        for place, (source, target) in enumerate(
            (
                (key_latent_hbm, key_latent_ref),
                (rotary_key_hbm, rotary_key_ref),
                (latent_gain_hbm, latent_gain_ref),
                (frequency_hbm, frequency_ref),
                (expert_input_hbm, expert_input_ref),
                (norm_gain_hbm, norm_gain_ref),
                (routes_hbm, routes_ref),
                (route_weight_hbm, route_weight_ref),
                (query_latent_hbm, query_latent_ref),
                (query_gain_hbm, query_gain_ref),
            )
        )
    ]
    with jax.named_scope("s00"):
        for argument in arguments:
            argument.start()
    near_place = me % NEAR

    def peer(step):
        return (flip(me, step), head_index)

    def remote(source, target, send_sem, recv_sem, device):
        return pltpu.make_async_remote_copy(
            src_ref=source,
            dst_ref=target,
            send_sem=send_sem,
            recv_sem=recv_sem,
            device_id=device,
            device_id_type=MESH,
        )

    head_lanes = attended.shape[1]
    heads = head_lanes // VALUE
    fetch_list = []
    for side in range(2):
        side_index = (row if side == 0 else 1 - row) * 2 + core
        columns = pl.ds(pl.multiple_of(side_index * head_lanes, head_lanes), head_lanes)
        turn_columns = pl.ds(pl.multiple_of(side_index * heads * ROTARY // 128 * 128, 128), 128)
        fetch_list += [
            (query_content_hbm.at[:, columns], query_columns_ref.at[side, :, :head_lanes]),
            (query_rotary_hbm.at[:, turn_columns], query_columns_ref.at[side, :, head_lanes:]),
            (key_content_hbm.at[:, columns], latent_columns_ref.at[side, :, :head_lanes]),
            (value_weight_hbm.at[:, columns], latent_columns_ref.at[side, :, head_lanes:]),
        ]
    fetch_list += [
        (output_weight_hbm, output_weight_ref),
        (shared_gate_hbm, shared_gate_ref),
        (shared_up_hbm, shared_up_ref),
        (shared_down_hbm, shared_down_ref),
        (gate_hbm, gate_ref),
        (up_hbm, up_ref),
        (down_hbm, down_ref),
    ]
    fetches = [
        pltpu.make_async_copy(
            source, target, weight_sem.at[place % 4 // 2 if place < 8 else place - 6]
        )
        for place, (source, target) in enumerate(fetch_list)
    ]
    for fetch in fetches:
        fetch.start()

    def turn(entries, cosine, sine):
        lane = lax.broadcasted_iota(jnp.int32, entries.shape, 1)
        crossed = jnp.where(
            lane % 2 == 0, -pltpu.roll(entries, 127, 1), pltpu.roll(entries, 1, 1)
        )
        return narrow(entries * cosine + crossed * sine)

    def angles(first, count):
        places = first + lax.broadcasted_iota(jnp.int32, (count, 128), 0)
        return places.astype(jnp.float32) * frequency_ref[...]

    with jax.named_scope("s01"):
        for argument in arguments[:4]:
            argument.wait()
    rank_width = key_latent_ref.shape[1]
    with jax.named_scope("s02"):
        latents[core, 0, :, :rank_width] = narrow(rms_rows(key_latent_ref[...], latent_gain_ref[...]))
    repeats = narrow(
        jnp.where(
            lax.broadcasted_iota(jnp.int32, (ROTARY, 128), 0)
            == lax.broadcasted_iota(jnp.int32, (ROTARY, 128), 1) % ROTARY,
            1.0,
            0.0,
        )
    )
    own_angles = angles((me * 4 + head_index) * own_rows, own_rows)
    with jax.named_scope("s03"):
        latents[core, 0, :, rank_width:] = turn(
            lax.dot_general(
                rotary_key_ref[...],
                repeats,
                (((0,), (0,)), ((), ())),
                preferred_element_type=jnp.float32,
            ),
            jnp.cos(own_angles),
            jnp.sin(own_angles),
        )
    with jax.named_scope("s04"):
        for argument in arguments[4:]:
            argument.wait()
    with jax.named_scope("s05"):
        expert_normed = narrow(rms_rows(expert_input_ref[...], norm_gain_ref[...]))
    with jax.named_scope("s06"):
        tokens[row, core] = expert_normed
    with jax.named_scope("s07"):
        queries[row, core] = narrow(rms_rows(query_latent_ref[...], query_gain_ref[...]))
    with jax.named_scope("s08"):
        info_ref[...] = jnp.zeros(info_ref.shape, jnp.float32)
    with jax.named_scope("s09"):
        info_ref[:picks, :own_rows] = routes_ref[...].astype(jnp.float32)
    with jax.named_scope("s10"):
        info_ref[picks : 2 * picks, :own_rows] = route_weight_ref[...]
    with jax.named_scope("s11"):
        greeted()

    def latent_ep(step):
        if step % 2 == 0:
            return remote(
                latents.at[core, 0],
                latents.at[core, step],
                ep_send.at[1],
                ep_recv.at[1, step],
                peer(step),
            )
        return remote(
            latents.at[core, step - 1],
            latents.at[core, step],
            ep_send.at[1],
            ep_recv.at[1, step],
            peer(1),
        )

    def latent_core(step):
        return remote(
            latents.at[core, step],
            latents.at[core, step],
            core_send.at[1],
            core_recv.at[1],
            core_peer,
        )

    def slots_ep(step):
        return remote(
            slots_ref.at[flip(me, step)],
            rows.at[row, core, step],
            ep_send.at[0],
            ep_recv.at[0, step],
            peer(step),
        )

    def peer_slots_ep(step):
        return remote(
            peer_slots_ref.at[flip(near_place, step)],
            rows.at[1 - row, core, step],
            peer_send.at[0],
            peer_recv.at[step],
            peer(step),
        )

    routes_of = {
        "y": (row, y_send, y_recv, y_peer),
        "core": (row, core_send, core_recv, core_peer),
        "cross": (1 - row, cross_send, cross_recv, core_peer),
    }

    def moved_rows(step, route, group=0):
        origin_row, send_sem, recv_sem, device = routes_of[route]
        block = rows.at[origin_row, core, step]
        source = block
        if isinstance(step, int) and step == 0:
            source = peer_slots_ref.at[near_place] if route == "cross" else slots_ref.at[me]
        place = 4 + step - NEAR if route == "y" else 4 + group
        return remote(source, block, send_sem.at[0], recv_sem.at[place], device)

    def moved(buffer, place, route):
        origin_row, send_sem, recv_sem, device = routes_of[route]
        block = buffer.at[origin_row, core]
        return remote(block, block, send_sem.at[2 + place], recv_sem.at[2 + place], device)

    info_y = remote(
        info_ref, peer_info_ref, y_send.at[1], y_recv.at[0], y_peer
    )
    with jax.named_scope("s12"):
        for step in (6, 4, 2, 1):
            latent_ep(step).start()
    with jax.named_scope("s13"):
        latent_core(0).start()
    with jax.named_scope("s14"):
        info_y.start()
    with jax.named_scope("s15"):
        for route in ("y", "core"):
            moved(tokens, 0, route).start()
    with jax.named_scope("s16"):
        for route in ("y", "core"):
            moved(queries, 1, route).start()
    expert_total = local_experts * ep_count
    with jax.named_scope("s17"):
        picker, weight = choose_slots(
            routes_ref[...].T, route_weight_ref[...].T, expert_total, capacity, 0, ep_count * slot_rows
        )
    with jax.named_scope("s18"):
        store_split(weight_ref, weight)

    def fill(target, chooser, origin_row):
        for start in range(0, width, stripe):
            target[:, :, start : start + stripe] = narrow(
                jnp.dot(
                    chooser,
                    tokens[origin_row, core, :, start : start + stripe],
                    preferred_element_type=jnp.float32,
                )
            ).reshape(target.shape[0], slot_rows, stripe)

    with jax.named_scope("s19"):
        fill(slots_ref, picker, row)
    @pl.when(outermost == 0)
    def _():
        for step in (6, 4, 7, 5):
            slots_ep(step).start()

    with jax.named_scope("s20"):
        for step in (2, 3):
            slots_ep(step).start()
    own_slots = pltpu.make_async_copy(slots_ref.at[me], rows.at[row, core, 0], own_sem.at[0])
    with jax.named_scope("s21"):
        own_slots.start()
    with jax.named_scope("s22"):
        moved_rows(0, "core").start()
    group_angles = angles(me * group_rows, group_rows)
    with jax.named_scope("s23"):
        cosine_ref[...] = jnp.cos(group_angles)
    with jax.named_scope("s24"):
        sine_ref[...] = jnp.sin(group_angles)

    def pass_latents(steps):
        for step in steps:
            latent_ep(step).wait_recv()
            if step % 2 == 0:
                latent_ep(step + 1).start()
            latent_core(step).start()

    with jax.named_scope("s25"):
        info_y.wait_recv()
    with jax.named_scope("s26"):
        peer_picker, peer_weight = choose_slots(
            peer_info_ref[:picks, :own_rows].T.astype(jnp.int32),
            peer_info_ref[picks : 2 * picks, :own_rows].T,
            expert_total,
            capacity,
            me // NEAR * NEAR * slot_rows,
            NEAR * slot_rows,
        )
    with jax.named_scope("s27"):
        store_split(peer_weight_ref, peer_weight)
    with jax.named_scope("s28"):
        pass_latents(range(2, ep_count, 2))
    with jax.named_scope("s29"):
        slots_ep(1).start()
    with jax.named_scope("s30"):
        moved(tokens, 0, "y").wait_recv()
    with jax.named_scope("s31"):
        moved(tokens, 0, "cross").start()
    with jax.named_scope("s32"):
        fill(peer_slots_ref, peer_picker, 1 - row)
    with jax.named_scope("s33"):
        for step in range(1, NEAR):
            peer_slots_ep(step).start()
    peer_own = pltpu.make_async_copy(
        peer_slots_ref.at[near_place], rows.at[1 - row, core, 0], own_sem.at[1]
    )
    with jax.named_scope("s34"):
        peer_own.start()
    with jax.named_scope("s35"):
        moved_rows(0, "cross").start()
    def project():
        for place, target in enumerate((query_columns_ref, latent_columns_ref)):
            pltpu.make_async_copy(target, target, weight_sem.at[place]).wait()
        query_rows = queries[...].reshape(group_rows, queries.shape[-1])
        for side in range(2):
            projected = jnp.dot(
                query_rows, query_columns_ref[side], preferred_element_type=jnp.float32
            )
            query_wide[side, :, :head_lanes] = narrow(projected[:, :head_lanes])
            query_wide[side, :, head_lanes:] = turn(
                projected[:, head_lanes:], cosine_ref[...], sine_ref[...]
            )
        for block in range(2):
            packed = latents[block].reshape(ep_count * own_rows, latents.shape[-1])
            span = slice(block * ep_count * own_rows, (block + 1) * ep_count * own_rows)
            for side in range(2):
                expanded = narrow(
                    jnp.dot(
                        packed[:, :rank_width],
                        latent_columns_ref[side],
                        preferred_element_type=jnp.float32,
                    )
                )
                keys[side, span, :head_lanes] = expanded[:, :head_lanes]
                keys[side, span, head_lanes:] = packed[:, rank_width:]
                values[side, span, :] = expanded[:, head_lanes:]

    block_rows = group_rows // 2

    def attend(side, block):
        span = slice(block * block_rows, (block + 1) * block_rows)
        query_block = query_wide[side, span, :]
        lane = lax.broadcasted_iota(jnp.int32, query_block.shape, 1)
        lane_head = jnp.where(
            lane < head_lanes,
            lane // CONTENT,
            (lane - head_lanes) // ROTARY - core * heads % (128 // ROTARY),
        )
        out_lane = lax.broadcasted_iota(jnp.int32, (block_rows, head_lanes), 1)
        result = jnp.zeros((block_rows, head_lanes), jnp.float32)
        stats = jnp.zeros((block_rows, head_lanes), jnp.float32)
        for head in range(heads):
            chosen = jnp.where(lane_head == head, query_block, jnp.zeros_like(query_block))
            scores = lax.dot_general(
                chosen, keys[side], (((1,), (1,)), ((), ())), preferred_element_type=jnp.float32
            ) * ((CONTENT + ROTARY) ** (-0.5))
            peak = jnp.max(scores, -1, keepdims=True)
            weights = jnp.exp(scores - peak)
            total = jnp.sum(weights, -1, keepdims=True)
            summed = jnp.dot(narrow(weights), values[side], preferred_element_type=jnp.float32)
            result = jnp.where(out_lane // VALUE == head, summed, result)
            stats = jnp.where(out_lane == 2 * head, peak, stats)
            stats = jnp.where(out_lane == 2 * head + 1, total, stats)
        if side == 0:
            own_sum[span, :] = result
            own_stats[span, :] = stats
        else:
            sent_sum[span, :] = narrow(result)
            sent_stats[8 * block : 8 * block + 8, :] = stats.T[:8]

    sum_y = remote(sent_sum, far_sum, y_send.at[4], y_recv.at[1], y_peer)
    stats_y = remote(sent_stats, far_stats, y_send.at[5], y_recv.at[8], y_peer)

    def merge():
        stats_y.wait_recv()
        sum_y.wait_recv()
        out_lane = lax.broadcasted_iota(jnp.int32, (block_rows, head_lanes), 1)
        for block in range(2):
            span = slice(block * block_rows, (block + 1) * block_rows)
            here = own_stats[span, :]
            there = far_stats[8 * block : 8 * block + 8, :].T
            result = jnp.zeros((block_rows, head_lanes), jnp.float32)
            for head in range(heads):
                peak_here, total_here = here[:, 2 * head : 2 * head + 1], here[:, 2 * head + 1 : 2 * head + 2]
                peak_there, total_there = there[:, 2 * head : 2 * head + 1], there[:, 2 * head + 1 : 2 * head + 2]
                peak = jnp.maximum(peak_here, peak_there)
                factor_here = jnp.exp(peak_here - peak)
                factor_there = jnp.exp(peak_there - peak)
                total = total_here * factor_here + total_there * factor_there
                summed = own_sum[span, :] * factor_here + wide(far_sum[span, :]) * factor_there
                result = jnp.where(out_lane // VALUE == head, summed / total, result)
            attended[span, :] = narrow(result)

    def mix():
        fetches[8].wait()
        for start in range(0, width, stripe):
            product = narrow(
                jnp.dot(
                    attended[...],
                    output_weight_ref[:, start : start + stripe],
                    preferred_element_type=jnp.float32,
                )
            )
            mixed[:, :, :, start : start + stripe] = product.reshape(2, 2, own_rows, stripe)

    def share():
        for fetch in fetches[9:12]:
            fetch.wait()
        for route in ("core", "cross"):
            moved(tokens, 0, route).wait_recv()
        hidden = gated_rows(
            tokens[...].reshape(group_rows, width), shared_gate_ref[...], shared_up_ref[...]
        )
        for start in range(0, width, stripe):
            product = narrow(
                jnp.dot(
                    hidden,
                    shared_down_ref[:, start : start + stripe],
                    preferred_element_type=jnp.float32,
                )
            )
            shared[:, :, :, start : start + stripe] = product.reshape(2, 2, own_rows, stripe)

    shared_half = remote(
        shared.at[:, 1 - core], half_shared, side_send.at[0], side_recv.at[0], core_peer
    )
    mixed_half = remote(
        mixed.at[:, 1 - core], half_mixed, side_send.at[1], side_recv.at[1], core_peer
    )
    shared_y = remote(
        shared.at[1 - row, core], far_shared, side_send.at[2], side_recv.at[2], y_peer
    )
    mixed_y = remote(mixed.at[1 - row, core], far_mixed, side_send.at[3], side_recv.at[3], y_peer)

    def mixed_far():
        mixed_half.wait_recv()
        mixed[1 - row, core] = narrow(wide(mixed[1 - row, core]) + wide(half_mixed[1 - row]))
        mixed_y.start()

    def arrive(step):
        slots_ep(step).wait_recv()
        moved_rows(step, "core").start()

    def arrive_peer(step):
        peer_slots_ep(step).wait_recv()
        moved_rows(step, "cross").start()

    def arrive_far(chunk, place):
        step = chunks[chunk] + place
        slots_ep(step).wait_recv()
        moved_rows(step, "y").start()
        moved_rows(step, "core", 1 + chunk).start()

    def arrive_far_peer(chunk, place):
        step = chunks[chunk] + place
        moved_rows(step, "y").wait_recv()
        moved_rows(step, "cross", 1 + chunk).start()

    def spans(expert):
        return slice(expert * capacity, (expert + 1) * capacity)

    def compute(first, count, expert):
        span = spans(expert)
        block = rows[:, :, pl.ds(first, count), span, :].reshape(4 * count * capacity, width)
        hidden = gated_rows(block, gate_ref[expert], up_ref[expert])
        for start in range(0, width, stripe):
            product = narrow(
                jnp.dot(
                    hidden,
                    down_ref[expert, :, start : start + stripe],
                    preferred_element_type=jnp.float32,
                )
            )
            part[:, :, pl.ds(first, count), span, start : start + stripe] = product.reshape(
                2, 2, count, capacity, stripe
            )

    def near_half():
        return remote(
            part.at[:, 1 - core, :NEAR],
            half_rows.at[:, :NEAR],
            half_send.at[0],
            half_recv.at[0],
            core_peer,
        )

    def far_half(chunk, expert):
        steps = pl.ds(chunks[chunk], 2)
        return remote(
            part.at[:, 1 - core, steps, spans(expert)],
            half_rows.at[:, steps, spans(expert)],
            half_send.at[0],
            half_recv.at[1 + chunk * local_experts + expert],
            core_peer,
        )

    def back_near(step):
        return remote(
            part.at[row, core, step],
            returned.at[me],
            back_send.at[0],
            back_recv.at[0],
            peer(step),
        )

    def back_peer(step):
        return remote(
            part.at[1 - row, core, step],
            returned_peer.at[near_place],
            peer_send.at[1],
            peer_recv.at[0],
            peer(step),
        )

    def back_far(step, expert):
        return remote(
            part.at[row, core, step, spans(expert)],
            returned.at[me, spans(expert)],
            back_send.at[0],
            back_recv.at[0],
            peer(step),
        )

    def y_copy(step, expert):
        return remote(
            part.at[1 - row, core, step, spans(expert)],
            far_rows.at[step - NEAR, spans(expert)],
            far_send.at[0],
            far_recv.at[expert, step - NEAR],
            y_peer,
        )

    def settle_near():
        near_half().wait_recv()
        order = list(range(1, NEAR)) + [0]
        for step in order:
            outer = narrow(wide(part[1 - row, core, step]) + wide(half_rows[1 - row, step]))
            if step:
                part[1 - row, core, step] = outer
                back_peer(step).start()
            else:
                returned_peer[near_place] = outer
        for step in order:
            total = narrow(wide(part[row, core, step]) + wide(half_rows[row, step]))
            if step:
                part[row, core, step] = total
                back_near(step).start()
            else:
                returned[me] = total

    def settle_outer(chunk, expert):
        far_half(chunk, expert).wait_recv()
        span = spans(expert)
        for step in (chunks[chunk], chunks[chunk] + 1):
            part[1 - row, core, step, span] = narrow(
                wide(part[1 - row, core, step, span]) + wide(half_rows[1 - row, step, span])
            )
            y_copy(step, expert).start()

    def settle_far(chunk, expert):
        span = spans(expert)
        for step in (chunks[chunk], chunks[chunk] + 1):
            y_copy(step, expert).wait_recv()
            part[row, core, step, span] = narrow(
                wide(part[row, core, step, span])
                + wide(half_rows[row, step, span])
                + wide(far_rows[step - NEAR, span])
            )
            back_far(step, expert).start()

    def wait_rows(first, count, group):
        for route in ("core", "cross"):
            origin_row, send_sem, recv_sem, device = routes_of[route]
            block = rows.at[origin_row, 1 - core, pl.ds(first, count)]
            remote(block, block, send_sem.at[0], recv_sem.at[4 + group], device).wait_recv()

    def far_chunk(chunk):
        wait_rows(chunks[chunk], 2, 1 + chunk)
        for expert in range(local_experts):
            compute(chunks[chunk], 2, expert)
            far_half(chunk, expert).start()

    def gather_latents():
        moved(queries, 1, "y").wait_recv()
        moved(queries, 1, "cross").start()
        pass_latents(range(1, ep_count, 2))

    def finish_latents():
        for route in ("core", "cross"):
            moved(queries, 1, route).wait_recv()
        arrived = latents.at[1 - core]
        remote(arrived, arrived, core_send.at[1], core_recv.at[1], core_peer).wait_recv()

    def near_compute():
        own_slots.wait()
        peer_own.wait()
        wait_rows(0, NEAR, 0)
        for expert in range(local_experts):
            compute(0, NEAR, expert)
        near_half().start()

    def inner(work):
        pl.when(outermost == 0)(work)

    def outer(work):
        pl.when(outermost == 1)(work)

    def attend_peer():
        gather_latents()
        finish_latents()
        project()
        attend(1, 0)
        attend(1, 1)
        stats_y.start()
        sum_y.start()

    def mix_own():
        merge()
        mix()
        mixed_half.start()

    def send_far():
        for step in (6, 4, 7, 5):
            slots_ep(step).start()

    with jax.named_scope("s36"):
        arrive_far(0, 0)
    with jax.named_scope("s37"):
        outer(attend_peer)
    with jax.named_scope("s38"):
        arrive_far(0, 1)
    with jax.named_scope("s39"):
        outer(send_far)
    with jax.named_scope("s40"):
        outer(lambda: attend(0, 0))
    with jax.named_scope("s41"):
        outer(lambda: attend(0, 1))
    with jax.named_scope("s42"):
        outer(mix_own)
    for fetch in fetches[12:]:
        fetch.wait()
    with jax.named_scope("s43"):
        for place in range(2):
            arrive_far_peer(0, place)
    with jax.named_scope("s44"):
        outer(mixed_far)
    with jax.named_scope("s45"):
        far_chunk(0)
    with jax.named_scope("s46"):
        for step in range(1, NEAR):
            arrive(step)
    with jax.named_scope("s47"):
        for expert in range(local_experts):
            settle_outer(0, expert)
    with jax.named_scope("s48"):
        for step in range(1, NEAR):
            arrive_peer(step)
    with jax.named_scope("s49"):
        inner(attend_peer)
    with jax.named_scope("s50"):
        inner(near_compute)
    with jax.named_scope("s51"):
        arrive_far(1, 0)
    with jax.named_scope("s52"):
        inner(lambda: attend(0, 0))
    with jax.named_scope("s53"):
        arrive_far(1, 1)
    with jax.named_scope("s54"):
        inner(lambda: attend(0, 1))
    with jax.named_scope("s55"):
        outer(near_compute)
    with jax.named_scope("s56"):
        settle_far(0, 0)
    with jax.named_scope("s57"):
        settle_far(0, 1)
    with jax.named_scope("s58"):
        inner(mix_own)
    with jax.named_scope("s59"):
        settle_near()
    with jax.named_scope("s60"):
        inner(mixed_far)
    with jax.named_scope("s61"):
        share()
    with jax.named_scope("s62"):
        shared_half.start()
    with jax.named_scope("s63"):
        for place in range(2):
            arrive_far_peer(1, place)
    with jax.named_scope("s64"):
        far_chunk(1)
    with jax.named_scope("s65"):
        for expert in range(local_experts):
            settle_outer(1, expert)
    with jax.named_scope("s66"):
        for expert in range(local_experts):
            settle_far(1, expert)
    with jax.named_scope("s67"):
        mixed_y.wait_recv()
    with jax.named_scope("s68"):
        both_out[0] = narrow(wide(mixed[row, core]) + wide(half_mixed[row]) + wide(far_mixed[...]))
    returns = returned_peer.at[: NEAR - 1]
    with jax.named_scope("s69"):
        remote(returns, returns, peer_send.at[1], peer_recv.at[0], core_peer).wait_recv()
    with jax.named_scope("s70"):
        shared_half.wait_recv()
    with jax.named_scope("s71"):
        for start in range(0, width, stripe):
            cut = slice(start, start + stripe)
            shared[1 - row, core, :, cut] = narrow(
                weighted_rows(
                    peer_weight_ref[...],
                    returned_peer[:, :, cut].reshape(NEAR * slot_rows, stripe),
                )
                + wide(shared[1 - row, core, :, cut])
                + wide(half_shared[1 - row, :, cut])
            )
    with jax.named_scope("s72"):
        shared_y.start()
    returns = returned.at[: ep_count - 1]
    with jax.named_scope("s73"):
        remote(returns, returns, back_send.at[0], back_recv.at[0], core_peer).wait_recv()
    with jax.named_scope("s74"):
        shared_y.wait_recv()
    with jax.named_scope("s75"):
        for start in range(0, width, stripe):
            cut = slice(start, start + stripe)
            both_out[1, :, cut] = narrow(
                weighted_rows(
                    weight_ref[...], returned[:, :, cut].reshape(ep_count * slot_rows, stripe)
                )
                + wide(shared[row, core, :, cut])
                + wide(half_shared[row, :, cut])
                + wide(far_shared[:, cut])
            )

    blocks = rows.at[0, 0]
    with jax.named_scope("s76"):
        for source, sem in (
            (slots_ref.at[: ep_count - 1], ep_send.at[0]),
            (latents.at[0, : ep_count - 1], ep_send.at[1]),
            (blocks, core_send.at[0]),
            (latents.at[0], core_send.at[1]),
            (blocks, cross_send.at[0]),
            (rows.at[0, 0, NEAR:], y_send.at[0]),
            (rows.at[0, 0, : NEAR - 1], peer_send.at[0]),
            (rows.at[0, 0, : NEAR - 1], peer_send.at[1]),
            (rows.at[0, 0, : ep_count - 1], back_send.at[0]),
            (rows.at[0, 0, NEAR:], far_send.at[0]),
            (part.at[0], half_send.at[0]),
        ):
            remote(source, source, sem, core_recv.at[0], core_peer).wait_send()
    with jax.named_scope("s77"):
        for route in ("y", "core", "cross"):
            moved(queries, 1, route).wait_send()
            moved(tokens, 0, route).wait_send()
    with jax.named_scope("s78"):
        for copy in (info_y, sum_y, stats_y, shared_half, mixed_half, shared_y, mixed_y):
            copy.wait_send()


def block_call(ep_count, capacity, *operands):
    query_latent, key_latent = operands[:2]
    own_rows, width = operands[5].shape
    head_lanes = operands[14].shape[0]
    local_experts = operands[15].shape[0]
    slot_rows = local_experts * capacity
    latent_shape = (own_rows, key_latent.shape[1] + 128)
    anywhere = pl.BlockSpec(memory_space=pl.ANY)

    def held(*shape):
        return pltpu.VMEM(shape, jnp.bfloat16)

    def precise(*shape):
        return pltpu.VMEM(shape, jnp.float32)

    def sems(*shape):
        return pltpu.SemaphoreType.DMA(shape)

    group_rows = 4 * own_rows
    key_rows = 2 * ep_count * own_rows
    row_block = (slot_rows, width)
    side = (own_rows, width)
    return pl.pallas_call(
        lambda *refs: block_kernel(ep_count, capacity, *refs),
        out_shape=jax.ShapeDtypeStruct((2,) + side, jnp.bfloat16),
        in_specs=[anywhere] * 21,
        out_specs=pl.BlockSpec(memory_space=pltpu.VMEM),
        scratch_shapes=[pltpu.VMEM(operand.shape, operand.dtype) for operand in operands[:10]]
        + [
            precise(group_rows, 128),
            precise(group_rows, 128),
            held(ep_count, *row_block),
            held(NEAR, *row_block),
            held(2, query_latent.shape[1], head_lanes + 128),
            held(2, key_latent.shape[1], 2 * head_lanes),
            held(head_lanes, width),
            held(3 * own_rows, ep_count * slot_rows),
            held(3 * own_rows, NEAR * slot_rows),
            held(2, 2, ep_count, *row_block),
            held(2, ep_count, *latent_shape),
            held(2, 2, *side),
            held(2, 2, *query_latent.shape),
        ]
        + [held(*operand.shape) for operand in operands[15:]]
        + [
            held(2, key_rows, head_lanes + 128),
            held(2, key_rows, head_lanes),
            held(2, group_rows, head_lanes + 128),
            held(group_rows, head_lanes),
            held(2, 2, ep_count, *row_block),
            held(2, ep_count, *row_block),
            held(ep_count - NEAR, *row_block),
            held(ep_count, *row_block),
            held(NEAR, *row_block),
            held(2, 2, *side),
            held(2, *side),
            held(*side),
            held(2, 2, *side),
            held(2, *side),
            held(*side),
            precise(8, 128),
            precise(8, 128),
            precise(group_rows, head_lanes),
            precise(group_rows, head_lanes),
            held(group_rows, head_lanes),
            held(group_rows, head_lanes),
            precise(16, head_lanes),
            precise(16, head_lanes),
        ]
        + [
            sems(2),
            sems(2, ep_count),
            sems(6),
            sems(9),
            sems(4),
            sems(7),
            sems(4),
            sems(7),
            sems(2),
            sems(NEAR),
            sems(1),
            sems(1),
            sems(1),
            sems(local_experts, ep_count - NEAR),
            sems(1),
            sems(1 + 2 * local_experts),
            sems(4),
            sems(4),
            sems(2),
            sems(9),
            sems(10),
        ],
        compiler_params=pltpu.CompilerParams(
            collective_id=0, has_side_effects=True, vmem_limit_bytes=VMEM_LIMIT
        ),
        name="block",
    )(*operands)


def shards(
    query_latent,
    key_latent,
    rotary_key,
    query_gain,
    latent_gain,
    query_content,
    query_rotary,
    key_content,
    value_weight,
    output_weight,
    expert_input,
    norm_gain,
    routes,
    route_weight,
    expert_gate,
    expert_up,
    expert_down,
    shared_gate,
    shared_up,
    shared_down,
):
    group_size = lax.axis_size("tp")
    expert_groups = lax.axis_size("ep")
    token_rows = expert_input.shape[0]
    picks = routes.shape[1]
    local_experts = expert_gate.shape[0]
    expert_total = local_experts * expert_groups
    capacity = 2 * token_rows * picks // expert_total
    if group_size != 4 or capacity % 16 or not fits_kernel(expert_groups, local_experts * capacity):
        return shards_plain(
            query_latent,
            key_latent,
            rotary_key,
            query_gain,
            latent_gain,
            query_content,
            query_rotary,
            key_content,
            value_weight,
            output_weight,
            expert_input,
            norm_gain,
            routes,
            route_weight,
            expert_gate,
            expert_up,
            expert_down,
            shared_gate,
            shared_up,
            shared_down,
        )
    frequency = rope_base ** (-np.arange(ROTARY // 2) * 2.0 / ROTARY)
    both = block_call(
        expert_groups,
        capacity,
        query_latent,
        key_latent,
        rotary_key.T,
        query_gain[None, :],
        latent_gain[None, :],
        expert_input,
        norm_gain[None, :],
        routes.T,
        route_weight.T,
        jnp.asarray(np.tile(np.repeat(frequency, 2), 128 // ROTARY)[None, :], jnp.float32),
        query_content,
        query_rotary,
        key_content,
        value_weight,
        output_weight,
        expert_gate,
        expert_up,
        expert_down,
        shared_gate,
        shared_up,
        shared_down,
    )
    return (both[0], both[1])


def solution(mesh):
    in_specs = (
        P(("ep", "tp"), None),
        P(("ep", "tp"), None),
        P(("ep", "tp"), None),
        P(),
        P(),
        P(),
        P(),
        P(),
        P(),
        P("tp", None),
        P(("ep", "tp"), None),
        P(),
        P(("ep", "tp"), None),
        P(("ep", "tp"), None),
        P("ep", None, "tp"),
        P("ep", None, "tp"),
        P("ep", "tp", None),
        P(None, "tp"),
        P(None, "tp"),
        P("tp", None),
    )
    out_specs = (P(("ep", "tp"), None), P(("ep", "tp"), None))
    return jax.shard_map(shards, mesh=mesh, in_specs=in_specs, out_specs=out_specs, check_vma=False)
```

```python
import math

import jax
import jax.numpy as jnp
import numpy as np
from jax import lax
from jax.experimental import pallas as pl
from jax.experimental.pallas import tpu as pltpu
from jax.sharding import PartitionSpec as P

HEADS = 8
CONTENT = 64
ROTARY = 32
VALUE = 64


norm_eps = 1e-06
rope_base = 10000.0


def rms_rows(entries, gain_row):
    widened = entries.astype(jnp.float32)
    return widened * lax.rsqrt(jnp.mean(widened * widened, -1, keepdims=True) + norm_eps) * gain_row


def turn_pairs(entries, positions):
    width_full = entries.shape[-1]
    frequency = rope_base ** (-jnp.arange(width_full // 2, dtype=jnp.float32) * 2.0 / width_full)
    angles = positions.astype(jnp.float32)[:, None] * frequency[None, :]
    cosine = jnp.cos(angles)[:, None, :]
    sine_part = jnp.sin(angles)[:, None, :]
    even_part = entries[..., 0::2]
    odd_part = entries[..., 1::2]
    joined = jnp.stack(
        [even_part * cosine - odd_part * sine_part, even_part * sine_part + odd_part * cosine], -1
    )
    return joined.reshape(entries.shape)


def absorb_block(carried, query_part, query_turn, key_part, key_turn, value_rows, score_scale):
    running_peak, running_total, summed = carried
    scores = jnp.einsum("qhc,khc->qhk", query_part, key_part, preferred_element_type=jnp.float32)
    scores = scores + jnp.einsum(
        "qhr,kr->qhk", query_turn, key_turn, preferred_element_type=jnp.float32
    )
    scores = scores * score_scale
    new_peak = jnp.maximum(running_peak, jnp.max(scores, -1))
    factor = jnp.exp(running_peak - new_peak)
    weights = jnp.exp(scores - new_peak[..., None])
    running_total = running_total * factor + jnp.sum(weights, -1)
    summed = summed * factor[..., None] + jnp.einsum(
        "qhk,khv->qhv", weights.astype(jnp.bfloat16), value_rows, preferred_element_type=jnp.float32
    )
    return (new_peak, running_total, summed)


def absorb_piece(carried, query_part, query_turn, key_part, key_turn, value_rows, score_scale):
    row_count = key_part.shape[0]
    key_block = math.gcd(row_count, 2048)
    if key_block == row_count:
        return absorb_block(
            carried, query_part, query_turn, key_part, key_turn, value_rows, score_scale
        )
    block_count = row_count // key_block

    def advance(state, pieces):
        return (
            absorb_block(
                state, query_part, query_turn, pieces[0], pieces[1], pieces[2], score_scale
            ),
            None,
        )

    stacked = (
        key_part.reshape((block_count, key_block) + key_part.shape[1:]),
        key_turn.reshape(block_count, key_block, key_turn.shape[1]),
        value_rows.reshape((block_count, key_block) + value_rows.shape[1:]),
    )
    carried, ignored = lax.scan(advance, carried, stacked)
    return carried


def expand_keys(latent_rows, key_columns, value_columns, head_local):
    row_count = latent_rows.shape[0]
    key_part = (
        jnp.dot(latent_rows, key_columns, preferred_element_type=jnp.float32)
        .astype(jnp.bfloat16)
        .reshape(row_count, head_local, CONTENT)
    )
    value_rows = (
        jnp.dot(latent_rows, value_columns, preferred_element_type=jnp.float32)
        .astype(jnp.bfloat16)
        .reshape(row_count, head_local, VALUE)
    )
    return (key_part, value_rows)


def expert_terms(row_block, gate_weight, up_weight, down_weight):
    gated = jnp.einsum("secd,edf->secf", row_block, gate_weight, preferred_element_type=jnp.float32)
    lifted = jnp.einsum("secd,edf->secf", row_block, up_weight, preferred_element_type=jnp.float32)
    hidden = (jax.nn.silu(gated) * lifted).astype(jnp.bfloat16)
    return jnp.einsum("secf,efd->secd", hidden, down_weight, preferred_element_type=jnp.float32)


def shared_terms(row_block, gate_weight, up_weight, down_weight):
    gated = jnp.dot(row_block, gate_weight, preferred_element_type=jnp.float32)
    lifted = jnp.dot(row_block, up_weight, preferred_element_type=jnp.float32)
    hidden = (jax.nn.silu(gated) * lifted).astype(jnp.bfloat16)
    return jnp.dot(hidden, down_weight, preferred_element_type=jnp.float32)


def shards_plain(
    query_latent,
    key_latent,
    rotary_key,
    query_gain,
    latent_gain,
    query_content,
    query_rotary,
    key_content,
    value_weight,
    output_weight,
    expert_input,
    norm_gain,
    routes,
    route_weight,
    expert_gate,
    expert_up,
    expert_down,
    shared_gate,
    shared_up,
    shared_down,
):
    group_size = lax.axis_size("tp")
    expert_groups = lax.axis_size("ep")
    own_rows = query_latent.shape[0]
    head_local = HEADS // group_size
    head_index = lax.axis_index("tp")
    group_rows_count = own_rows * group_size
    group_start = lax.axis_index("ep") * group_rows_count
    own_start = group_start + head_index * own_rows
    score_scale = (CONTENT + ROTARY) ** (-0.5)
    query_normed = rms_rows(query_latent, query_gain).astype(jnp.bfloat16)
    latent_normed = rms_rows(key_latent, latent_gain).astype(jnp.bfloat16)
    own_positions = own_start + jnp.arange(own_rows, dtype=jnp.int32)
    key_turned = turn_pairs(rotary_key.astype(jnp.float32)[:, None, :], own_positions)[
        :, 0, :
    ].astype(jnp.bfloat16)
    token_rows = expert_input.shape[0]
    picks = routes.shape[1]
    local_experts = expert_gate.shape[0]
    expert_total = local_experts * expert_groups
    capacity = 2 * token_rows * picks // expert_total
    slot_total = expert_total * capacity
    model_width = expert_input.shape[1]
    expert_normed = rms_rows(expert_input, norm_gain).astype(jnp.bfloat16)
    flat_routes = routes.reshape(-1)
    marks = (flat_routes[:, None] == jnp.arange(expert_total, dtype=jnp.int32)[None, :]).astype(
        jnp.int32
    )
    ranks = jnp.sum((jnp.cumsum(marks, 0) - marks) * marks, 1)
    targets = flat_routes * capacity + ranks
    picker = (jnp.arange(slot_total, dtype=jnp.int32)[:, None] == targets[None, :]).astype(
        jnp.int32
    )
    picker = jnp.sum(picker.reshape(slot_total, token_rows, picks), 2).astype(jnp.bfloat16)
    outgoing = jnp.dot(picker, expert_normed, preferred_element_type=jnp.float32).astype(
        jnp.bfloat16
    )
    outgoing = outgoing.reshape(expert_groups, local_experts, capacity, model_width)
    received = lax.all_to_all(outgoing, "ep", split_axis=0, concat_axis=0, tiled=True)
    group_query, group_latent, group_turn, gathered_rows, gathered_tokens = (
        lax.all_gather(query_normed, "tp", axis=0, tiled=True),
        lax.all_gather(latent_normed, "tp", axis=0, tiled=True),
        lax.all_gather(key_turned, "tp", axis=0, tiled=True),
        lax.all_gather(received, "tp", axis=0, tiled=True),
        lax.all_gather(expert_normed, "tp", axis=0, tiled=True),
    )
    positions = group_start + jnp.arange(group_rows_count, dtype=jnp.int32)
    content_columns = lax.dynamic_slice_in_dim(
        query_content, head_index * head_local * CONTENT, head_local * CONTENT, 1
    )
    rotary_columns = lax.dynamic_slice_in_dim(
        query_rotary, head_index * head_local * ROTARY, head_local * ROTARY, 1
    )
    query_part = (
        jnp.dot(group_query, content_columns, preferred_element_type=jnp.float32)
        .astype(jnp.bfloat16)
        .reshape(group_rows_count, head_local, CONTENT)
    )
    query_turn = turn_pairs(
        jnp.dot(group_query, rotary_columns, preferred_element_type=jnp.float32).reshape(
            group_rows_count, head_local, ROTARY
        ),
        positions,
    ).astype(jnp.bfloat16)
    key_columns = lax.dynamic_slice_in_dim(
        key_content, head_index * head_local * CONTENT, head_local * CONTENT, 1
    )
    value_columns = lax.dynamic_slice_in_dim(
        value_weight, head_index * head_local * VALUE, head_local * VALUE, 1
    )
    carry_start = (
        jnp.full((group_rows_count, head_local), -jnp.inf, jnp.float32),
        jnp.zeros((group_rows_count, head_local), jnp.float32),
        jnp.zeros((group_rows_count, head_local, VALUE), jnp.float32),
    )
    key_part, value_rows = expand_keys(
        lax.all_gather(group_latent, "ep", axis=0, tiled=True),
        key_columns,
        value_columns,
        head_local,
    )
    running_peak, running_total, summed = absorb_piece(
        carry_start,
        query_part,
        query_turn,
        key_part,
        lax.all_gather(group_turn, "ep", axis=0, tiled=True),
        value_rows,
        score_scale,
    )
    attended = (
        (summed / running_total[..., None])
        .astype(jnp.bfloat16)
        .reshape(group_rows_count, head_local * VALUE)
    )
    routed_term = expert_terms(gathered_rows, expert_gate, expert_up, expert_down)
    shared_term = shared_terms(gathered_tokens, shared_gate, shared_up, shared_down)
    mixer_term = jnp.dot(attended, output_weight, preferred_element_type=jnp.float32)
    mixer_sum, routed_sum, shared_sum = (
        lax.psum_scatter(
            mixer_term.astype(jnp.bfloat16), "tp", scatter_dimension=0, tiled=True
        ).astype(jnp.float32),
        lax.psum_scatter(
            routed_term.astype(jnp.bfloat16), "tp", scatter_dimension=0, tiled=True
        ).astype(jnp.float32),
        lax.psum_scatter(
            shared_term.astype(jnp.bfloat16), "tp", scatter_dimension=0, tiled=True
        ).astype(jnp.float32),
    )
    mixer_out = mixer_sum.astype(jnp.bfloat16)
    returned = lax.all_to_all(
        routed_sum.astype(jnp.bfloat16), "ep", split_axis=0, concat_axis=0, tiled=True
    )
    returned = returned.reshape(slot_total, model_width)
    picked = jnp.take(returned, targets, axis=0).reshape(token_rows, picks, model_width)
    combined = jnp.sum(route_weight[..., None] * picked.astype(jnp.float32), 1) + shared_sum
    expert_out = combined.astype(jnp.bfloat16)
    return (mixer_out, expert_out)


MESH = pl.DeviceIdType.MESH
VMEM_LIMIT = 60 * 1024 * 1024
NEAR = 4


def fits_kernel(ep_count, slot_rows):
    return ep_count == 2 * NEAR and NEAR * slot_rows % 128 == 0


def flip(place, bits, width=3):
    flipped = place
    for power in range(width):
        bit = 2**power
        flipped = flipped + bit * (bits // bit % 2) * (1 - 2 * (place // bit % 2))
    return flipped


def greet(ep_count, me, head_index):
    barrier = pltpu.get_barrier_semaphore()
    for step in range(1, ep_count):
        pl.semaphore_signal(
            barrier, inc=1, device_id=(flip(me, step), head_index), device_id_type=MESH
        )
    row, core = head_index // 2, head_index % 2
    for other in ((1 - row) * 2 + core, row * 2 + 1 - core):
        pl.semaphore_signal(barrier, inc=1, device_id=(me, other), device_id_type=MESH)
    return lambda: pl.semaphore_wait(barrier, ep_count + 1)


def gated_rows(rows, gate_weight, up_weight):
    gated = jnp.dot(rows, gate_weight, preferred_element_type=jnp.float32)
    lifted = jnp.dot(rows, up_weight, preferred_element_type=jnp.float32)
    return (gated / (1.0 + jnp.exp(-gated)) * lifted).astype(jnp.bfloat16)


def wide(entries):
    return entries.astype(jnp.float32)


def narrow(entries):
    return entries.astype(jnp.bfloat16)


def choose_slots(routes, weights, expert_total, capacity, first_slot, slot_count):
    own_rows = routes.shape[0]
    expert_lane = lax.broadcasted_iota(jnp.int32, (own_rows, expert_total), 1)
    named = [
        jnp.where(routes[:, pick : pick + 1] == expert_lane, 1.0, 0.0)
        for pick in range(routes.shape[1])
    ]
    earlier = narrow(
        jnp.where(
            lax.broadcasted_iota(jnp.int32, (own_rows, own_rows), 0)
            > lax.broadcasted_iota(jnp.int32, (own_rows, own_rows), 1),
            1.0,
            0.0,
        )
    )
    ahead = jnp.dot(earlier, narrow(sum(named)), preferred_element_type=jnp.float32)
    slot_lane = lax.broadcasted_iota(jnp.int32, (own_rows, slot_count), 1) + first_slot
    picker = jnp.zeros(slot_lane.shape, jnp.float32)
    weight = jnp.zeros(slot_lane.shape, jnp.float32)
    for pick, marks in enumerate(named):
        rank = jnp.sum(ahead * marks, 1, keepdims=True).astype(jnp.int32)
        chosen = slot_lane == routes[:, pick : pick + 1] * capacity + rank
        picker = jnp.where(chosen, 1.0, picker)
        weight = jnp.where(chosen, weights[:, pick : pick + 1], weight)
    return narrow(picker.T), weight


def store_split(target, weight):
    own_rows = weight.shape[0]
    high = narrow(weight)
    rest = weight - wide(high)
    middle = narrow(rest)
    target[:own_rows] = high
    target[own_rows : 2 * own_rows] = middle
    target[2 * own_rows :] = narrow(rest - wide(middle))


def weighted_rows(split_weight, entries):
    picked = jnp.dot(split_weight, entries, preferred_element_type=jnp.float32)
    own_rows = picked.shape[0] // 3
    return picked[:own_rows] + picked[own_rows : 2 * own_rows] + picked[2 * own_rows :]


def block_kernel(
    ep_count,
    capacity,
    query_latent_hbm,
    key_latent_hbm,
    rotary_key_hbm,
    query_gain_hbm,
    latent_gain_hbm,
    expert_input_hbm,
    norm_gain_hbm,
    routes_hbm,
    route_weight_hbm,
    frequency_hbm,
    query_content_hbm,
    query_rotary_hbm,
    key_content_hbm,
    value_weight_hbm,
    output_weight_hbm,
    gate_hbm,
    up_hbm,
    down_hbm,
    shared_gate_hbm,
    shared_up_hbm,
    shared_down_hbm,
    both_out,
    query_latent_ref,
    key_latent_ref,
    rotary_key_ref,
    query_gain_ref,
    latent_gain_ref,
    expert_input_ref,
    norm_gain_ref,
    routes_ref,
    route_weight_ref,
    frequency_ref,
    cosine_ref,
    sine_ref,
    slots_ref,
    peer_slots_ref,
    query_columns_ref,
    latent_columns_ref,
    output_weight_ref,
    weight_ref,
    peer_weight_ref,
    rows,
    latents,
    tokens,
    queries,
    gate_ref,
    up_ref,
    down_ref,
    shared_gate_ref,
    shared_up_ref,
    shared_down_ref,
    keys,
    values,
    query_wide,
    attended,
    part,
    half_rows,
    far_rows,
    returned,
    returned_peer,
    mixed,
    half_mixed,
    far_mixed,
    shared,
    half_shared,
    far_shared,
    info_ref,
    peer_info_ref,
    own_sum,
    own_stats,
    sent_sum,
    far_sum,
    sent_stats,
    far_stats,
    ep_send,
    ep_recv,
    y_send,
    y_recv,
    core_send,
    core_recv,
    cross_send,
    cross_recv,
    peer_send,
    peer_recv,
    back_send,
    back_recv,
    far_send,
    far_recv,
    half_send,
    half_recv,
    side_send,
    side_recv,
    own_sem,
    weight_sem,
    input_sem,
):
    me = lax.axis_index("ep")
    head_index = lax.axis_index("tp")
    row, core = head_index // 2, head_index % 2
    y_peer = (me, (1 - row) * 2 + core)
    core_peer = (me, row * 2 + 1 - core)
    local_experts = gate_ref.shape[0]
    width = rows.shape[-1]
    own_rows = tokens.shape[2]
    slot_rows = rows.shape[3]
    group_rows = attended.shape[0]
    picks = routes_ref.shape[0]
    stripe = math.gcd(width, 512)
    far_steps = range(NEAR, ep_count)
    outermost = 1 - (me // 2 + me // 4) % 2
    chunks = (NEAR + 2 * (1 - outermost), NEAR + 2 * outermost)
    greeted = greet(ep_count, me, head_index)
    arguments = [
        pltpu.make_async_copy(source, target, input_sem.at[place])
        for place, (source, target) in enumerate(
            (
                (key_latent_hbm, key_latent_ref),
                (rotary_key_hbm, rotary_key_ref),
                (latent_gain_hbm, latent_gain_ref),
                (frequency_hbm, frequency_ref),
                (expert_input_hbm, expert_input_ref),
                (norm_gain_hbm, norm_gain_ref),
                (routes_hbm, routes_ref),
                (route_weight_hbm, route_weight_ref),
                (query_latent_hbm, query_latent_ref),
                (query_gain_hbm, query_gain_ref),
            )
        )
    ]
    with jax.named_scope("s00"):
        for argument in arguments:
            argument.start()
    near_place = me % NEAR

    def peer(step):
        return (flip(me, step), head_index)

    def remote(source, target, send_sem, recv_sem, device):
        return pltpu.make_async_remote_copy(
            src_ref=source,
            dst_ref=target,
            send_sem=send_sem,
            recv_sem=recv_sem,
            device_id=device,
            device_id_type=MESH,
        )

    head_lanes = attended.shape[1]
    heads = head_lanes // VALUE
    fetch_list = []
    for side in range(2):
        side_index = (row if side == 0 else 1 - row) * 2 + core
        columns = pl.ds(pl.multiple_of(side_index * head_lanes, head_lanes), head_lanes)
        turn_columns = pl.ds(pl.multiple_of(side_index * heads * ROTARY // 128 * 128, 128), 128)
        fetch_list += [
            (query_content_hbm.at[:, columns], query_columns_ref.at[side, :, :head_lanes]),
            (query_rotary_hbm.at[:, turn_columns], query_columns_ref.at[side, :, head_lanes:]),
            (key_content_hbm.at[:, columns], latent_columns_ref.at[side, :, :head_lanes]),
            (value_weight_hbm.at[:, columns], latent_columns_ref.at[side, :, head_lanes:]),
        ]
    fetch_list += [
        (output_weight_hbm, output_weight_ref),
        (shared_gate_hbm, shared_gate_ref),
        (shared_up_hbm, shared_up_ref),
        (shared_down_hbm, shared_down_ref),
        (gate_hbm, gate_ref),
        (up_hbm, up_ref),
        (down_hbm, down_ref),
    ]
    fetches = [
        pltpu.make_async_copy(
            source, target, weight_sem.at[place % 4 // 2 if place < 8 else place - 6]
        )
        for place, (source, target) in enumerate(fetch_list)
    ]
    for fetch in fetches:
        fetch.start()

    def turn(entries, cosine, sine):
        lane = lax.broadcasted_iota(jnp.int32, entries.shape, 1)
        crossed = jnp.where(
            lane % 2 == 0, -pltpu.roll(entries, 127, 1), pltpu.roll(entries, 1, 1)
        )
        return narrow(entries * cosine + crossed * sine)

    def angles(first, count):
        places = first + lax.broadcasted_iota(jnp.int32, (count, 128), 0)
        return places.astype(jnp.float32) * frequency_ref[...]

    with jax.named_scope("s01"):
        for argument in arguments[:4]:
            argument.wait()
    rank_width = key_latent_ref.shape[1]
    with jax.named_scope("s02"):
        latents[core, 0, :, :rank_width] = narrow(rms_rows(key_latent_ref[...], latent_gain_ref[...]))
    repeats = narrow(
        jnp.where(
            lax.broadcasted_iota(jnp.int32, (ROTARY, 128), 0)
            == lax.broadcasted_iota(jnp.int32, (ROTARY, 128), 1) % ROTARY,
            1.0,
            0.0,
        )
    )
    own_angles = angles((me * 4 + head_index) * own_rows, own_rows)
    with jax.named_scope("s03"):
        latents[core, 0, :, rank_width:] = turn(
            lax.dot_general(
                rotary_key_ref[...],
                repeats,
                (((0,), (0,)), ((), ())),
                preferred_element_type=jnp.float32,
            ),
            jnp.cos(own_angles),
            jnp.sin(own_angles),
        )
    with jax.named_scope("s04"):
        for argument in arguments[4:]:
            argument.wait()
    with jax.named_scope("s05"):
        expert_normed = narrow(rms_rows(expert_input_ref[...], norm_gain_ref[...]))
    with jax.named_scope("s06"):
        tokens[row, core] = expert_normed
    with jax.named_scope("s07"):
        queries[row, core] = narrow(rms_rows(query_latent_ref[...], query_gain_ref[...]))
    with jax.named_scope("s08"):
        info_ref[...] = jnp.zeros(info_ref.shape, jnp.float32)
    with jax.named_scope("s09"):
        info_ref[:picks, :own_rows] = routes_ref[...].astype(jnp.float32)
    with jax.named_scope("s10"):
        info_ref[picks : 2 * picks, :own_rows] = route_weight_ref[...]
    with jax.named_scope("s11"):
        greeted()

    def latent_ep(step):
        if step % 2 == 0:
            return remote(
                latents.at[core, 0],
                latents.at[core, step],
                ep_send.at[1],
                ep_recv.at[1, step],
                peer(step),
            )
        return remote(
            latents.at[core, step - 1],
            latents.at[core, step],
            ep_send.at[1],
            ep_recv.at[1, step],
            peer(1),
        )

    def latent_core(step):
        return remote(
            latents.at[core, step],
            latents.at[core, step],
            core_send.at[1],
            core_recv.at[1],
            core_peer,
        )

    def slots_ep(step):
        return remote(
            slots_ref.at[flip(me, step)],
            rows.at[row, core, step],
            ep_send.at[0],
            ep_recv.at[0, step],
            peer(step),
        )

    def peer_slots_ep(step):
        return remote(
            peer_slots_ref.at[flip(near_place, step)],
            rows.at[1 - row, core, step],
            peer_send.at[0],
            peer_recv.at[step],
            peer(step),
        )

    routes_of = {
        "y": (row, y_send, y_recv, y_peer),
        "core": (row, core_send, core_recv, core_peer),
        "cross": (1 - row, cross_send, cross_recv, core_peer),
    }

    def moved_rows(step, route, group=0):
        origin_row, send_sem, recv_sem, device = routes_of[route]
        block = rows.at[origin_row, core, step]
        source = block
        if isinstance(step, int) and step == 0:
            source = peer_slots_ref.at[near_place] if route == "cross" else slots_ref.at[me]
        place = 4 + step - NEAR if route == "y" else 4 + group
        return remote(source, block, send_sem.at[0], recv_sem.at[place], device)

    def moved(buffer, place, route):
        origin_row, send_sem, recv_sem, device = routes_of[route]
        block = buffer.at[origin_row, core]
        return remote(block, block, send_sem.at[2 + place], recv_sem.at[2 + place], device)

    info_y = remote(
        info_ref, peer_info_ref, y_send.at[1], y_recv.at[0], y_peer
    )
    with jax.named_scope("s12"):
        for step in (6, 4, 2, 1):
            latent_ep(step).start()
    with jax.named_scope("s13"):
        latent_core(0).start()
    with jax.named_scope("s14"):
        info_y.start()
    with jax.named_scope("s15"):
        for route in ("y", "core"):
            moved(tokens, 0, route).start()
    with jax.named_scope("s16"):
        for route in ("y", "core"):
            moved(queries, 1, route).start()
    expert_total = local_experts * ep_count
    with jax.named_scope("s17"):
        picker, weight = choose_slots(
            routes_ref[...].T, route_weight_ref[...].T, expert_total, capacity, 0, ep_count * slot_rows
        )
    with jax.named_scope("s18"):
        store_split(weight_ref, weight)

    def fill(target, chooser, origin_row):
        for start in range(0, width, stripe):
            target[:, :, start : start + stripe] = narrow(
                jnp.dot(
                    chooser,
                    tokens[origin_row, core, :, start : start + stripe],
                    preferred_element_type=jnp.float32,
                )
            ).reshape(target.shape[0], slot_rows, stripe)

    with jax.named_scope("s19"):
        fill(slots_ref, picker, row)
    @pl.when(outermost == 0)
    def _():
        for step in (6, 4, 7, 5):
            slots_ep(step).start()

    with jax.named_scope("s20"):
        for step in (2, 3):
            slots_ep(step).start()
    own_slots = pltpu.make_async_copy(slots_ref.at[me], rows.at[row, core, 0], own_sem.at[0])
    with jax.named_scope("s21"):
        own_slots.start()
    with jax.named_scope("s22"):
        moved_rows(0, "core").start()
    group_angles = angles(me * group_rows, group_rows)
    with jax.named_scope("s23"):
        cosine_ref[...] = jnp.cos(group_angles)
    with jax.named_scope("s24"):
        sine_ref[...] = jnp.sin(group_angles)

    def pass_latents(steps):
        for step in steps:
            latent_ep(step).wait_recv()
            if step % 2 == 0:
                latent_ep(step + 1).start()
            latent_core(step).start()

    with jax.named_scope("s25"):
        info_y.wait_recv()
    with jax.named_scope("s26"):
        peer_picker, peer_weight = choose_slots(
            peer_info_ref[:picks, :own_rows].T.astype(jnp.int32),
            peer_info_ref[picks : 2 * picks, :own_rows].T,
            expert_total,
            capacity,
            me // NEAR * NEAR * slot_rows,
            NEAR * slot_rows,
        )
    with jax.named_scope("s27"):
        store_split(peer_weight_ref, peer_weight)
    with jax.named_scope("s28"):
        pass_latents(range(2, ep_count, 2))
    with jax.named_scope("s29"):
        slots_ep(1).start()
    with jax.named_scope("s30"):
        moved(tokens, 0, "y").wait_recv()
    with jax.named_scope("s31"):
        moved(tokens, 0, "cross").start()
    with jax.named_scope("s32"):
        fill(peer_slots_ref, peer_picker, 1 - row)
    with jax.named_scope("s33"):
        for step in range(1, NEAR):
            peer_slots_ep(step).start()
    peer_own = pltpu.make_async_copy(
        peer_slots_ref.at[near_place], rows.at[1 - row, core, 0], own_sem.at[1]
    )
    with jax.named_scope("s34"):
        peer_own.start()
    with jax.named_scope("s35"):
        moved_rows(0, "cross").start()
    def project():
        for place, target in enumerate((query_columns_ref, latent_columns_ref)):
            pltpu.make_async_copy(target, target, weight_sem.at[place]).wait()
        query_rows = queries[...].reshape(group_rows, queries.shape[-1])
        for side in range(2):
            projected = jnp.dot(
                query_rows, query_columns_ref[side], preferred_element_type=jnp.float32
            )
            query_wide[side, :, :head_lanes] = narrow(projected[:, :head_lanes])
            query_wide[side, :, head_lanes:] = turn(
                projected[:, head_lanes:], cosine_ref[...], sine_ref[...]
            )
        for block in range(2):
            packed = latents[block].reshape(ep_count * own_rows, latents.shape[-1])
            span = slice(block * ep_count * own_rows, (block + 1) * ep_count * own_rows)
            for side in range(2):
                expanded = narrow(
                    jnp.dot(
                        packed[:, :rank_width],
                        latent_columns_ref[side],
                        preferred_element_type=jnp.float32,
                    )
                )
                keys[side, span, :head_lanes] = expanded[:, :head_lanes]
                keys[side, span, head_lanes:] = packed[:, rank_width:]
                values[side, span, :] = expanded[:, head_lanes:]

    block_rows = group_rows // 2

    def attend(side, block):
        span = slice(block * block_rows, (block + 1) * block_rows)
        query_block = query_wide[side, span, :]
        lane = lax.broadcasted_iota(jnp.int32, query_block.shape, 1)
        lane_head = jnp.where(
            lane < head_lanes,
            lane // CONTENT,
            (lane - head_lanes) // ROTARY - core * heads % (128 // ROTARY),
        )
        out_lane = lax.broadcasted_iota(jnp.int32, (block_rows, head_lanes), 1)
        result = jnp.zeros((block_rows, head_lanes), jnp.float32)
        stats = jnp.zeros((block_rows, head_lanes), jnp.float32)
        for head in range(heads):
            chosen = jnp.where(lane_head == head, query_block, jnp.zeros_like(query_block))
            scores = lax.dot_general(
                chosen, keys[side], (((1,), (1,)), ((), ())), preferred_element_type=jnp.float32
            ) * ((CONTENT + ROTARY) ** (-0.5))
            peak = jnp.max(scores, -1, keepdims=True)
            weights = jnp.exp(scores - peak)
            total = jnp.sum(weights, -1, keepdims=True)
            summed = jnp.dot(narrow(weights), values[side], preferred_element_type=jnp.float32)
            result = jnp.where(out_lane // VALUE == head, summed, result)
            stats = jnp.where(out_lane == 2 * head, peak, stats)
            stats = jnp.where(out_lane == 2 * head + 1, total, stats)
        if side == 0:
            own_sum[span, :] = result
            own_stats[span, :] = stats
        else:
            sent_sum[span, :] = narrow(result)
            sent_stats[8 * block : 8 * block + 8, :] = stats.T[:8]

    sum_y = remote(sent_sum, far_sum, y_send.at[4], y_recv.at[1], y_peer)
    stats_y = remote(sent_stats, far_stats, y_send.at[5], y_recv.at[8], y_peer)

    def merge():
        stats_y.wait_recv()
        sum_y.wait_recv()
        out_lane = lax.broadcasted_iota(jnp.int32, (block_rows, head_lanes), 1)
        for block in range(2):
            span = slice(block * block_rows, (block + 1) * block_rows)
            here = own_stats[span, :]
            there = far_stats[8 * block : 8 * block + 8, :].T
            result = jnp.zeros((block_rows, head_lanes), jnp.float32)
            for head in range(heads):
                peak_here, total_here = here[:, 2 * head : 2 * head + 1], here[:, 2 * head + 1 : 2 * head + 2]
                peak_there, total_there = there[:, 2 * head : 2 * head + 1], there[:, 2 * head + 1 : 2 * head + 2]
                peak = jnp.maximum(peak_here, peak_there)
                factor_here = jnp.exp(peak_here - peak)
                factor_there = jnp.exp(peak_there - peak)
                total = total_here * factor_here + total_there * factor_there
                summed = own_sum[span, :] * factor_here + wide(far_sum[span, :]) * factor_there
                result = jnp.where(out_lane // VALUE == head, summed / total, result)
            attended[span, :] = narrow(result)

    def mix():
        fetches[8].wait()
        for start in range(0, width, stripe):
            product = narrow(
                jnp.dot(
                    attended[...],
                    output_weight_ref[:, start : start + stripe],
                    preferred_element_type=jnp.float32,
                )
            )
            mixed[:, :, :, start : start + stripe] = product.reshape(2, 2, own_rows, stripe)

    def share():
        for fetch in fetches[9:12]:
            fetch.wait()
        for route in ("core", "cross"):
            moved(tokens, 0, route).wait_recv()
        hidden = gated_rows(
            tokens[...].reshape(group_rows, width), shared_gate_ref[...], shared_up_ref[...]
        )
        for start in range(0, width, stripe):
            product = narrow(
                jnp.dot(
                    hidden,
                    shared_down_ref[:, start : start + stripe],
                    preferred_element_type=jnp.float32,
                )
            )
            shared[:, :, :, start : start + stripe] = product.reshape(2, 2, own_rows, stripe)

    shared_half = remote(
        shared.at[:, 1 - core], half_shared, side_send.at[0], side_recv.at[0], core_peer
    )
    mixed_half = remote(
        mixed.at[:, 1 - core], half_mixed, side_send.at[1], side_recv.at[1], core_peer
    )
    shared_y = remote(
        shared.at[1 - row, core], far_shared, side_send.at[2], side_recv.at[2], y_peer
    )
    mixed_y = remote(mixed.at[1 - row, core], far_mixed, side_send.at[3], side_recv.at[3], y_peer)

    def mixed_far():
        mixed_half.wait_recv()
        mixed[1 - row, core] = narrow(wide(mixed[1 - row, core]) + wide(half_mixed[1 - row]))
        mixed_y.start()

    def arrive(step):
        slots_ep(step).wait_recv()
        moved_rows(step, "core").start()

    def arrive_peer(step):
        peer_slots_ep(step).wait_recv()
        moved_rows(step, "cross").start()

    def arrive_far(chunk, place):
        step = chunks[chunk] + place
        slots_ep(step).wait_recv()
        moved_rows(step, "y").start()
        moved_rows(step, "core", 1 + chunk).start()

    def arrive_far_peer(chunk, place):
        step = chunks[chunk] + place
        moved_rows(step, "y").wait_recv()
        moved_rows(step, "cross", 1 + chunk).start()

    def spans(expert):
        return slice(expert * capacity, (expert + 1) * capacity)

    def compute(first, count, expert):
        span = spans(expert)
        block = rows[:, :, pl.ds(first, count), span, :].reshape(4 * count * capacity, width)
        hidden = gated_rows(block, gate_ref[expert], up_ref[expert])
        for start in range(0, width, stripe):
            product = narrow(
                jnp.dot(
                    hidden,
                    down_ref[expert, :, start : start + stripe],
                    preferred_element_type=jnp.float32,
                )
            )
            part[:, :, pl.ds(first, count), span, start : start + stripe] = product.reshape(
                2, 2, count, capacity, stripe
            )

    def near_half():
        return remote(
            part.at[:, 1 - core, :NEAR],
            half_rows.at[:, :NEAR],
            half_send.at[0],
            half_recv.at[0],
            core_peer,
        )

    def far_half(chunk, expert):
        steps = pl.ds(chunks[chunk], 2)
        return remote(
            part.at[:, 1 - core, steps, spans(expert)],
            half_rows.at[:, steps, spans(expert)],
            half_send.at[0],
            half_recv.at[1 + chunk * local_experts + expert],
            core_peer,
        )

    def back_near(step):
        return remote(
            part.at[row, core, step],
            returned.at[me],
            back_send.at[0],
            back_recv.at[0],
            peer(step),
        )

    def back_peer(step):
        return remote(
            part.at[1 - row, core, step],
            returned_peer.at[near_place],
            peer_send.at[1],
            peer_recv.at[0],
            peer(step),
        )

    def back_far(step, expert):
        return remote(
            part.at[row, core, step, spans(expert)],
            returned.at[me, spans(expert)],
            back_send.at[0],
            back_recv.at[0],
            peer(step),
        )

    def y_copy(step, expert):
        return remote(
            part.at[1 - row, core, step, spans(expert)],
            far_rows.at[step - NEAR, spans(expert)],
            far_send.at[0],
            far_recv.at[expert, step - NEAR],
            y_peer,
        )

    def settle_near():
        near_half().wait_recv()
        order = list(range(1, NEAR)) + [0]
        for step in order:
            outer = narrow(wide(part[1 - row, core, step]) + wide(half_rows[1 - row, step]))
            if step:
                part[1 - row, core, step] = outer
                back_peer(step).start()
            else:
                returned_peer[near_place] = outer
        for step in order:
            total = narrow(wide(part[row, core, step]) + wide(half_rows[row, step]))
            if step:
                part[row, core, step] = total
                back_near(step).start()
            else:
                returned[me] = total

    def settle_outer(chunk, expert):
        far_half(chunk, expert).wait_recv()
        span = spans(expert)
        for step in (chunks[chunk], chunks[chunk] + 1):
            part[1 - row, core, step, span] = narrow(
                wide(part[1 - row, core, step, span]) + wide(half_rows[1 - row, step, span])
            )
            y_copy(step, expert).start()

    def settle_far(chunk, expert):
        span = spans(expert)
        for step in (chunks[chunk], chunks[chunk] + 1):
            y_copy(step, expert).wait_recv()
            part[row, core, step, span] = narrow(
                wide(part[row, core, step, span])
                + wide(half_rows[row, step, span])
                + wide(far_rows[step - NEAR, span])
            )
            back_far(step, expert).start()

    def wait_rows(first, count, group):
        for route in ("core", "cross"):
            origin_row, send_sem, recv_sem, device = routes_of[route]
            block = rows.at[origin_row, 1 - core, pl.ds(first, count)]
            remote(block, block, send_sem.at[0], recv_sem.at[4 + group], device).wait_recv()

    def far_chunk(chunk):
        wait_rows(chunks[chunk], 2, 1 + chunk)
        for expert in range(local_experts):
            compute(chunks[chunk], 2, expert)
            far_half(chunk, expert).start()

    def gather_latents():
        moved(queries, 1, "y").wait_recv()
        moved(queries, 1, "cross").start()
        pass_latents(range(1, ep_count, 2))

    def finish_latents():
        for route in ("core", "cross"):
            moved(queries, 1, route).wait_recv()
        arrived = latents.at[1 - core]
        remote(arrived, arrived, core_send.at[1], core_recv.at[1], core_peer).wait_recv()

    def near_compute():
        own_slots.wait()
        peer_own.wait()
        wait_rows(0, NEAR, 0)
        for expert in range(local_experts):
            compute(0, NEAR, expert)
        near_half().start()

    def inner(work):
        pl.when(outermost == 0)(work)

    def outer(work):
        pl.when(outermost == 1)(work)

    def attend_peer():
        gather_latents()
        finish_latents()
        project()
        attend(1, 0)
        attend(1, 1)
        stats_y.start()
        sum_y.start()

    def mix_own():
        merge()
        mix()
        mixed_half.start()

    def send_far():
        for step in (6, 4, 7, 5):
            slots_ep(step).start()

    with jax.named_scope("s36"):
        arrive_far(0, 0)
    with jax.named_scope("s37"):
        outer(attend_peer)
    with jax.named_scope("s38"):
        arrive_far(0, 1)
    with jax.named_scope("s39"):
        outer(send_far)
    with jax.named_scope("s40"):
        outer(lambda: attend(0, 0))
    with jax.named_scope("s41"):
        outer(lambda: attend(0, 1))
    with jax.named_scope("s42"):
        outer(mix_own)
    for fetch in fetches[12:]:
        fetch.wait()
    with jax.named_scope("s43"):
        for place in range(2):
            arrive_far_peer(0, place)
    with jax.named_scope("s44"):
        outer(mixed_far)
    with jax.named_scope("s45"):
        far_chunk(0)
    with jax.named_scope("s46"):
        for step in range(1, NEAR):
            arrive(step)
    with jax.named_scope("s47"):
        for expert in range(local_experts):
            settle_outer(0, expert)
    with jax.named_scope("s48"):
        for step in range(1, NEAR):
            arrive_peer(step)
    with jax.named_scope("s49"):
        inner(attend_peer)
    with jax.named_scope("s50"):
        inner(near_compute)
    with jax.named_scope("s51"):
        inner(lambda: settle_far(0, 0))
    with jax.named_scope("s52"):
        arrive_far(1, 0)
    with jax.named_scope("s53"):
        inner(lambda: settle_far(0, 1))
    with jax.named_scope("s54"):
        inner(lambda: attend(0, 0))
    with jax.named_scope("s55"):
        arrive_far(1, 1)
    with jax.named_scope("s56"):
        inner(lambda: attend(0, 1))
    with jax.named_scope("s57"):
        outer(near_compute)
    with jax.named_scope("s58"):
        outer(lambda: settle_far(0, 0))
    with jax.named_scope("s59"):
        outer(lambda: settle_far(0, 1))
    with jax.named_scope("s60"):
        inner(mix_own)
    with jax.named_scope("s61"):
        settle_near()
    with jax.named_scope("s62"):
        inner(mixed_far)
    with jax.named_scope("s63"):
        share()
    with jax.named_scope("s64"):
        shared_half.start()
    with jax.named_scope("s65"):
        for place in range(2):
            arrive_far_peer(1, place)
    with jax.named_scope("s66"):
        far_chunk(1)
    with jax.named_scope("s67"):
        for expert in range(local_experts):
            settle_outer(1, expert)
    with jax.named_scope("s68"):
        for expert in range(local_experts):
            settle_far(1, expert)
    with jax.named_scope("s69"):
        mixed_y.wait_recv()
    with jax.named_scope("s70"):
        both_out[0] = narrow(wide(mixed[row, core]) + wide(half_mixed[row]) + wide(far_mixed[...]))
    returns = returned_peer.at[: NEAR - 1]
    with jax.named_scope("s71"):
        remote(returns, returns, peer_send.at[1], peer_recv.at[0], core_peer).wait_recv()
    with jax.named_scope("s72"):
        shared_half.wait_recv()
    with jax.named_scope("s73"):
        for start in range(0, width, stripe):
            cut = slice(start, start + stripe)
            shared[1 - row, core, :, cut] = narrow(
                weighted_rows(
                    peer_weight_ref[...],
                    returned_peer[:, :, cut].reshape(NEAR * slot_rows, stripe),
                )
                + wide(shared[1 - row, core, :, cut])
                + wide(half_shared[1 - row, :, cut])
            )
    with jax.named_scope("s74"):
        shared_y.start()
    returns = returned.at[: ep_count - 1]
    with jax.named_scope("s75"):
        remote(returns, returns, back_send.at[0], back_recv.at[0], core_peer).wait_recv()
    with jax.named_scope("s76"):
        shared_y.wait_recv()
    with jax.named_scope("s77"):
        for start in range(0, width, stripe):
            cut = slice(start, start + stripe)
            both_out[1, :, cut] = narrow(
                weighted_rows(
                    weight_ref[...], returned[:, :, cut].reshape(ep_count * slot_rows, stripe)
                )
                + wide(shared[row, core, :, cut])
                + wide(half_shared[row, :, cut])
                + wide(far_shared[:, cut])
            )

    blocks = rows.at[0, 0]
    with jax.named_scope("s78"):
        for source, sem in (
            (slots_ref.at[: ep_count - 1], ep_send.at[0]),
            (latents.at[0, : ep_count - 1], ep_send.at[1]),
            (blocks, core_send.at[0]),
            (latents.at[0], core_send.at[1]),
            (blocks, cross_send.at[0]),
            (rows.at[0, 0, NEAR:], y_send.at[0]),
            (rows.at[0, 0, : NEAR - 1], peer_send.at[0]),
            (rows.at[0, 0, : NEAR - 1], peer_send.at[1]),
            (rows.at[0, 0, : ep_count - 1], back_send.at[0]),
            (rows.at[0, 0, NEAR:], far_send.at[0]),
            (part.at[0], half_send.at[0]),
        ):
            remote(source, source, sem, core_recv.at[0], core_peer).wait_send()
    with jax.named_scope("s79"):
        for route in ("y", "core", "cross"):
            moved(queries, 1, route).wait_send()
            moved(tokens, 0, route).wait_send()
    with jax.named_scope("s80"):
        for copy in (info_y, sum_y, stats_y, shared_half, mixed_half, shared_y, mixed_y):
            copy.wait_send()


def block_call(ep_count, capacity, *operands):
    query_latent, key_latent = operands[:2]
    own_rows, width = operands[5].shape
    head_lanes = operands[14].shape[0]
    local_experts = operands[15].shape[0]
    slot_rows = local_experts * capacity
    latent_shape = (own_rows, key_latent.shape[1] + 128)
    anywhere = pl.BlockSpec(memory_space=pl.ANY)

    def held(*shape):
        return pltpu.VMEM(shape, jnp.bfloat16)

    def precise(*shape):
        return pltpu.VMEM(shape, jnp.float32)

    def sems(*shape):
        return pltpu.SemaphoreType.DMA(shape)

    group_rows = 4 * own_rows
    key_rows = 2 * ep_count * own_rows
    row_block = (slot_rows, width)
    side = (own_rows, width)
    return pl.pallas_call(
        lambda *refs: block_kernel(ep_count, capacity, *refs),
        out_shape=jax.ShapeDtypeStruct((2,) + side, jnp.bfloat16),
        in_specs=[anywhere] * 21,
        out_specs=pl.BlockSpec(memory_space=pltpu.VMEM),
        scratch_shapes=[pltpu.VMEM(operand.shape, operand.dtype) for operand in operands[:10]]
        + [
            precise(group_rows, 128),
            precise(group_rows, 128),
            held(ep_count, *row_block),
            held(NEAR, *row_block),
            held(2, query_latent.shape[1], head_lanes + 128),
            held(2, key_latent.shape[1], 2 * head_lanes),
            held(head_lanes, width),
            held(3 * own_rows, ep_count * slot_rows),
            held(3 * own_rows, NEAR * slot_rows),
            held(2, 2, ep_count, *row_block),
            held(2, ep_count, *latent_shape),
            held(2, 2, *side),
            held(2, 2, *query_latent.shape),
        ]
        + [held(*operand.shape) for operand in operands[15:]]
        + [
            held(2, key_rows, head_lanes + 128),
            held(2, key_rows, head_lanes),
            held(2, group_rows, head_lanes + 128),
            held(group_rows, head_lanes),
            held(2, 2, ep_count, *row_block),
            held(2, ep_count, *row_block),
            held(ep_count - NEAR, *row_block),
            held(ep_count, *row_block),
            held(NEAR, *row_block),
            held(2, 2, *side),
            held(2, *side),
            held(*side),
            held(2, 2, *side),
            held(2, *side),
            held(*side),
            precise(8, 128),
            precise(8, 128),
            precise(group_rows, head_lanes),
            precise(group_rows, head_lanes),
            held(group_rows, head_lanes),
            held(group_rows, head_lanes),
            precise(16, head_lanes),
            precise(16, head_lanes),
        ]
        + [
            sems(2),
            sems(2, ep_count),
            sems(6),
            sems(9),
            sems(4),
            sems(7),
            sems(4),
            sems(7),
            sems(2),
            sems(NEAR),
            sems(1),
            sems(1),
            sems(1),
            sems(local_experts, ep_count - NEAR),
            sems(1),
            sems(1 + 2 * local_experts),
            sems(4),
            sems(4),
            sems(2),
            sems(9),
            sems(10),
        ],
        compiler_params=pltpu.CompilerParams(
            collective_id=0, has_side_effects=True, vmem_limit_bytes=VMEM_LIMIT
        ),
        name="block",
    )(*operands)


def shards(
    query_latent,
    key_latent,
    rotary_key,
    query_gain,
    latent_gain,
    query_content,
    query_rotary,
    key_content,
    value_weight,
    output_weight,
    expert_input,
    norm_gain,
    routes,
    route_weight,
    expert_gate,
    expert_up,
    expert_down,
    shared_gate,
    shared_up,
    shared_down,
):
    group_size = lax.axis_size("tp")
    expert_groups = lax.axis_size("ep")
    token_rows = expert_input.shape[0]
    picks = routes.shape[1]
    local_experts = expert_gate.shape[0]
    expert_total = local_experts * expert_groups
    capacity = 2 * token_rows * picks // expert_total
    if group_size != 4 or capacity % 16 or not fits_kernel(expert_groups, local_experts * capacity):
        return shards_plain(
            query_latent,
            key_latent,
            rotary_key,
            query_gain,
            latent_gain,
            query_content,
            query_rotary,
            key_content,
            value_weight,
            output_weight,
            expert_input,
            norm_gain,
            routes,
            route_weight,
            expert_gate,
            expert_up,
            expert_down,
            shared_gate,
            shared_up,
            shared_down,
        )
    frequency = rope_base ** (-np.arange(ROTARY // 2) * 2.0 / ROTARY)
    both = block_call(
        expert_groups,
        capacity,
        query_latent,
        key_latent,
        rotary_key.T,
        query_gain[None, :],
        latent_gain[None, :],
        expert_input,
        norm_gain[None, :],
        routes.T,
        route_weight.T,
        jnp.asarray(np.tile(np.repeat(frequency, 2), 128 // ROTARY)[None, :], jnp.float32),
        query_content,
        query_rotary,
        key_content,
        value_weight,
        output_weight,
        expert_gate,
        expert_up,
        expert_down,
        shared_gate,
        shared_up,
        shared_down,
    )
    return (both[0], both[1])


def solution(mesh):
    in_specs = (
        P(("ep", "tp"), None),
        P(("ep", "tp"), None),
        P(("ep", "tp"), None),
        P(),
        P(),
        P(),
        P(),
        P(),
        P(),
        P("tp", None),
        P(("ep", "tp"), None),
        P(),
        P(("ep", "tp"), None),
        P(("ep", "tp"), None),
        P("ep", None, "tp"),
        P("ep", None, "tp"),
        P("ep", "tp", None),
        P(None, "tp"),
        P(None, "tp"),
        P("tp", None),
    )
    out_specs = (P(("ep", "tp"), None), P(("ep", "tp"), None))
    return jax.shard_map(shards, mesh=mesh, in_specs=in_specs, out_specs=out_specs, check_vma=False)
```
